128 devices in a mesh: sp: 16 (over z, x), tp: 8 (over y, core).
Axes of the slice: x: 4, y: 4, z: 4, core: 2. Of those that a mesh axis runs over, the one named last changes fastest.
Arguments:
- latent: bfloat16 [32768, 2048], P(('sp', 'tp')), may hold values from -8 to 8
- context: bfloat16 [512, 2048], P('sp'), may hold values from -8 to 8
- latent_condition: bfloat16 [2048], replicated, may hold values from -4 to 4
- context_condition: bfloat16 [2048], replicated, may hold values from -4 to 4
- shift_weight: bfloat16 [2048, 2048], P('sp', 'tp'), may hold values from -0.125 to 0.125
- scale_weight: bfloat16 [2048, 2048], P('sp', 'tp'), may hold values from -0.125 to 0.125
- gate_weight: bfloat16 [2048, 2048], P('sp', 'tp'), may hold values from -0.125 to 0.125
- norm_gain: float32 [2048], replicated, may hold values from 0.1 to 1.9
- query_weight: bfloat16 [2048, 512], replicated, may hold values from -0.125 to 0.125
- key_weight: bfloat16 [2048, 512], replicated, may hold values from -0.125 to 0.125
- value_weight: bfloat16 [2048, 1024], replicated, may hold values from -0.125 to 0.125
- outgate_weight: bfloat16 [2048, 1024], replicated, may hold values from -0.125 to 0.125
- down_weight: bfloat16 [2048, 32], replicated, may hold values from -0.125 to 0.125
- up_weight: bfloat16 [32, 512], replicated, may hold values from -2 to 2
- decay_bias: float32 [512], replicated, as said below
- out_weight: bfloat16 [1024, 2048], replicated, may hold values from -0.1875 to 0.1875
- post_gain: float32 [2048], replicated, may hold values from 0.1 to 1.9
Outputs:
- updated: bfloat16 [32768, 2048], P(('sp', 'tp'))
The draws below stay inside these ranges and needn't reach their ends.
Inputs may be any that keep to these rules, and one draw needn't show every extreme that they name: decay_bias is at least 0; counting heads from 0, the channels of heads 1, 3, 5, … are at least log(2048) + 2, those of heads 0, 2, 4, … at most 1.5.
All inputs are finite; a program needn't handle non-finite values.
Results may differ from the reference program's by a relative error of at most 0.0035.
The reference program's roundings to bfloat16 on the way count: a program that leaves them out, or rounds other values in their place, can miss the bound.
Values may be sent and summed in bfloat16 or wider, within the bound.
A program may use at most 192 MiB of HBM per device.

```python
import jax
import jax.numpy as jnp
from jax import lax

D = 2048
HEADS = 16
DK = 32
DV = 64
RANK = 32
BLOCK = 32
CTX = 512
KEYW = 512
VALW = 1024
LATENT = 32768


def draw_latent(key, part):
    noise_key, slow_key = jax.random.split(key)
    noise_part = jax.random.normal(noise_key, (LATENT, D), jnp.float32)
    slow_part = jax.random.normal(slow_key, (LATENT // 128, D), jnp.float32)
    values = noise_part + jnp.repeat(slow_part, 128, axis=0)
    return jnp.clip(values, -8.0, 8.0).astype(jnp.bfloat16)


def draw_context(key, part):
    noise_key, slow_key = jax.random.split(jax.random.fold_in(key, 7))
    noise_part = jax.random.normal(noise_key, (CTX, D), jnp.float32)
    slow_part = 1.5 * jax.random.normal(slow_key, (CTX // 4, D), jnp.float32)
    values = noise_part + jnp.repeat(slow_part, 4, axis=0)
    return jnp.clip(values, -8.0, 8.0).astype(jnp.bfloat16)


def draw_decay_bias(key, part):
    channel = jnp.arange(HEADS * DK)
    weak_head = channel // DK % 2 == 1
    unit_draw = jax.random.uniform(key, (HEADS * DK,), jnp.float32)
    strong_value = 1.5 * unit_draw
    weak_value = jnp.log(LATENT / 16.0) + 2.0 + 2.0 * unit_draw
    return jnp.where(weak_head, weak_value, strong_value).astype(jnp.float32)


def levels(key, shape, cuts, smallest, largest):
    level = 1.0
    for position, parts in cuts:
        steps = jax.random.uniform(jax.random.fold_in(jax.random.fold_in(key, 6), position), (parts,), jnp.float32, smallest / len(cuts), largest / len(cuts))
        level = level * jnp.repeat(jnp.exp(steps), shape[position] // parts).reshape((-1,) + (1,) * (len(shape) - 1 - position))
    return level


def normal_values(stream_key, shape, deviation, bound, pieces=(), dtype=jnp.bfloat16):
    array = jax.random.normal(stream_key, shape, jnp.float32) * deviation
    if len(pieces) > 0:
        array = levels(stream_key, shape, pieces, -0.22, 0.18) * array
    return jnp.clip(array, min=-bound, max=bound).astype(dtype)


def setup_inputs(seed: int = 0) -> dict:
    seeds = jax.random.split(jax.random.key(seed), 18)
    latent = draw_latent(jax.random.fold_in(seeds[17], 71), 0)
    context = draw_context(jax.random.fold_in(seeds[17], 71), 0)
    latent_condition = normal_values(seeds[2], (D,), 1.0, 4.0)
    context_condition = normal_values(seeds[3], (D,), 1.0, 4.0)
    shift_weight = normal_values(seeds[4], (D, D), D ** -0.5, 0.125, ((0, 16), (1, 8)))
    scale_weight = normal_values(seeds[5], (D, D), D ** -0.5, 0.125, ((0, 16), (1, 8)))
    gate_weight = normal_values(seeds[6], (D, D), D ** -0.5, 0.125, ((0, 16), (1, 8)))
    norm_gain = jnp.clip(1.0 + 0.18 * jax.random.normal(seeds[7], (D,), jnp.float32), 0.1, 1.9)
    query_weight = normal_values(seeds[8], (D, KEYW), D ** -0.5, 0.125)
    key_weight = normal_values(seeds[9], (D, KEYW), D ** -0.5, 0.125)
    value_weight = normal_values(seeds[10], (D, VALW), D ** -0.5, 0.125)
    outgate_weight = normal_values(seeds[11], (D, VALW), D ** -0.5, 0.125)
    down_weight = normal_values(seeds[12], (D, RANK), D ** -0.5, 0.125)
    up_weight = normal_values(seeds[13], (RANK, KEYW), (RANK // 4) ** -0.5, 2.0)
    decay_bias = draw_decay_bias(jax.random.fold_in(seeds[17], 71), 0)
    out_weight = normal_values(seeds[15], (VALW, D), VALW ** -0.5, 0.1875)
    post_gain = jnp.clip(1.0 + 0.18 * jax.random.normal(seeds[16], (D,), jnp.float32), 0.1, 1.9)
    return dict(latent=latent, context=context, latent_condition=latent_condition, context_condition=context_condition, shift_weight=shift_weight, scale_weight=scale_weight, gate_weight=gate_weight, norm_gain=norm_gain, query_weight=query_weight, key_weight=key_weight, value_weight=value_weight, outgate_weight=outgate_weight, down_weight=down_weight, up_weight=up_weight, decay_bias=decay_bias, out_weight=out_weight, post_gain=post_gain)


epsilon = 1e-06
decay_temper = 16.0
highest = lax.Precision.HIGHEST

def rms_factor(values):
    return lax.rsqrt(lax.optimization_barrier(jnp.mean(values * values, axis=-1, keepdims=True)) + epsilon)

def stored(values):
    return lax.optimization_barrier(values.astype(jnp.bfloat16))

def modulated(tokens, norm_gain, shift_row, scale_row):
    values = tokens.astype(jnp.float32)
    return (values * rms_factor(values) * norm_gain * (1.0 + scale_row) + shift_row).astype(jnp.bfloat16)

def project(normed, weight):
    return jnp.dot(normed, weight, preferred_element_type=jnp.float32)

def log_decays(normed, down_weight, up_weight, decay_bias):
    low_rank = project(normed, down_weight).astype(jnp.bfloat16)
    return jax.nn.log_sigmoid(project(low_rank, up_weight) + decay_bias) / decay_temper

def weighted_state(key_rows, value_rows, weights):
    row_count = key_rows.shape[0]
    scaled = (key_rows.astype(jnp.float32) * weights).reshape(row_count, HEADS, DK)
    value_heads = value_rows.astype(jnp.float32).reshape(row_count, HEADS, DV)
    return jnp.einsum('sha,she->hae', scaled, value_heads, precision=highest)

def segment_states(key_rows, value_rows, log_decay):
    inclusive = jnp.cumsum(log_decay, axis=0)
    total_log = inclusive[-1]
    after_log = total_log - inclusive
    before_log = inclusive - log_decay
    return (weighted_state(key_rows, value_rows, jnp.exp(after_log)), weighted_state(key_rows, value_rows, jnp.exp(before_log)), total_log)

def block_terms(query_heads, key_heads, value_heads, log_heads):
    block_count = query_heads.shape[0] // BLOCK
    q_blocks = query_heads.reshape(block_count, BLOCK, HEADS, DK)
    k_blocks = key_heads.reshape(block_count, BLOCK, HEADS, DK)
    v_blocks = value_heads.reshape(block_count, BLOCK, HEADS, DV)
    inside = jnp.cumsum(log_heads.reshape(block_count, BLOCK, HEADS, DK), axis=1)
    closing = inside[:, -1]
    q_decayed = q_blocks * jnp.exp(inside)
    k_decayed = k_blocks * jnp.exp(-inside)
    scores = jnp.einsum('ntha,nsha->nhts', q_decayed, k_decayed, precision=highest)
    lower_mask = jnp.tril(jnp.ones((BLOCK, BLOCK), bool))
    scores = jnp.where(lower_mask, scores, 0.0)
    within = jnp.einsum('nhts,nshe->nthe', scores, v_blocks, precision=highest)
    summary = jnp.einsum('nsha,nshe->nhae', k_blocks * jnp.exp(closing[:, None] - inside), v_blocks, precision=highest)
    return (q_decayed, within, closing, summary)

def direction(query_heads, key_heads, value_heads, log_heads, start_state):
    q_decayed, within, closing, summary = block_terms(query_heads, key_heads, value_heads, log_heads)

    def advance(carry_state, inputs):
        closing_one, summary_one = inputs
        return (jnp.exp(closing_one)[..., None] * carry_state + summary_one, carry_state)
    last_state, entering = lax.scan(advance, start_state, (closing, summary))
    across = jnp.einsum('ntha,nhae->nthe', q_decayed, entering, precision=highest)
    return (within + across).reshape(-1, HEADS, DV)

def reference(latent, context, latent_condition, context_condition, shift_weight, scale_weight, gate_weight, norm_gain, query_weight, key_weight, value_weight, outgate_weight, down_weight, up_weight, decay_bias, out_weight, post_gain):
    conditions = jnp.stack([latent_condition, context_condition])
    cond_act = jax.nn.silu(conditions.astype(jnp.float32)).astype(jnp.bfloat16)
    shifts = project(cond_act, shift_weight)
    scales = project(cond_act, scale_weight)
    gates = project(cond_act, gate_weight)
    ctx_normed = modulated(context, norm_gain, shifts[1], scales[1])
    ctx_keys = stored(project(ctx_normed, key_weight))
    ctx_values = stored(project(ctx_normed, value_weight))
    ctx_log = log_decays(ctx_normed, down_weight, up_weight, decay_bias)
    ctx_forward, ctx_backward, unused_total = segment_states(ctx_keys, ctx_values, ctx_log)
    normed = modulated(latent, norm_gain, shifts[0], scales[0])
    row_count = latent.shape[0]
    query_rows = stored(project(normed, query_weight))
    key_rows = stored(project(normed, key_weight))
    value_rows = stored(project(normed, value_weight))
    outgate_rows = stored(project(normed, outgate_weight))
    log_decay = log_decays(normed, down_weight, up_weight, decay_bias)
    query_heads = query_rows.astype(jnp.float32).reshape(row_count, HEADS, DK) * DK ** (-0.5)
    key_heads = key_rows.astype(jnp.float32).reshape(row_count, HEADS, DK)
    value_heads = value_rows.astype(jnp.float32).reshape(row_count, HEADS, DV)
    log_heads = log_decay.reshape(row_count, HEADS, DK)
    forward_out = direction(query_heads, key_heads, value_heads, log_heads, ctx_forward)
    backward_out = jnp.flip(direction(jnp.flip(query_heads, 0), jnp.flip(key_heads, 0), jnp.flip(value_heads, 0), jnp.flip(log_heads, 0), ctx_backward), 0)
    mixed_heads = forward_out + backward_out
    normalized = mixed_heads * rms_factor(mixed_heads)
    gate_heads = jax.nn.silu(outgate_rows.astype(jnp.float32).reshape(row_count, HEADS, DV))
    gated = (normalized * gate_heads).reshape(row_count, HEADS * DV).astype(jnp.bfloat16)
    branch = stored(project(gated, out_weight)).astype(jnp.float32)
    result = latent.astype(jnp.float32) + gates[0] * (branch * rms_factor(branch)) * post_gain
    return result.astype(jnp.bfloat16)
```

```python
import jax
import jax.numpy as jnp
from jax import lax
from jax.experimental import pallas as pl
from jax.experimental.pallas import tpu as pltpu
from jax.sharding import PartitionSpec as P

F32 = jnp.float32
BF16 = jnp.bfloat16
MESH = pl.DeviceIdType.MESH
EPS = 1e-06

NSP = 16
NTP = 8
D = 2048
HEADS = 16
DK = 32
DV = 64
ROWS = 256
CROWS = 32
ALL = ROWS + CROWS
T = 64
NB = ROWS // T
NG = 4
MSG = 80

LOCAL = ("down", "key", "value", "query", "outgate", "out")


def dot(a, b):
    return jnp.dot(a, b, preferred_element_type=F32)


def dot_dims(a, b, ca, cb):
    return lax.dot_general(a, b, (((ca,), (cb,)), ((), ())), preferred_element_type=F32)


def iota(shape, dim):
    return lax.broadcasted_iota(jnp.int32, shape, dim)


def split3(x):
    hi = x.astype(BF16)
    rest = x - hi.astype(F32)
    mid = rest.astype(BF16)
    return hi, mid, (rest - mid.astype(F32)).astype(BF16)


def sum_rows(tri, x):
    hi, mid, lo = split3(x)
    return dot(tri, hi) + dot(tri, mid) + dot(tri, lo)


def log_decays(pre):
    return (jnp.minimum(pre, 0.0) - jnp.log1p(jnp.exp(-jnp.abs(pre)))) * (1.0 / 16.0)


def put_message(ref, at, state, total):
    hi, mid, lo = split3(total)
    row = iota((16, 128), 0)
    tail = jnp.where(
        row == 0,
        hi.astype(F32),
        jnp.where(row == 1, mid.astype(F32), jnp.where(row == 2, lo.astype(F32), 0.0)),
    )
    ref[at, 0:64, :] = state.astype(BF16)
    ref[at, 64:MSG, :] = tail.astype(BF16)


def get_message(ref, at):
    state = ref[at, 0:64, :].astype(F32)
    tail = ref[at, 64:MSG, :].astype(F32)
    return state, tail[0:1] + tail[1:2] + tail[2:3]


def kernel(
    latent,
    context,
    lat_cond,
    ctx_cond,
    shift_w,
    scale_w,
    gate_w,
    gain,
    query_w,
    key_w,
    value_w,
    outgate_w,
    down_w,
    up_w,
    bias,
    out_w,
    post_gain,
    out,
    s,
):
    sp = lax.axis_index("sp")
    tp = lax.axis_index("tp")

    def sp_peer(d):
        return lax.rem(sp + d, NSP)

    def tp_peer(d):
        return lax.rem(tp + d, NTP)

    barrier = pltpu.get_barrier_semaphore()
    for d in range(1, NSP):
        pl.semaphore_signal(barrier, inc=1, device_id=(sp_peer(d), tp), device_id_type=MESH)
    for d in range(1, NTP):
        pl.semaphore_signal(barrier, inc=1, device_id=(sp, tp_peer(d)), device_id_type=MESH)

    pairs = dict(
        latent=(latent, s["lat"]),
        context=(context, s["ctx"]),
        down=(down_w, s["wd"]),
        key=(key_w, s["wk"]),
        value=(value_w, s["wv"]),
        query=(query_w, s["wq"]),
        outgate=(outgate_w, s["wg"]),
        out=(out_w, s["wo"]),
    )
    loads = {
        name: pltpu.make_async_copy(src, dst, s["load_sem"].at[i])
        for i, (name, (src, dst)) in enumerate(pairs.items())
    }
    for name in loads:
        loads[name].start()

    sends = []

    def exchange(axis, src, dst, send_sem, recv_sem):
        n, peer = (NSP, sp_peer) if axis == "sp" else (NTP, tp_peer)
        for d in range(1, n):
            to = peer(d)
            copy = pltpu.make_async_remote_copy(
                src_ref=src(to),
                dst_ref=dst(sp if axis == "sp" else tp),
                send_sem=send_sem.at[d - 1],
                recv_sem=recv_sem.at[d - 1],
                device_id=(to, tp) if axis == "sp" else (sp, to),
                device_id_type=MESH,
            )
            copy.start()
            sends.append(copy)

    def arrive(axis, dst, send_sem, recv_sem):
        n, peer = (NSP, sp_peer) if axis == "sp" else (NTP, tp_peer)
        for d in range(1, n):
            origin = peer(n - d)
            pltpu.make_async_remote_copy(
                src_ref=dst(origin),
                dst_ref=dst(origin),
                send_sem=send_sem.at[d - 1],
                recv_sem=recv_sem.at[d - 1],
                device_id=(origin, tp) if axis == "sp" else (sp, origin),
                device_id_type=MESH,
            ).wait_recv()

    cols = pl.ds(pl.multiple_of(sp * 128, 128), 128)
    parity = lax.rem(iota((16, 128), 0), 2)
    cond = jnp.where(
        parity == 0,
        jnp.broadcast_to(lat_cond[:, cols].astype(F32), (16, 128)),
        jnp.broadcast_to(ctx_cond[:, cols].astype(F32), (16, 128)),
    )
    act = (cond * lax.logistic(cond)).astype(BF16)
    row8 = iota((8, 256), 0)
    part = jnp.where(
        row8 < 2,
        dot(act, shift_w[...])[0:8],
        jnp.where(row8 < 4, dot(act, scale_w[...])[0:8], dot(act, gate_w[...])[0:8]),
    )
    mod1, mod2 = s["mod1"], s["mod2"]
    mod1[sp] = part
    pl.semaphore_wait(barrier, NSP + NTP - 2)
    exchange("sp", lambda to: mod1.at[sp], lambda i: mod1.at[i], s["m1s"], s["m1r"])

    head128, head256, tri, ones = s["head128"], s["head256"], s["tri"], s["ones"]

    def as_bf16(cond):
        return jnp.where(cond, 1.0, 0.0).astype(BF16)

    head128[...] = as_bf16(iota((256, 128), 0) // 64 == iota((256, 128), 1) // 32)
    head256[...] = as_bf16(iota((256, 256), 0) // 64 == iota((256, 256), 1) // 64)
    r256, c256 = iota((256, 256), 0), iota((256, 256), 1)
    tri[...] = as_bf16((r256 // T == c256 // T) & (c256 <= r256))

    arrive("sp", lambda i: mod1.at[i], s["m1s"], s["m1r"])
    total = mod1[0]
    for i in range(1, NSP):
        total = total + mod1[i]
    mod2[tp] = total
    exchange("tp", lambda to: mod2.at[tp], lambda i: mod2.at[i], s["m2s"], s["m2r"])
    loads["latent"].wait()
    loads["context"].wait()
    arrive("tp", lambda i: mod2.at[i], s["m2s"], s["m2r"])
    modv = s["modv"]
    for j in range(NTP):
        modv[:, j * 256 : (j + 1) * 256] = mod2[j]

    lat, ctx, normed = s["lat"], s["ctx"], s["normed"]

    def norm_rows(x, row):
        x = x.astype(F32)
        factor = lax.rsqrt(jnp.mean(x * x, axis=-1, keepdims=True) + EPS)
        scaled = x * factor * gain[...] * (1.0 + modv[2 + row : 3 + row, :])
        return (scaled + modv[row : row + 1, :]).astype(BF16)

    @pl.loop(0, ROWS // 16)
    def _(i):
        at = pl.ds(pl.multiple_of(i * 16, 16), 16)
        normed[at, :] = norm_rows(lat[at, :], 0)

    @pl.loop(0, CROWS // 16)
    def _(i):
        at = pl.multiple_of(i * 16, 16)
        normed[pl.ds(ROWS + at, 16), :] = norm_rows(ctx[pl.ds(at, 16), :], 1)

    ld, lcum, kk, vv = s["ld"], s["lcum"], s["kk"], s["vv"]
    loads["down"].wait()
    low = dot(normed[...], s["wd"][...]).astype(BF16)
    ld[...] = log_decays(dot(low, up_w[...]) + bias[...])
    lcum[0:ROWS, :] = sum_rows(tri[...], ld[0:ROWS, :])
    lcum[ROWS:ALL, :] = sum_rows(tri[0:CROWS, 0:CROWS], ld[ROWS:ALL, :])
    loads["key"].wait()
    kk[...] = dot(normed[...], s["wk"][...]).astype(BF16)
    loads["value"].wait()

    @pl.loop(0, 2)
    def _(c):
        at = pl.ds(pl.multiple_of(c * 512, 512), 512)
        vv[:, at] = dot(normed[...], s["wv"][:, at]).astype(BF16)

    lane_head = lax.rem(iota((64, 256), 1), 128) // 32
    summ, ent, tots = s["summ"], s["ent"], s["tots"]

    def summaries(rows, count, at):
        cum = lcum[rows, :]
        before = cum - ld[rows, :]
        closing = cum[count - 1 : count, :]
        keys = kk[rows, :].astype(F32)
        key_f = (keys * jnp.exp(closing - cum)).astype(BF16)
        key_b = (keys * jnp.exp(before)).astype(BF16)
        for g in range(NG):
            k_at = slice(g * 128, (g + 1) * 128)
            both = jnp.concatenate([key_f[:, k_at], key_b[:, k_at]], axis=1)
            full = dot_dims(vv[rows, g * 256 : (g + 1) * 256], both, 0, 0)
            state = jnp.zeros((64, 256), F32)
            for h in range(4):
                state = jnp.where(lane_head == h, full[h * 64 : (h + 1) * 64], state)
            summ[at, :, g * 256 : (g + 1) * 256] = state

    summaries(slice(ROWS, ALL), CROWS, NB)
    ctx_msg, seg_msg = s["ctx_msg"], s["seg_msg"]
    ctx_all, recv_a, grp_all, back, recv_c = (
        s["ctx_all"],
        s["recv_a"],
        s["grp_all"],
        s["back"],
        s["recv_c"],
    )
    ctx_total = lcum[ALL - 8 : ALL, :][7:8]
    for g in range(NG):
        for d in range(2):
            at = slice(g * 256 + d * 128, g * 256 + (d + 1) * 128)
            put_message(
                ctx_msg, d * NG + g, summ[NB, :, at], ctx_total[:, g * 128 : (g + 1) * 128]
            )
    ctx_all[sp] = ctx_msg[tp]
    exchange("sp", lambda to: ctx_all.at[sp], lambda i: ctx_all.at[i], s["cs"], s["cr"])

    @pl.loop(0, NB)
    def _(n):
        summaries(pl.ds(pl.multiple_of(n * T, T), T), T, n)

    closings = [lcum[n * T + T - 8 : n * T + T, :][7:8] for n in range(NB)]
    for n in range(NB):
        tots[n : n + 1, :] = closings[n]
    for g in range(NG):
        k_at = slice(g * 128, (g + 1) * 128)
        close = [c[:, k_at] for c in closings]
        whole = close[0] + close[1] + close[2] + close[3]
        for d in range(2):
            at = slice(g * 256 + d * 128, g * 256 + (d + 1) * 128)
            run = jnp.zeros((64, 128), F32)
            for n in range(NB) if d == 0 else reversed(range(NB)):
                ent[n, :, at] = run.astype(BF16)
                run = jnp.exp(close[n]) * run + summ[n, :, at]
            put_message(seg_msg, d * NG + g, run, whole)
    recv_a[tp] = seg_msg[tp]
    exchange("tp", lambda to: seg_msg.at[to], lambda i: recv_a.at[i], s["as"], s["ar"])

    qq, gg = s["qq"], s["gg"]
    loads["query"].wait()
    qq[...] = dot(normed[0:ROWS, :], s["wq"][...]).astype(BF16)

    flip = lax.div(tp, NTP // 2)
    arrive("tp", lambda i: recv_a.at[i], s["as"], s["ar"])
    pre_s, pre_c = s["pre_s"], s["pre_c"]
    run = jnp.zeros((64, 128), F32)
    run_log = jnp.zeros((1, 128), F32)
    for i in range(NTP):
        at = i + flip * (NTP - 1 - 2 * i)
        pre_s[at] = run
        pre_c[at] = jnp.broadcast_to(run_log, (8, 128))
        state, total = get_message(recv_a, at)
        run = jnp.exp(total) * run + state
        run_log = run_log + total
    put_message(grp_all, sp, run, run_log)
    exchange("sp", lambda to: grp_all.at[sp], lambda i: grp_all.at[i], s["gs"], s["gr"])

    loads["outgate"].wait()

    @pl.loop(0, 2)
    def _(c):
        at = pl.ds(pl.multiple_of(c * 512, 512), 512)
        gg[:, at] = dot(normed[0:ROWS, :], s["wg"][:, at]).astype(BF16)

    mixed, qd = s["mixed"], s["qd"]
    t_row = iota((64, 256), 0)
    s_col = lax.rem(iota((64, 256), 1), 64)
    up_to, from_on = s_col <= t_row, s_col >= t_row

    def four(x, mask):
        return jnp.concatenate([x, x, x, x], axis=0) * mask

    @pl.loop(0, NB)
    def _(n):
        rows = pl.ds(pl.multiple_of(n * T, T), T)
        cum = lcum[rows, :]
        before = cum - ld[rows, :]
        middle, closing = cum[T // 2 - 1 : T // 2, :], cum[T - 1 : T, :]
        ahead = jnp.zeros((1, 512), F32)
        behind = jnp.zeros((1, 512), F32)
        for m in range(NB):
            ahead = ahead + jnp.where(m < n, tots[m : m + 1, :], 0.0)
            behind = behind + jnp.where(m > n, tots[m : m + 1, :], 0.0)
        q = qq[rows, :].astype(F32) * DK**-0.5
        k = kk[rows, :].astype(F32)
        qm_f = (q * jnp.exp(cum - middle)).astype(BF16)
        qm_b = (q * jnp.exp(middle - before)).astype(BF16)
        km_f = (k * jnp.exp(middle - cum)).astype(BF16)
        km_b = (k * jnp.exp(before - middle)).astype(BF16)
        qs_f = (q * jnp.exp(cum)).astype(BF16)
        qs_b = (q * jnp.exp(closing - before)).astype(BF16)
        qd_f = (q * jnp.exp(cum + ahead)).astype(BF16)
        qd_b = (q * jnp.exp(closing - before + behind)).astype(BF16)
        for g in range(NG):
            k_at = slice(g * 128, (g + 1) * 128)
            v_at = slice(g * 256, (g + 1) * 256)
            qd[rows, v_at] = jnp.concatenate([qd_f[:, k_at], qd_b[:, k_at]], axis=1)
            score_f = dot_dims(qm_f[:, k_at], four(km_f[:, k_at], head128[...]), 1, 1)
            score_b = dot_dims(qm_b[:, k_at], four(km_b[:, k_at], head128[...]), 1, 1)
            score = jnp.where(up_to, score_f, 0.0) + jnp.where(from_on, score_b, 0.0)
            within = dot(score.astype(BF16), four(vv[rows, v_at], head256[...]))
            entering = ent[n, :, v_at]
            states = jnp.concatenate(
                [
                    four(entering[:, 0:128], head128[...]),
                    four(entering[:, 128:256], head128[...]),
                ],
                axis=1,
            )
            across = dot_dims(
                jnp.concatenate([qs_f[:, k_at], qs_b[:, k_at]], axis=1), states, 1, 1
            )
            mixed[rows, v_at] = within + across

    arrive("sp", lambda i: ctx_all.at[i], s["cs"], s["cr"])
    arrive("sp", lambda i: grp_all.at[i], s["gs"], s["gr"])
    reach = jnp.zeros((64, 128), F32)
    for i in range(NSP):
        state, total = get_message(ctx_all, i + flip * (NSP - 1 - 2 * i))
        reach = jnp.exp(total) * reach + state
    rank = sp + flip * (NSP - 1 - 2 * sp)
    for i in range(NSP):
        state, total = get_message(grp_all, i + flip * (NSP - 1 - 2 * i))
        reach = jnp.where(i < rank, jnp.exp(total) * reach + state, reach)
    for j in range(NTP):
        back[j] = (pre_s[j] + jnp.exp(pre_c[j][0:1]) * reach).astype(BF16)
    recv_c[tp] = back[tp]
    exchange("tp", lambda to: back.at[to], lambda i: recv_c.at[i], s["bs"], s["br"])
    ones[...] = head256[...]
    arrive("tp", lambda i: recv_c.at[i], s["bs"], s["br"])

    gated = s["gated"]
    for g in range(NG):
        v_at = slice(g * 256, (g + 1) * 256)
        states = jnp.concatenate(
            [four(recv_c[g], head128[...]), four(recv_c[NG + g], head128[...])], axis=1
        )
        values = mixed[:, v_at] + dot_dims(qd[:, v_at], states, 1, 1)
        square = values * values
        hi = square.astype(BF16)
        low = (square - hi.astype(F32)).astype(BF16)
        power = dot(hi, ones[...]) + dot(low, ones[...])
        gate = gg[:, v_at].astype(F32)
        normal = values * lax.rsqrt(power * (1.0 / DV) + EPS)
        gated[:, v_at] = (normal * (gate * lax.logistic(gate))).astype(BF16)

    branch = s["branch"]
    loads["out"].wait()

    @pl.loop(0, 4)
    def _(c):
        at = pl.ds(pl.multiple_of(c * 512, 512), 512)
        branch[:, at] = dot(gated[...], s["wo"][:, at]).astype(BF16)

    @pl.loop(0, ROWS // 16)
    def _(i):
        at = pl.ds(pl.multiple_of(i * 16, 16), 16)
        b = branch[at, :].astype(F32)
        factor = lax.rsqrt(jnp.mean(b * b, axis=-1, keepdims=True) + EPS)
        added = modv[4:5, :] * (b * factor) * post_gain[...]
        out[at, :] = (lat[at, :].astype(F32) + added).astype(BF16)

    for copy in sends:
        copy.wait_send()


def scratch():
    vmem, sems = pltpu.VMEM, pltpu.SemaphoreType.DMA
    return dict(
        lat=vmem((ROWS, D), BF16),
        ctx=vmem((CROWS, D), BF16),
        wd=vmem((D, 32), BF16),
        wk=vmem((D, 512), BF16),
        wv=vmem((D, 1024), BF16),
        wq=vmem((D, 512), BF16),
        wg=vmem((D, 1024), BF16),
        wo=vmem((1024, D), BF16),
        mod1=vmem((NSP, 8, 256), F32),
        mod2=vmem((NTP, 8, 256), F32),
        modv=vmem((8, D), F32),
        normed=vmem((ALL, D), BF16),
        head128=vmem((256, 128), BF16),
        head256=vmem((256, 256), BF16),
        ones=vmem((256, 256), BF16),
        tri=vmem((256, 256), BF16),
        ld=vmem((ALL, 512), F32),
        lcum=vmem((ALL, 512), F32),
        kk=vmem((ALL, 512), BF16),
        vv=vmem((ALL, 1024), BF16),
        qq=vmem((ROWS, 512), BF16),
        gg=vmem((ROWS, 1024), BF16),
        summ=vmem((NB + 1, 64, 1024), F32),
        ent=vmem((NB, 64, 1024), BF16),
        tots=vmem((8, 512), F32),
        ctx_msg=vmem((NTP, MSG, 128), BF16),
        seg_msg=vmem((NTP, MSG, 128), BF16),
        ctx_all=vmem((NSP, MSG, 128), BF16),
        grp_all=vmem((NSP, MSG, 128), BF16),
        recv_a=vmem((NTP, MSG, 128), BF16),
        pre_s=vmem((NTP, 64, 128), F32),
        pre_c=vmem((NTP, 8, 128), F32),
        back=vmem((NTP, 64, 128), BF16),
        recv_c=vmem((NTP, 64, 128), BF16),
        mixed=vmem((ROWS, 1024), F32),
        qd=vmem((ROWS, 1024), BF16),
        gated=vmem((ROWS, 1024), BF16),
        branch=vmem((ROWS, D), BF16),
        load_sem=sems((8,)),
        m1s=sems((NSP - 1,)),
        m1r=sems((NSP - 1,)),
        m2s=sems((NTP - 1,)),
        m2r=sems((NTP - 1,)),
        cs=sems((NSP - 1,)),
        cr=sems((NSP - 1,)),
        gs=sems((NSP - 1,)),
        gr=sems((NSP - 1,)),
        bs=sems((NTP - 1,)),
        br=sems((NTP - 1,)),
        **{"as": sems((NTP - 1,)), "ar": sems((NTP - 1,))},
    )


def shards(
    latent,
    context,
    latent_condition,
    context_condition,
    shift_weight,
    scale_weight,
    gate_weight,
    norm_gain,
    query_weight,
    key_weight,
    value_weight,
    outgate_weight,
    down_weight,
    up_weight,
    decay_bias,
    out_weight,
    post_gain,
):
    spaces = "hhvvvvvvhhhhhvvhv"
    specs = [
        pl.BlockSpec(memory_space=pltpu.VMEM if c == "v" else pl.ANY) for c in spaces
    ]
    return pl.pallas_call(
        kernel,
        out_shape=jax.ShapeDtypeStruct((ROWS, D), BF16),
        in_specs=specs,
        out_specs=pl.BlockSpec(memory_space=pltpu.VMEM),
        scratch_shapes=[scratch()],
        compiler_params=pltpu.CompilerParams(
            collective_id=0, has_side_effects=True, vmem_limit_bytes=60 * 1024 * 1024
        ),
    )(
        latent,
        context,
        latent_condition[None],
        context_condition[None],
        shift_weight,
        scale_weight,
        gate_weight,
        norm_gain[None],
        query_weight,
        key_weight,
        value_weight,
        outgate_weight,
        down_weight,
        up_weight,
        decay_bias[None],
        out_weight,
        post_gain[None],
    )


def solution(mesh):
    tokens = P(("sp", "tp"), None)
    maps = P("sp", "tp")
    placed = (tokens, P("sp", None), P(), P(), maps, maps, maps) + (P(),) * 10
    return jax.shard_map(
        shards, mesh=mesh, in_specs=placed, out_specs=tokens, check_vma=False
    )
```

```python
import jax
import jax.numpy as jnp
from jax import lax
from jax.experimental import pallas as pl
from jax.experimental.pallas import tpu as pltpu
from jax.sharding import PartitionSpec as P

F32 = jnp.float32
BF16 = jnp.bfloat16
MESH = pl.DeviceIdType.MESH
EPS = 1e-06

NSP = 16
NTP = 8
D = 2048
HEADS = 16
DK = 32
DV = 64
ROWS = 256
CROWS = 32
ALL = ROWS + CROWS
T = 64
NB = ROWS // T
NG = 4
MSG = 80


def far_first(lengths):
    steps = [(a, b) for a in range(lengths[0]) for b in range(lengths[1]) if (a, b) != (0, 0)]
    hops = [0, 1, 2, 1]
    weight = 2 if lengths[1] == 2 else 1
    return sorted(steps, key=lambda t: -(weight * hops[t[0]] + hops[t[1]]))


SP_STEPS = far_first((4, 4))
TP_STEPS = far_first((4, 2))


def dot(a, b):
    return jnp.dot(a, b, preferred_element_type=F32)


def dot_dims(a, b, ca, cb):
    return lax.dot_general(a, b, (((ca,), (cb,)), ((), ())), preferred_element_type=F32)


def iota(shape, dim):
    return lax.broadcasted_iota(jnp.int32, shape, dim)


def split3(x):
    hi = x.astype(BF16)
    rest = x - hi.astype(F32)
    mid = rest.astype(BF16)
    return hi, mid, (rest - mid.astype(F32)).astype(BF16)


def sum_rows(tri, x):
    hi, mid, lo = split3(x)
    return dot(tri, hi) + dot(tri, mid) + dot(tri, lo)


def log_decays(pre):
    return (jnp.minimum(pre, 0.0) - jnp.log1p(jnp.exp(-jnp.abs(pre)))) * (1.0 / 16.0)


def put_message(ref, at, state, total):
    hi, mid, lo = split3(total)
    row = iota((16, 128), 0)
    tail = jnp.where(
        row == 0,
        hi.astype(F32),
        jnp.where(row == 1, mid.astype(F32), jnp.where(row == 2, lo.astype(F32), 0.0)),
    )
    ref[at, 0:64, :] = state.astype(BF16)
    ref[at, 64:MSG, :] = tail.astype(BF16)


def get_message(ref, at):
    state = ref[at, 0:64, :].astype(F32)
    tail = ref[at, 64:MSG, :].astype(F32)
    return state, tail[0:1] + tail[1:2] + tail[2:3]


def kernel(
    latent,
    context,
    lat_cond,
    ctx_cond,
    shift_w,
    scale_w,
    gate_w,
    gain,
    query_w,
    key_w,
    value_w,
    outgate_w,
    down_w,
    up_w,
    bias,
    out_w,
    post_gain,
    out,
    s,
):
    sp = lax.axis_index("sp")
    tp = lax.axis_index("tp")

    z, x = lax.div(sp, 4), lax.rem(sp, 4)
    y, c = lax.div(tp, 2), lax.rem(tp, 2)

    def sp_peer(step):
        return lax.rem(z + step[0], 4) * 4 + lax.rem(x + step[1], 4)

    def tp_peer(step):
        return lax.rem(y + step[0], 4) * 2 + lax.rem(c + step[1], 2)

    barrier = pltpu.get_barrier_semaphore()
    for step in SP_STEPS:
        pl.semaphore_signal(barrier, inc=1, device_id=(sp_peer(step), tp), device_id_type=MESH)
    for step in TP_STEPS:
        pl.semaphore_signal(barrier, inc=1, device_id=(sp, tp_peer(step)), device_id_type=MESH)

    pairs = dict(
        lat_cond=(lat_cond, s["lat_cond"]),
        ctx_cond=(ctx_cond, s["ctx_cond"]),
        shift=(shift_w, s["shift_w"]),
        scale=(scale_w, s["scale_w"]),
        gate=(gate_w, s["gate_w"]),
        latent=(latent, s["lat"]),
        context=(context, s["ctx"]),
        gain=(gain, s["gain"]),
        bias=(bias, s["bias"]),
        up=(up_w, s["up_w"]),
        post=(post_gain, s["post_gain"]),
        down=(down_w, s["wd"]),
        key=(key_w, s["wk"]),
        value=(value_w, s["wv"]),
        query=(query_w, s["wq"]),
        outgate=(outgate_w, s["wg"]),
        out=(out_w, s["wo"]),
    )
    loads = {
        name: pltpu.make_async_copy(src, dst, s["load_sem"].at[i])
        for i, (name, (src, dst)) in enumerate(pairs.items())
    }
    for name in loads:
        loads[name].start()

    def loaded(*names):
        for name in names:
            loads[name].wait()

    sends = []

    def exchange(axis, src, dst, send_sem, recv_sem):
        steps, peer = (SP_STEPS, sp_peer) if axis == "sp" else (TP_STEPS, tp_peer)
        for d, step in enumerate(steps):
            to = peer(step)
            copy = pltpu.make_async_remote_copy(
                src_ref=src(to),
                dst_ref=dst(sp if axis == "sp" else tp),
                send_sem=send_sem.at[d],
                recv_sem=recv_sem.at[d],
                device_id=(to, tp) if axis == "sp" else (sp, to),
                device_id_type=MESH,
            )
            copy.start()
            sends.append(copy)

    def arrive(axis, dst, send_sem, recv_sem):
        steps, wrap, peer = (
            (SP_STEPS, (4, 4), sp_peer) if axis == "sp" else (TP_STEPS, (4, 2), tp_peer)
        )
        for d, step in reversed(list(enumerate(steps))):
            origin = peer((wrap[0] - step[0], wrap[1] - step[1]))
            pltpu.make_async_remote_copy(
                src_ref=dst(origin),
                dst_ref=dst(origin),
                send_sem=send_sem.at[d],
                recv_sem=recv_sem.at[d],
                device_id=(origin, tp) if axis == "sp" else (sp, origin),
                device_id_type=MESH,
            ).wait_recv()

    loaded("lat_cond", "ctx_cond", "shift", "scale", "gate")
    row16 = iota((16, 128), 0)

    def cond_row(name):
        mine = jnp.where(row16 == sp, s[name][...].astype(F32), 0.0)
        return jnp.broadcast_to(jnp.sum(mine, axis=0, keepdims=True), (16, 128))

    cond = jnp.where(lax.rem(row16, 2) == 0, cond_row("lat_cond"), cond_row("ctx_cond"))
    act = (cond * lax.logistic(cond)).astype(BF16)
    row8 = iota((8, 256), 0)
    part = jnp.where(
        row8 < 2,
        dot(act, s["shift_w"][...])[0:8],
        jnp.where(row8 < 4, dot(act, s["scale_w"][...])[0:8], dot(act, s["gate_w"][...])[0:8]),
    )
    mod1, mod2 = s["mod1"], s["mod2"]
    mod1[sp] = part
    pl.semaphore_wait(barrier, NSP + NTP - 2)
    exchange("sp", lambda to: mod1.at[sp], lambda i: mod1.at[i], s["m1s"], s["m1r"])

    head128, head256, tri, ones = s["head128"], s["head256"], s["tri"], s["ones"]

    def as_bf16(cond):
        return jnp.where(cond, 1.0, 0.0).astype(BF16)

    head128[...] = as_bf16(iota((256, 128), 0) // 64 == iota((256, 128), 1) // 32)
    head256[...] = as_bf16(iota((256, 256), 0) // 64 == iota((256, 256), 1) // 64)
    r256, c256 = iota((256, 256), 0), iota((256, 256), 1)
    tri[...] = as_bf16((r256 // T == c256 // T) & (c256 <= r256))

    lat, ctx, normed, ready = s["lat"], s["ctx"], s["normed"], s["ready"]
    gain_row = s["gain"]

    def norm_rows(x):
        x = x.astype(F32)
        factor = lax.rsqrt(jnp.mean(x * x, axis=-1, keepdims=True) + EPS)
        return x * factor * gain_row[...]

    loaded("latent", "context", "gain")

    @pl.loop(0, CROWS // 16)
    def _(i):
        at = pl.multiple_of(i * 16, 16)
        ready[pl.ds(ROWS + at, 16), :] = norm_rows(ctx[pl.ds(at, 16), :])

    @pl.loop(0, ROWS // 16)
    def _(i):
        at = pl.ds(pl.multiple_of(i * 16, 16), 16)
        ready[at, :] = norm_rows(lat[at, :])

    arrive("sp", lambda i: mod1.at[i], s["m1s"], s["m1r"])
    total = mod1[0]
    for i in range(1, NSP):
        total = total + mod1[i]
    mod2[tp] = total
    exchange("tp", lambda to: mod2.at[tp], lambda i: mod2.at[i], s["m2s"], s["m2r"])
    arrive("tp", lambda i: mod2.at[i], s["m2s"], s["m2r"])
    modv = s["modv"]
    for j in range(NTP):
        modv[:, j * 256 : (j + 1) * 256] = mod2[j]

    loaded("bias", "up", "post", "down", "key", "value", "query", "outgate", "out")

    def modulated(at, row):
        scaled = ready[at, :] * (1.0 + modv[2 + row : 3 + row, :])
        normed[at, :] = (scaled + modv[row : row + 1, :]).astype(BF16)

    @pl.loop(0, ROWS // 32)
    def _(i):
        modulated(pl.ds(pl.multiple_of(i * 32, 32), 32), 0)

    modulated(pl.ds(ROWS, CROWS), 1)

    ld, lcum, kk, vv = s["ld"], s["lcum"], s["kk"], s["vv"]
    low = dot_dims(normed[...], s["wd"][...], 1, 1).astype(BF16)
    ld[...] = log_decays(dot(low, s["up_w"][...]) + s["bias"][...])
    lcum[0:ROWS, :] = sum_rows(tri[...], ld[0:ROWS, :])
    lcum[ROWS:ALL, :] = sum_rows(tri[0:CROWS, 0:CROWS], ld[ROWS:ALL, :])
    kk[...] = dot(normed[...], s["wk"][...]).astype(BF16)

    @pl.loop(0, 2)
    def _(c):
        at = pl.ds(pl.multiple_of(c * 512, 512), 512)
        vv[:, at] = dot(normed[...], s["wv"][:, at]).astype(BF16)

    lane_head = lax.rem(iota((64, 256), 1), 128) // 32
    summ, ent, tots = s["summ"], s["ent"], s["tots"]

    def summaries(rows, count, at):
        cum = lcum[rows, :]
        before = cum - ld[rows, :]
        closing = cum[count - 1 : count, :]
        keys = kk[rows, :].astype(F32)
        key_f = (keys * jnp.exp(closing - cum)).astype(BF16)
        key_b = (keys * jnp.exp(before)).astype(BF16)
        for g in range(NG):
            k_at = slice(g * 128, (g + 1) * 128)
            both = jnp.concatenate([key_f[:, k_at], key_b[:, k_at]], axis=1)
            full = dot_dims(vv[rows, g * 256 : (g + 1) * 256], both, 0, 0)
            state = jnp.zeros((64, 256), F32)
            for h in range(4):
                state = jnp.where(lane_head == h, full[h * 64 : (h + 1) * 64], state)
            summ[at, :, g * 256 : (g + 1) * 256] = state

    summaries(slice(ROWS, ALL), CROWS, NB)
    ctx_msg, seg_msg = s["ctx_msg"], s["seg_msg"]
    ctx_all, recv_a, grp_all, back, recv_c = (
        s["ctx_all"],
        s["recv_a"],
        s["grp_all"],
        s["back"],
        s["recv_c"],
    )
    ctx_total = lcum[ALL - 8 : ALL, :][7:8]
    for g in range(NG):
        for d in range(2):
            at = slice(g * 256 + d * 128, g * 256 + (d + 1) * 128)
            put_message(
                ctx_msg, d * NG + g, summ[NB, :, at], ctx_total[:, g * 128 : (g + 1) * 128]
            )
    ctx_all[sp] = ctx_msg[tp]
    exchange("sp", lambda to: ctx_all.at[sp], lambda i: ctx_all.at[i], s["cs"], s["cr"])

    @pl.loop(0, NB)
    def _(n):
        summaries(pl.ds(pl.multiple_of(n * T, T), T), T, n)

    closings = [lcum[n * T + T - 8 : n * T + T, :][7:8] for n in range(NB)]
    for n in range(NB):
        tots[n : n + 1, :] = closings[n]
    for g in range(NG):
        k_at = slice(g * 128, (g + 1) * 128)
        close = [c[:, k_at] for c in closings]
        whole = close[0] + close[1] + close[2] + close[3]
        for d in range(2):
            at = slice(g * 256 + d * 128, g * 256 + (d + 1) * 128)
            run = jnp.zeros((64, 128), F32)
            for n in range(NB) if d == 0 else reversed(range(NB)):
                ent[n, :, at] = run.astype(BF16)
                run = jnp.exp(close[n]) * run + summ[n, :, at]
            put_message(seg_msg, d * NG + g, run, whole)
    recv_a[tp] = seg_msg[tp]
    exchange("tp", lambda to: seg_msg.at[to], lambda i: recv_a.at[i], s["as"], s["ar"])

    qq, gg = s["qq"], s["gg"]
    qq[...] = dot(normed[0:ROWS, :], s["wq"][...]).astype(BF16)

    flip = lax.div(tp, NTP // 2)
    arrive("tp", lambda i: recv_a.at[i], s["as"], s["ar"])
    pre_s, pre_c = s["pre_s"], s["pre_c"]
    run = jnp.zeros((64, 128), F32)
    run_log = jnp.zeros((1, 128), F32)
    for i in range(NTP):
        at = i + flip * (NTP - 1 - 2 * i)
        pre_s[at] = run
        pre_c[at] = jnp.broadcast_to(run_log, (8, 128))
        state, total = get_message(recv_a, at)
        run = jnp.exp(total) * run + state
        run_log = run_log + total
    put_message(grp_all, sp, run, run_log)
    exchange("sp", lambda to: grp_all.at[sp], lambda i: grp_all.at[i], s["gs"], s["gr"])


    @pl.loop(0, 2)
    def _(c):
        at = pl.ds(pl.multiple_of(c * 512, 512), 512)
        gg[:, at] = dot(normed[0:ROWS, :], s["wg"][:, at]).astype(BF16)

    mixed, qd = s["mixed"], s["qd"]
    t_row = iota((64, 256), 0)
    s_col = lax.rem(iota((64, 256), 1), 64)
    up_to, from_on = s_col <= t_row, s_col >= t_row

    def four(x, mask):
        return jnp.concatenate([x, x, x, x], axis=0) * mask

    @pl.loop(0, NB)
    def _(n):
        rows = pl.ds(pl.multiple_of(n * T, T), T)
        cum = lcum[rows, :]
        before = cum - ld[rows, :]
        middle, closing = cum[T // 2 - 1 : T // 2, :], cum[T - 1 : T, :]
        ahead = jnp.zeros((1, 512), F32)
        behind = jnp.zeros((1, 512), F32)
        for m in range(NB):
            ahead = ahead + jnp.where(m < n, tots[m : m + 1, :], 0.0)
            behind = behind + jnp.where(m > n, tots[m : m + 1, :], 0.0)
        q = qq[rows, :].astype(F32) * DK**-0.5
        k = kk[rows, :].astype(F32)
        qm_f = (q * jnp.exp(cum - middle)).astype(BF16)
        qm_b = (q * jnp.exp(middle - before)).astype(BF16)
        km_f = (k * jnp.exp(middle - cum)).astype(BF16)
        km_b = (k * jnp.exp(before - middle)).astype(BF16)
        qs_f = (q * jnp.exp(cum)).astype(BF16)
        qs_b = (q * jnp.exp(closing - before)).astype(BF16)
        qd_f = (q * jnp.exp(cum + ahead)).astype(BF16)
        qd_b = (q * jnp.exp(closing - before + behind)).astype(BF16)
        for g in range(NG):
            k_at = slice(g * 128, (g + 1) * 128)
            v_at = slice(g * 256, (g + 1) * 256)
            qd[rows, v_at] = jnp.concatenate([qd_f[:, k_at], qd_b[:, k_at]], axis=1)
            score_f = dot_dims(qm_f[:, k_at], four(km_f[:, k_at], head128[...]), 1, 1)
            score_b = dot_dims(qm_b[:, k_at], four(km_b[:, k_at], head128[...]), 1, 1)
            score = jnp.where(up_to, score_f, 0.0) + jnp.where(from_on, score_b, 0.0)
            within = dot(score.astype(BF16), four(vv[rows, v_at], head256[...]))
            entering = ent[n, :, v_at]
            states = jnp.concatenate(
                [
                    four(entering[:, 0:128], head128[...]),
                    four(entering[:, 128:256], head128[...]),
                ],
                axis=1,
            )
            across = dot_dims(
                jnp.concatenate([qs_f[:, k_at], qs_b[:, k_at]], axis=1), states, 1, 1
            )
            mixed[rows, v_at] = within + across

    arrive("sp", lambda i: ctx_all.at[i], s["cs"], s["cr"])
    reach = jnp.zeros((64, 128), F32)
    for i in range(NSP):
        state, total = get_message(ctx_all, i + flip * (NSP - 1 - 2 * i))
        reach = jnp.exp(total) * reach + state
    arrive("sp", lambda i: grp_all.at[i], s["gs"], s["gr"])
    rank = sp + flip * (NSP - 1 - 2 * sp)
    for i in range(NSP):
        state, total = get_message(grp_all, i + flip * (NSP - 1 - 2 * i))
        reach = jnp.where(i < rank, jnp.exp(total) * reach + state, reach)
    for j in range(NTP):
        back[j] = (pre_s[j] + jnp.exp(pre_c[j][0:1]) * reach).astype(BF16)
    recv_c[tp] = back[tp]
    exchange("tp", lambda to: back.at[to], lambda i: recv_c.at[i], s["bs"], s["br"])
    ones[...] = head256[...]
    arrive("tp", lambda i: recv_c.at[i], s["bs"], s["br"])

    gated = s["gated"]
    for g in range(NG):
        v_at = slice(g * 256, (g + 1) * 256)
        states = jnp.concatenate(
            [four(recv_c[g], head128[...]), four(recv_c[NG + g], head128[...])], axis=1
        )
        values = mixed[:, v_at] + dot_dims(qd[:, v_at], states, 1, 1)
        square = values * values
        hi = square.astype(BF16)
        low = (square - hi.astype(F32)).astype(BF16)
        power = dot(hi, ones[...]) + dot(low, ones[...])
        gate = gg[:, v_at].astype(F32)
        normal = values * lax.rsqrt(power * (1.0 / DV) + EPS)
        gated[:, v_at] = (normal * (gate * lax.logistic(gate))).astype(BF16)

    branch, result = s["branch"], s["result"]
    squares = jnp.zeros((ROWS, 128), F32)
    for i in range(4):
        at = slice(i * 512, (i + 1) * 512)
        part = dot(gated[...], s["wo"][:, at]).astype(BF16)
        branch[:, at] = part
        part = part.astype(F32)
        part = part * part
        for j in range(4):
            squares = squares + part[:, j * 128 : (j + 1) * 128]
    mean = jnp.sum(squares, axis=-1, keepdims=True) * (1.0 / D)
    s["factor"][...] = jnp.broadcast_to(lax.rsqrt(mean + EPS), (ROWS, 128))
    weight = s["weight"]
    weight[...] = jnp.broadcast_to(modv[4:5, :] * s["post_gain"][...], (8, D))

    @pl.loop(0, ROWS // 16)
    def _(i):
        at = pl.ds(pl.multiple_of(i * 16, 16), 16)
        factor = s["factor"][at, 0:1]
        added = branch[at, :].astype(F32) * factor * weight[0:1, :]
        result[at, :] = (lat[at, :].astype(F32) + added).astype(BF16)

        @pl.when(lax.rem(i, 4) == 3)
        def _():
            rows = pl.ds(pl.multiple_of((i - 3) * 16, 64), 64)
            pltpu.make_async_copy(
                result.at[rows, :], out.at[rows, :], s["out_sem"].at[lax.div(i, 4)]
            ).start()

    for i in range(ROWS // 64):
        rows = pl.ds(i * 64, 64)
        pltpu.make_async_copy(result.at[rows, :], out.at[rows, :], s["out_sem"].at[i]).wait()

    for copy in sends:
        copy.wait_send()


def scratch():
    vmem, sems = pltpu.VMEM, pltpu.SemaphoreType.DMA
    return dict(
        lat=vmem((ROWS, D), BF16),
        ctx=vmem((CROWS, D), BF16),
        wd=vmem((32, D), BF16),
        wk=vmem((D, 512), BF16),
        wv=vmem((D, 1024), BF16),
        wq=vmem((D, 512), BF16),
        wg=vmem((D, 1024), BF16),
        wo=vmem((1024, D), BF16),
        mod1=vmem((NSP, 8, 256), F32),
        mod2=vmem((NTP, 8, 256), F32),
        modv=vmem((8, D), F32),
        normed=vmem((ALL, D), BF16),
        head128=vmem((256, 128), BF16),
        head256=vmem((256, 256), BF16),
        ones=vmem((256, 256), BF16),
        tri=vmem((256, 256), BF16),
        ld=vmem((ALL, 512), F32),
        lcum=vmem((ALL, 512), F32),
        kk=vmem((ALL, 512), BF16),
        vv=vmem((ALL, 1024), BF16),
        qq=vmem((ROWS, 512), BF16),
        gg=vmem((ROWS, 1024), BF16),
        summ=vmem((NB + 1, 64, 1024), F32),
        ent=vmem((NB, 64, 1024), BF16),
        tots=vmem((8, 512), F32),
        ctx_msg=vmem((NTP, MSG, 128), BF16),
        seg_msg=vmem((NTP, MSG, 128), BF16),
        ctx_all=vmem((NSP, MSG, 128), BF16),
        grp_all=vmem((NSP, MSG, 128), BF16),
        recv_a=vmem((NTP, MSG, 128), BF16),
        pre_s=vmem((NTP, 64, 128), F32),
        pre_c=vmem((NTP, 8, 128), F32),
        back=vmem((NTP, 64, 128), BF16),
        recv_c=vmem((NTP, 64, 128), BF16),
        mixed=vmem((ROWS, 1024), F32),
        qd=vmem((ROWS, 1024), BF16),
        gated=vmem((ROWS, 1024), BF16),
        branch=vmem((ROWS, D), BF16),
        lat_cond=vmem((16, 128), BF16),
        ctx_cond=vmem((16, 128), BF16),
        shift_w=vmem((128, 256), BF16),
        scale_w=vmem((128, 256), BF16),
        gate_w=vmem((128, 256), BF16),
        gain=vmem((1, D), F32),
        bias=vmem((1, 512), F32),
        up_w=vmem((32, 512), BF16),
        post_gain=vmem((1, D), F32),
        ready=vmem((ALL, D), F32),
        result=vmem((ROWS, D), BF16),
        factor=vmem((ROWS, 128), F32),
        weight=vmem((8, D), F32),
        out_sem=sems((4,)),
        load_sem=sems((17,)),
        m1s=sems((NSP - 1,)),
        m1r=sems((NSP - 1,)),
        m2s=sems((NTP - 1,)),
        m2r=sems((NTP - 1,)),
        cs=sems((NSP - 1,)),
        cr=sems((NSP - 1,)),
        gs=sems((NSP - 1,)),
        gr=sems((NSP - 1,)),
        bs=sems((NTP - 1,)),
        br=sems((NTP - 1,)),
        **{"as": sems((NTP - 1,)), "ar": sems((NTP - 1,))},
    )


def shards(
    latent,
    context,
    latent_condition,
    context_condition,
    shift_weight,
    scale_weight,
    gate_weight,
    norm_gain,
    query_weight,
    key_weight,
    value_weight,
    outgate_weight,
    down_weight,
    up_weight,
    decay_bias,
    out_weight,
    post_gain,
):
    hbm = pl.BlockSpec(memory_space=pl.ANY)
    return pl.pallas_call(
        kernel,
        out_shape=jax.ShapeDtypeStruct((ROWS, D), BF16),
        in_specs=[hbm] * 17,
        out_specs=hbm,
        scratch_shapes=[scratch()],
        compiler_params=pltpu.CompilerParams(
            collective_id=0, has_side_effects=True, vmem_limit_bytes=60 * 1024 * 1024
        ),
    )(
        latent,
        context,
        latent_condition.reshape(16, 128),
        context_condition.reshape(16, 128),
        shift_weight,
        scale_weight,
        gate_weight,
        norm_gain[None],
        query_weight,
        key_weight,
        value_weight,
        outgate_weight,
        down_weight.T,
        up_weight,
        decay_bias[None],
        out_weight,
        post_gain[None],
    )


def solution(mesh):
    tokens = P(("sp", "tp"), None)
    maps = P("sp", "tp")
    placed = (tokens, P("sp", None), P(), P(), maps, maps, maps) + (P(),) * 10
    return jax.shard_map(
        shards, mesh=mesh, in_specs=placed, out_specs=tokens, check_vma=False
    )
```

```python
import jax
import jax.numpy as jnp
from jax import lax
from jax.experimental import pallas as pl
from jax.experimental.pallas import tpu as pltpu
from jax.sharding import PartitionSpec as P

F32 = jnp.float32
BF16 = jnp.bfloat16
MESH = pl.DeviceIdType.MESH
EPS = 1e-06

NSP = 16
NTP = 8
D = 2048
HEADS = 16
DK = 32
DV = 64
ROWS = 256
CROWS = 32
ALL = ROWS + CROWS
T = 64
NB = ROWS // T
NG = 4
MSG = 80


def far_first(lengths):
    steps = [(a, b) for a in range(lengths[0]) for b in range(lengths[1]) if (a, b) != (0, 0)]
    hops = [0, 1, 2, 1]
    weight = 2 if lengths[1] == 2 else 1
    return sorted(steps, key=lambda t: -(weight * hops[t[0]] + hops[t[1]]))


SP_STEPS = far_first((4, 4))
TP_STEPS = far_first((4, 2))


def dot(a, b):
    return jnp.dot(a, b, preferred_element_type=F32)


def dot_dims(a, b, ca, cb):
    return lax.dot_general(a, b, (((ca,), (cb,)), ((), ())), preferred_element_type=F32)


def iota(shape, dim):
    return lax.broadcasted_iota(jnp.int32, shape, dim)


def split3(x):
    hi = x.astype(BF16)
    rest = x - hi.astype(F32)
    mid = rest.astype(BF16)
    return hi, mid, (rest - mid.astype(F32)).astype(BF16)


def sum_rows(tri, x):
    hi, mid, lo = split3(x)
    return dot(tri, hi) + dot(tri, mid) + dot(tri, lo)


def log_decays(pre):
    return (jnp.minimum(pre, 0.0) - jnp.log1p(jnp.exp(-jnp.abs(pre)))) * (1.0 / 16.0)


def put_message(ref, at, state, total):
    hi, mid, lo = split3(total)
    row = iota((16, 128), 0)
    tail = jnp.where(
        row == 0,
        hi.astype(F32),
        jnp.where(row == 1, mid.astype(F32), jnp.where(row == 2, lo.astype(F32), 0.0)),
    )
    ref[at, 0:64, :] = state.astype(BF16)
    ref[at, 64:MSG, :] = tail.astype(BF16)


def get_message(ref, at):
    state = ref[at, 0:64, :].astype(F32)
    tail = ref[at, 64:MSG, :].astype(F32)
    return state, tail[0:1] + tail[1:2] + tail[2:3]


def kernel(
    latent,
    context,
    lat_cond,
    ctx_cond,
    shift_w,
    scale_w,
    gate_w,
    gain,
    query_w,
    key_w,
    value_w,
    outgate_w,
    down_w,
    up_w,
    bias,
    out_w,
    post_gain,
    out,
    s,
):
    sp = lax.axis_index("sp")
    tp = lax.axis_index("tp")

    z, x = lax.div(sp, 4), lax.rem(sp, 4)
    y, c = lax.div(tp, 2), lax.rem(tp, 2)

    def sp_peer(step):
        return lax.rem(z + step[0], 4) * 4 + lax.rem(x + step[1], 4)

    def tp_peer(step):
        return lax.rem(y + step[0], 4) * 2 + lax.rem(c + step[1], 2)

    barrier = pltpu.get_barrier_semaphore()
    for step in SP_STEPS:
        pl.semaphore_signal(barrier, inc=1, device_id=(sp_peer(step), tp), device_id_type=MESH)
    for step in TP_STEPS:
        pl.semaphore_signal(barrier, inc=1, device_id=(sp, tp_peer(step)), device_id_type=MESH)

    pairs = dict(
        lat_cond=(lat_cond, s["lat_cond"]),
        ctx_cond=(ctx_cond, s["ctx_cond"]),
        shift=(shift_w, s["shift_w"]),
        scale=(scale_w, s["scale_w"]),
        gate=(gate_w, s["gate_w"]),
        latent=(latent, s["lat"]),
        context=(context, s["ctx"]),
        gain=(gain, s["gain"]),
        bias=(bias, s["bias"]),
        up=(up_w, s["up_w"]),
        post=(post_gain, s["post_gain"]),
        down=(down_w, s["wd"]),
        key=(key_w, s["wk"]),
        value=(value_w, s["wv"]),
        query=(query_w, s["wq"]),
        outgate=(outgate_w, s["wg"]),
        out=(out_w, s["wo"]),
    )
    loads = {
        name: pltpu.make_async_copy(src, dst, s["load_sem"].at[i])
        for i, (name, (src, dst)) in enumerate(pairs.items())
    }
    for name in loads:
        loads[name].start()

    def loaded(*names):
        for name in names:
            loads[name].wait()

    sends = []

    def exchange(axis, src, dst, send_sem, recv_sem):
        steps, peer = (SP_STEPS, sp_peer) if axis == "sp" else (TP_STEPS, tp_peer)
        for d, step in enumerate(steps):
            to = peer(step)
            copy = pltpu.make_async_remote_copy(
                src_ref=src(to),
                dst_ref=dst(sp if axis == "sp" else tp),
                send_sem=send_sem.at[d],
                recv_sem=recv_sem.at[d],
                device_id=(to, tp) if axis == "sp" else (sp, to),
                device_id_type=MESH,
            )
            copy.start()
            sends.append(copy)

    def arrive(axis, dst, send_sem, recv_sem):
        steps, wrap, peer = (
            (SP_STEPS, (4, 4), sp_peer) if axis == "sp" else (TP_STEPS, (4, 2), tp_peer)
        )
        for d, step in reversed(list(enumerate(steps))):
            origin = peer((wrap[0] - step[0], wrap[1] - step[1]))
            pltpu.make_async_remote_copy(
                src_ref=dst(origin),
                dst_ref=dst(origin),
                send_sem=send_sem.at[d],
                recv_sem=recv_sem.at[d],
                device_id=(origin, tp) if axis == "sp" else (sp, origin),
                device_id_type=MESH,
            ).wait_recv()

    loaded("lat_cond", "ctx_cond", "shift", "scale", "gate")
    row16 = iota((16, 128), 0)

    def cond_row(name):
        mine = jnp.where(row16 == sp, s[name][...].astype(F32), 0.0)
        return jnp.broadcast_to(jnp.sum(mine, axis=0, keepdims=True), (16, 128))

    cond = jnp.where(lax.rem(row16, 2) == 0, cond_row("lat_cond"), cond_row("ctx_cond"))
    act = (cond * lax.logistic(cond)).astype(BF16)
    row8 = iota((8, 256), 0)
    part = jnp.where(
        row8 < 2,
        dot(act, s["shift_w"][...])[0:8],
        jnp.where(row8 < 4, dot(act, s["scale_w"][...])[0:8], dot(act, s["gate_w"][...])[0:8]),
    )
    mod1, mod2 = s["mod1"], s["mod2"]
    mod1[sp] = part
    pl.semaphore_wait(barrier, NSP + NTP - 2)
    exchange("sp", lambda to: mod1.at[sp], lambda i: mod1.at[i], s["m1s"], s["m1r"])

    head128, head256, tri, ones = s["head128"], s["head256"], s["tri"], s["ones"]

    def as_bf16(cond):
        return jnp.where(cond, 1.0, 0.0).astype(BF16)

    head128[...] = as_bf16(iota((256, 128), 0) // 64 == iota((256, 128), 1) // 32)
    head256[...] = as_bf16(iota((256, 256), 0) // 64 == iota((256, 256), 1) // 64)
    r256, c256 = iota((256, 256), 0), iota((256, 256), 1)
    tri[...] = as_bf16((r256 // T == c256 // T) & (c256 <= r256))

    lat, ctx, normed, ready = s["lat"], s["ctx"], s["normed"], s["ready"]
    gain_row = s["gain"]

    def norm_rows(x):
        x = x.astype(F32)
        factor = lax.rsqrt(jnp.mean(x * x, axis=-1, keepdims=True) + EPS)
        return x * factor * gain_row[...]

    loaded("latent", "context", "gain")

    @pl.loop(0, CROWS // 16)
    def _(i):
        at = pl.multiple_of(i * 16, 16)
        ready[pl.ds(ROWS + at, 16), :] = norm_rows(ctx[pl.ds(at, 16), :])

    @pl.loop(0, ROWS // 16)
    def _(i):
        at = pl.ds(pl.multiple_of(i * 16, 16), 16)
        ready[at, :] = norm_rows(lat[at, :])

    arrive("sp", lambda i: mod1.at[i], s["m1s"], s["m1r"])
    total = mod1[0]
    for i in range(1, NSP):
        total = total + mod1[i]
    mod2[tp] = total
    exchange("tp", lambda to: mod2.at[tp], lambda i: mod2.at[i], s["m2s"], s["m2r"])
    arrive("tp", lambda i: mod2.at[i], s["m2s"], s["m2r"])
    modv = s["modv"]
    for j in range(NTP):
        modv[:, j * 256 : (j + 1) * 256] = mod2[j]

    loaded("bias", "up", "post", "down", "key", "value", "query", "outgate", "out")

    def modulated(at, row):
        scaled = ready[at, :] * (1.0 + modv[2 + row : 3 + row, :])
        normed[at, :] = (scaled + modv[row : row + 1, :]).astype(BF16)

    @pl.loop(0, ROWS // 32)
    def _(i):
        modulated(pl.ds(pl.multiple_of(i * 32, 32), 32), 0)

    modulated(pl.ds(ROWS, CROWS), 1)

    ld, lcum, kk, vv = s["ld"], s["lcum"], s["kk"], s["vv"]

    def project(rows):
        low = dot_dims(normed[rows, :], s["wd"][...], 1, 1).astype(BF16)
        ld[rows, :] = log_decays(dot(low, s["up_w"][...]) + s["bias"][...])
        kk[rows, :] = dot(normed[rows, :], s["wk"][...]).astype(BF16)
        for i in range(2):
            at = slice(i * 512, (i + 1) * 512)
            vv[rows, at] = dot(normed[rows, :], s["wv"][:, at]).astype(BF16)

    own, ctx_rows = slice(0, ROWS), slice(ROWS, ALL)
    project(own)
    lcum[own, :] = sum_rows(tri[...], ld[own, :])

    ent, tots, kd = s["ent"], s["tots"], s["kd"]
    ctx_msg, seg_msg = s["ctx_msg"], s["seg_msg"]
    ctx_all, recv_a, grp_all, back, recv_c = (
        s["ctx_all"],
        s["recv_a"],
        s["grp_all"],
        s["back"],
        s["recv_c"],
    )
    lane_head = lax.rem(iota((64, 256), 1), 128) // 32
    closings = [lcum[n * T + T - 8 : n * T + T, :][7:8] for n in range(NB)]
    whole = closings[0] + closings[1] + closings[2] + closings[3]

    def own_lanes(full):
        state = jnp.zeros((64, 256), F32)
        for h in range(4):
            state = jnp.where(lane_head == h, full[h * 64 : (h + 1) * 64], state)
        return state

    for n in range(NB):
        tots[n : n + 1, :] = closings[n]
        rows = slice(n * T, (n + 1) * T)
        ahead = behind = jnp.zeros((1, 512), F32)
        for m in range(n):
            ahead = ahead + closings[m]
        for m in range(n + 1, NB):
            behind = behind + closings[m]
        cum = lcum[rows, :]
        keys = kk[rows, :].astype(F32)
        key_f = (keys * jnp.exp(closings[n] - cum + behind)).astype(BF16)
        key_b = (keys * jnp.exp(cum - ld[rows, :] + ahead)).astype(BF16)
        for g in range(NG):
            k_at = slice(g * 128, (g + 1) * 128)
            kd[rows, g * 256 : (g + 1) * 256] = jnp.concatenate(
                [key_f[:, k_at], key_b[:, k_at]], axis=1
            )
    for g in range(NG):
        v_at = slice(g * 256, (g + 1) * 256)
        state = own_lanes(dot_dims(vv[own, v_at], kd[:, v_at], 0, 0))
        for d in range(2):
            put_message(
                seg_msg,
                d * NG + g,
                state[:, d * 128 : (d + 1) * 128],
                whole[:, g * 128 : (g + 1) * 128],
            )
    recv_a[tp] = seg_msg[tp]
    exchange("tp", lambda to: seg_msg.at[to], lambda i: recv_a.at[i], s["as"], s["ar"])

    project(ctx_rows)
    lcum[ctx_rows, :] = sum_rows(tri[0:CROWS, 0:CROWS], ld[ctx_rows, :])
    summ = s["summ"]

    def summaries(rows, count, put):
        cum = lcum[rows, :]
        before = cum - ld[rows, :]
        closing = cum[count - 1 : count, :]
        keys = kk[rows, :].astype(F32)
        key_f = (keys * jnp.exp(closing - cum)).astype(BF16)
        key_b = (keys * jnp.exp(before)).astype(BF16)
        for g in range(NG):
            k_at = slice(g * 128, (g + 1) * 128)
            both = jnp.concatenate([key_f[:, k_at], key_b[:, k_at]], axis=1)
            put(g, own_lanes(dot_dims(vv[rows, g * 256 : (g + 1) * 256], both, 0, 0)))

    ctx_total = lcum[ALL - 8 : ALL, :][7:8]

    def put_context(g, state):
        for d in range(2):
            put_message(
                ctx_msg,
                d * NG + g,
                state[:, d * 128 : (d + 1) * 128],
                ctx_total[:, g * 128 : (g + 1) * 128],
            )

    summaries(ctx_rows, CROWS, put_context)
    ctx_all[sp] = ctx_msg[tp]
    exchange("sp", lambda to: ctx_all.at[sp], lambda i: ctx_all.at[i], s["cs"], s["cr"])

    qq, gg = s["qq"], s["gg"]
    qq[...] = dot(normed[0:ROWS, :], s["wq"][...]).astype(BF16)

    @pl.loop(0, NB)
    def _(n):
        def put(g, state):
            summ[n, :, g * 256 : (g + 1) * 256] = state

        summaries(pl.ds(pl.multiple_of(n * T, T), T), T, put)

    for g in range(NG):
        close = [jnp.exp(tots[n : n + 1, g * 128 : (g + 1) * 128]) for n in range(NB)]
        for d in range(2):
            at = slice(g * 256 + d * 128, g * 256 + (d + 1) * 128)
            run = jnp.zeros((64, 128), F32)
            for n in range(NB) if d == 0 else reversed(range(NB)):
                ent[n, :, at] = run.astype(BF16)
                run = close[n] * run + summ[n, :, at]

    flip = lax.div(tp, NTP // 2)
    arrive("tp", lambda i: recv_a.at[i], s["as"], s["ar"])
    pre_s, pre_c = s["pre_s"], s["pre_c"]
    run = jnp.zeros((64, 128), F32)
    run_log = jnp.zeros((1, 128), F32)
    for i in range(NTP):
        at = i + flip * (NTP - 1 - 2 * i)
        pre_s[at] = run
        pre_c[at] = jnp.broadcast_to(run_log, (8, 128))
        state, total = get_message(recv_a, at)
        run = jnp.exp(total) * run + state
        run_log = run_log + total
    put_message(grp_all, sp, run, run_log)
    exchange("sp", lambda to: grp_all.at[sp], lambda i: grp_all.at[i], s["gs"], s["gr"])


    @pl.loop(0, 2)
    def _(c):
        at = pl.ds(pl.multiple_of(c * 512, 512), 512)
        gg[:, at] = dot(normed[0:ROWS, :], s["wg"][:, at]).astype(BF16)

    mixed, qd = s["mixed"], s["qd"]
    t_row = iota((64, 256), 0)
    s_col = lax.rem(iota((64, 256), 1), 64)
    up_to, from_on = s_col <= t_row, s_col >= t_row

    def four(x, mask):
        return jnp.concatenate([x, x, x, x], axis=0) * mask

    @pl.loop(0, NB)
    def _(n):
        rows = pl.ds(pl.multiple_of(n * T, T), T)
        cum = lcum[rows, :]
        before = cum - ld[rows, :]
        middle, closing = cum[T // 2 - 1 : T // 2, :], cum[T - 1 : T, :]
        ahead = jnp.zeros((1, 512), F32)
        behind = jnp.zeros((1, 512), F32)
        for m in range(NB):
            ahead = ahead + jnp.where(m < n, tots[m : m + 1, :], 0.0)
            behind = behind + jnp.where(m > n, tots[m : m + 1, :], 0.0)
        q = qq[rows, :].astype(F32) * DK**-0.5
        k = kk[rows, :].astype(F32)
        qm_f = (q * jnp.exp(cum - middle)).astype(BF16)
        qm_b = (q * jnp.exp(middle - before)).astype(BF16)
        km_f = (k * jnp.exp(middle - cum)).astype(BF16)
        km_b = (k * jnp.exp(before - middle)).astype(BF16)
        qs_f = (q * jnp.exp(cum)).astype(BF16)
        qs_b = (q * jnp.exp(closing - before)).astype(BF16)
        qd_f = (q * jnp.exp(cum + ahead)).astype(BF16)
        qd_b = (q * jnp.exp(closing - before + behind)).astype(BF16)
        for g in range(NG):
            k_at = slice(g * 128, (g + 1) * 128)
            v_at = slice(g * 256, (g + 1) * 256)
            qd[rows, v_at] = jnp.concatenate([qd_f[:, k_at], qd_b[:, k_at]], axis=1)
            score_f = dot_dims(qm_f[:, k_at], four(km_f[:, k_at], head128[...]), 1, 1)
            score_b = dot_dims(qm_b[:, k_at], four(km_b[:, k_at], head128[...]), 1, 1)
            score = jnp.where(up_to, score_f, 0.0) + jnp.where(from_on, score_b, 0.0)
            within = dot(score.astype(BF16), four(vv[rows, v_at], head256[...]))
            entering = ent[n, :, v_at]
            states = jnp.concatenate(
                [
                    four(entering[:, 0:128], head128[...]),
                    four(entering[:, 128:256], head128[...]),
                ],
                axis=1,
            )
            across = dot_dims(
                jnp.concatenate([qs_f[:, k_at], qs_b[:, k_at]], axis=1), states, 1, 1
            )
            mixed[rows, v_at] = within + across

    arrive("sp", lambda i: ctx_all.at[i], s["cs"], s["cr"])
    reach = jnp.zeros((64, 128), F32)
    for i in range(NSP):
        state, total = get_message(ctx_all, i + flip * (NSP - 1 - 2 * i))
        reach = jnp.exp(total) * reach + state
    arrive("sp", lambda i: grp_all.at[i], s["gs"], s["gr"])
    rank = sp + flip * (NSP - 1 - 2 * sp)
    for i in range(NSP):
        state, total = get_message(grp_all, i + flip * (NSP - 1 - 2 * i))
        reach = jnp.where(i < rank, jnp.exp(total) * reach + state, reach)
    for j in range(NTP):
        back[j] = (pre_s[j] + jnp.exp(pre_c[j][0:1]) * reach).astype(BF16)
    recv_c[tp] = back[tp]
    exchange("tp", lambda to: back.at[to], lambda i: recv_c.at[i], s["bs"], s["br"])
    ones[...] = head256[...]
    silu = s["silu"]

    @pl.loop(0, ROWS // 32)
    def _(i):
        at = pl.ds(pl.multiple_of(i * 32, 32), 32)
        gate = gg[at, :].astype(F32)
        silu[at, :] = gate * lax.logistic(gate)

    weight = s["weight"]
    weight[...] = jnp.broadcast_to(modv[4:5, :] * s["post_gain"][...], (8, D))
    arrive("tp", lambda i: recv_c.at[i], s["bs"], s["br"])

    gated = s["gated"]
    for g in range(NG):
        v_at = slice(g * 256, (g + 1) * 256)
        states = jnp.concatenate(
            [four(recv_c[g], head128[...]), four(recv_c[NG + g], head128[...])], axis=1
        )
        values = mixed[:, v_at] + dot_dims(qd[:, v_at], states, 1, 1)
        square = values * values
        hi = square.astype(BF16)
        low = (square - hi.astype(F32)).astype(BF16)
        power = dot(hi, ones[...]) + dot(low, ones[...])
        normal = values * lax.rsqrt(power * (1.0 / DV) + EPS)
        gated[:, v_at] = (normal * silu[:, v_at]).astype(BF16)

    branch = s["branch"]
    squares = jnp.zeros((ROWS, 128), F32)
    for i in range(4):
        at = slice(i * 512, (i + 1) * 512)
        part = dot(gated[...], s["wo"][:, at]).astype(BF16)
        branch[:, at] = part
        part = part.astype(F32)
        part = part * part
        for j in range(4):
            squares = squares + part[:, j * 128 : (j + 1) * 128]
    mean = jnp.sum(squares, axis=-1, keepdims=True) * (1.0 / D)
    s["factor"][...] = jnp.broadcast_to(lax.rsqrt(mean + EPS), (ROWS, 128))

    @pl.loop(0, ROWS // 16)
    def _(i):
        at = pl.ds(pl.multiple_of(i * 16, 16), 16)
        factor = s["factor"][at, 0:1]
        added = branch[at, :].astype(F32) * factor * weight[0:1, :]
        out[at, :] = (lat[at, :].astype(F32) + added).astype(BF16)


    for copy in sends:
        copy.wait_send()


def scratch():
    vmem, sems = pltpu.VMEM, pltpu.SemaphoreType.DMA
    return dict(
        lat=vmem((ROWS, D), BF16),
        ctx=vmem((CROWS, D), BF16),
        wd=vmem((32, D), BF16),
        wk=vmem((D, 512), BF16),
        wv=vmem((D, 1024), BF16),
        wq=vmem((D, 512), BF16),
        wg=vmem((D, 1024), BF16),
        wo=vmem((1024, D), BF16),
        mod1=vmem((NSP, 8, 256), F32),
        mod2=vmem((NTP, 8, 256), F32),
        modv=vmem((8, D), F32),
        normed=vmem((ALL, D), BF16),
        head128=vmem((256, 128), BF16),
        head256=vmem((256, 256), BF16),
        ones=vmem((256, 256), BF16),
        tri=vmem((256, 256), BF16),
        ld=vmem((ALL, 512), F32),
        lcum=vmem((ALL, 512), F32),
        kk=vmem((ALL, 512), BF16),
        vv=vmem((ALL, 1024), BF16),
        qq=vmem((ROWS, 512), BF16),
        gg=vmem((ROWS, 1024), BF16),
        summ=vmem((NB, 64, 1024), F32),
        kd=vmem((ROWS, 1024), BF16),
        silu=vmem((ROWS, 1024), F32),
        ent=vmem((NB, 64, 1024), BF16),
        tots=vmem((8, 512), F32),
        ctx_msg=vmem((NTP, MSG, 128), BF16),
        seg_msg=vmem((NTP, MSG, 128), BF16),
        ctx_all=vmem((NSP, MSG, 128), BF16),
        grp_all=vmem((NSP, MSG, 128), BF16),
        recv_a=vmem((NTP, MSG, 128), BF16),
        pre_s=vmem((NTP, 64, 128), F32),
        pre_c=vmem((NTP, 8, 128), F32),
        back=vmem((NTP, 64, 128), BF16),
        recv_c=vmem((NTP, 64, 128), BF16),
        mixed=vmem((ROWS, 1024), F32),
        qd=vmem((ROWS, 1024), BF16),
        gated=vmem((ROWS, 1024), BF16),
        branch=vmem((ROWS, D), BF16),
        lat_cond=vmem((16, 128), BF16),
        ctx_cond=vmem((16, 128), BF16),
        shift_w=vmem((128, 256), BF16),
        scale_w=vmem((128, 256), BF16),
        gate_w=vmem((128, 256), BF16),
        gain=vmem((1, D), F32),
        bias=vmem((1, 512), F32),
        up_w=vmem((32, 512), BF16),
        post_gain=vmem((1, D), F32),
        ready=vmem((ALL, D), F32),
        factor=vmem((ROWS, 128), F32),
        weight=vmem((8, D), F32),
        load_sem=sems((17,)),
        m1s=sems((NSP - 1,)),
        m1r=sems((NSP - 1,)),
        m2s=sems((NTP - 1,)),
        m2r=sems((NTP - 1,)),
        cs=sems((NSP - 1,)),
        cr=sems((NSP - 1,)),
        gs=sems((NSP - 1,)),
        gr=sems((NSP - 1,)),
        bs=sems((NTP - 1,)),
        br=sems((NTP - 1,)),
        **{"as": sems((NTP - 1,)), "ar": sems((NTP - 1,))},
    )


def shards(
    latent,
    context,
    latent_condition,
    context_condition,
    shift_weight,
    scale_weight,
    gate_weight,
    norm_gain,
    query_weight,
    key_weight,
    value_weight,
    outgate_weight,
    down_weight,
    up_weight,
    decay_bias,
    out_weight,
    post_gain,
):
    hbm = pl.BlockSpec(memory_space=pl.ANY)
    return pl.pallas_call(
        kernel,
        out_shape=pltpu.VMEM((ROWS, D), BF16),
        in_specs=[hbm] * 17,
        out_specs=pl.BlockSpec(memory_space=pltpu.VMEM),
        scratch_shapes=[scratch()],
        compiler_params=pltpu.CompilerParams(
            collective_id=0, has_side_effects=True, vmem_limit_bytes=60 * 1024 * 1024
        ),
    )(
        latent,
        context,
        latent_condition.reshape(16, 128),
        context_condition.reshape(16, 128),
        shift_weight,
        scale_weight,
        gate_weight,
        norm_gain[None],
        query_weight,
        key_weight,
        value_weight,
        outgate_weight,
        down_weight.T,
        up_weight,
        decay_bias[None],
        out_weight,
        post_gain[None],
    )


def solution(mesh):
    tokens = P(("sp", "tp"), None)
    maps = P("sp", "tp")
    placed = (tokens, P("sp", None), P(), P(), maps, maps, maps) + (P(),) * 10
    return jax.shard_map(
        shards, mesh=mesh, in_specs=placed, out_specs=tokens, check_vma=False
    )
```

```python
import jax
import jax.numpy as jnp
from jax import lax
from jax.experimental import pallas as pl
from jax.experimental.pallas import tpu as pltpu
from jax.sharding import PartitionSpec as P

F32 = jnp.float32
BF16 = jnp.bfloat16
MESH = pl.DeviceIdType.MESH
EPS = 1e-06

NSP = 16
NTP = 8
D = 2048
HEADS = 16
DK = 32
DV = 64
ROWS = 256
CROWS = 32
ALL = ROWS + CROWS
T = 64
NB = ROWS // T
NG = 4
MSG = 80


def far_first(lengths):
    steps = [(a, b) for a in range(lengths[0]) for b in range(lengths[1]) if (a, b) != (0, 0)]
    hops = [0, 1, 2, 1]
    weight = 2 if lengths[1] == 2 else 1
    return sorted(steps, key=lambda t: -(weight * hops[t[0]] + hops[t[1]]))


SP_STEPS = far_first((4, 4))
TP_STEPS = far_first((4, 2))


def dot(a, b):
    return jnp.dot(a, b, preferred_element_type=F32)


def dot_dims(a, b, ca, cb):
    return lax.dot_general(a, b, (((ca,), (cb,)), ((), ())), preferred_element_type=F32)


def iota(shape, dim):
    return lax.broadcasted_iota(jnp.int32, shape, dim)


def split3(x):
    hi = x.astype(BF16)
    rest = x - hi.astype(F32)
    mid = rest.astype(BF16)
    return hi, mid, (rest - mid.astype(F32)).astype(BF16)


def sum_rows(tri, x):
    hi, mid, lo = split3(x)
    return dot(tri, hi) + dot(tri, mid) + dot(tri, lo)


def log_decays(pre):
    return (jnp.minimum(pre, 0.0) - jnp.log1p(jnp.exp(-jnp.abs(pre)))) * (1.0 / 16.0)


def put_message(ref, at, state, total):
    hi, mid, lo = split3(total)
    row = iota((16, 128), 0)
    tail = jnp.where(
        row == 0,
        hi.astype(F32),
        jnp.where(row == 1, mid.astype(F32), jnp.where(row == 2, lo.astype(F32), 0.0)),
    )
    ref[at, 0:64, :] = state.astype(BF16)
    ref[at, 64:MSG, :] = tail.astype(BF16)


def get_message(ref, at):
    state = ref[at, 0:64, :].astype(F32)
    tail = ref[at, 64:MSG, :].astype(F32)
    return state, tail[0:1] + tail[1:2] + tail[2:3]


def kernel(
    latent,
    context,
    lat_cond,
    ctx_cond,
    shift_w,
    scale_w,
    gate_w,
    gain,
    query_w,
    key_w,
    value_w,
    outgate_w,
    down_w,
    up_w,
    bias,
    out_w,
    post_gain,
    out,
    s,
):
    sp = lax.axis_index("sp")
    tp = lax.axis_index("tp")

    z, x = lax.div(sp, 4), lax.rem(sp, 4)
    y, c = lax.div(tp, 2), lax.rem(tp, 2)

    def sp_peer(step):
        return lax.rem(z + step[0], 4) * 4 + lax.rem(x + step[1], 4)

    def tp_peer(step):
        return lax.rem(y + step[0], 4) * 2 + lax.rem(c + step[1], 2)

    barrier = pltpu.get_barrier_semaphore()
    for step in SP_STEPS:
        pl.semaphore_signal(barrier, inc=1, device_id=(sp_peer(step), tp), device_id_type=MESH)
    for step in TP_STEPS:
        pl.semaphore_signal(barrier, inc=1, device_id=(sp, tp_peer(step)), device_id_type=MESH)

    pairs = dict(
        lat_cond=(lat_cond, s["lat_cond"]),
        ctx_cond=(ctx_cond, s["ctx_cond"]),
        shift=(shift_w, s["shift_w"]),
        scale=(scale_w, s["scale_w"]),
        gate=(gate_w, s["gate_w"]),
        latent=(latent, s["lat"]),
        context=(context, s["ctx"]),
        gain=(gain, s["gain"]),
        bias=(bias, s["bias"]),
        up=(up_w, s["up_w"]),
        post=(post_gain, s["post_gain"]),
        down=(down_w, s["wd"]),
        key=(key_w, s["wk"]),
        value=(value_w, s["wv"]),
        query=(query_w, s["wq"]),
        outgate=(outgate_w, s["wg"]),
        out=(out_w, s["wo"]),
    )
    loads = {
        name: pltpu.make_async_copy(src, dst, s["load_sem"].at[i])
        for i, (name, (src, dst)) in enumerate(pairs.items())
    }
    for name in loads:
        loads[name].start()

    def loaded(*names):
        for name in names:
            loads[name].wait()

    sends = []

    flip = lax.div(tp, NTP // 2)

    def exchange(axis, src, dst, send_sem, recv_sem, ordered=False):
        steps, peer = (SP_STEPS, sp_peer) if axis == "sp" else (TP_STEPS, tp_peer)
        for d, step in enumerate(steps):
            to = peer(step)
            copy = pltpu.make_async_remote_copy(
                src_ref=src(to),
                dst_ref=dst(sp if axis == "sp" else tp),
                send_sem=send_sem.at[d],
                recv_sem=recv_sem.at[d],
                device_id=(to, tp) if axis == "sp" else (sp, to),
                device_id_type=MESH,
            )
            later = (to - sp) * (1 - 2 * flip) > 0 if ordered else None
            if ordered:
                pl.when(later)(copy.start)
            else:
                copy.start()
            sends.append((copy, later))

    def arrive(axis, dst, send_sem, recv_sem, ordered=False):
        steps, wrap, peer = (
            (SP_STEPS, (4, 4), sp_peer) if axis == "sp" else (TP_STEPS, (4, 2), tp_peer)
        )
        for d, step in reversed(list(enumerate(steps))):
            origin = peer((wrap[0] - step[0], wrap[1] - step[1]))
            copy = pltpu.make_async_remote_copy(
                src_ref=dst(origin),
                dst_ref=dst(origin),
                send_sem=send_sem.at[d],
                recv_sem=recv_sem.at[d],
                device_id=(origin, tp) if axis == "sp" else (sp, origin),
                device_id_type=MESH,
            )
            if ordered:
                pl.when((sp - origin) * (1 - 2 * flip) > 0)(copy.wait_recv)
            else:
                copy.wait_recv()

    loaded("lat_cond", "ctx_cond", "shift", "scale", "gate")
    row16 = iota((16, 128), 0)

    def cond_row(name):
        mine = jnp.where(row16 == sp, s[name][...].astype(F32), 0.0)
        return jnp.broadcast_to(jnp.sum(mine, axis=0, keepdims=True), (16, 128))

    cond = jnp.where(lax.rem(row16, 2) == 0, cond_row("lat_cond"), cond_row("ctx_cond"))
    act = (cond * lax.logistic(cond)).astype(BF16)
    row8 = iota((8, 256), 0)
    part = jnp.where(
        row8 < 2,
        dot(act, s["shift_w"][...])[0:8],
        jnp.where(row8 < 4, dot(act, s["scale_w"][...])[0:8], dot(act, s["gate_w"][...])[0:8]),
    )
    mod1, mod2 = s["mod1"], s["mod2"]
    mod1[sp] = part
    pl.semaphore_wait(barrier, NSP + NTP - 2)
    exchange("sp", lambda to: mod1.at[sp], lambda i: mod1.at[i], s["m1s"], s["m1r"])

    head128, head256, tri, ones = s["head128"], s["head256"], s["tri"], s["ones"]

    def as_bf16(cond):
        return jnp.where(cond, 1.0, 0.0).astype(BF16)

    head128[...] = as_bf16(iota((256, 128), 0) // 64 == iota((256, 128), 1) // 32)
    head256[...] = as_bf16(iota((256, 256), 0) // 64 == iota((256, 256), 1) // 64)
    r256, c256 = iota((256, 256), 0), iota((256, 256), 1)
    tri[...] = as_bf16((r256 // T == c256 // T) & (c256 <= r256))

    lat, ctx, normed, ready = s["lat"], s["ctx"], s["normed"], s["ready"]
    gain_row = s["gain"]

    def norm_rows(x):
        x = x.astype(F32)
        factor = lax.rsqrt(jnp.mean(x * x, axis=-1, keepdims=True) + EPS)
        return x * factor * gain_row[...]

    loaded("latent", "context", "gain")

    @pl.loop(0, CROWS // 16)
    def _(i):
        at = pl.multiple_of(i * 16, 16)
        ready[pl.ds(ROWS + at, 16), :] = norm_rows(ctx[pl.ds(at, 16), :])

    @pl.loop(0, ROWS // 16)
    def _(i):
        at = pl.ds(pl.multiple_of(i * 16, 16), 16)
        ready[at, :] = norm_rows(lat[at, :])

    arrive("sp", lambda i: mod1.at[i], s["m1s"], s["m1r"])
    total = mod1[0]
    for i in range(1, NSP):
        total = total + mod1[i]
    mod2[tp] = total
    exchange("tp", lambda to: mod2.at[tp], lambda i: mod2.at[i], s["m2s"], s["m2r"])
    arrive("tp", lambda i: mod2.at[i], s["m2s"], s["m2r"])
    modv = s["modv"]
    for j in range(NTP):
        modv[:, j * 256 : (j + 1) * 256] = mod2[j]

    loaded("bias", "up", "post", "down", "key", "value", "query", "outgate", "out")

    def modulated(at, row):
        scaled = ready[at, :] * (1.0 + modv[2 + row : 3 + row, :])
        normed[at, :] = (scaled + modv[row : row + 1, :]).astype(BF16)

    @pl.loop(0, ROWS // 32)
    def _(i):
        modulated(pl.ds(pl.multiple_of(i * 32, 32), 32), 0)

    modulated(pl.ds(ROWS, CROWS), 1)

    ld, lcum, kk, vv = s["ld"], s["lcum"], s["kk"], s["vv"]

    def project(rows):
        low = dot_dims(normed[rows, :], s["wd"][...], 1, 1).astype(BF16)
        ld[rows, :] = log_decays(dot(low, s["up_w"][...]) + s["bias"][...])
        kk[rows, :] = dot(normed[rows, :], s["wk"][...]).astype(BF16)
        for i in range(2):
            at = slice(i * 512, (i + 1) * 512)
            vv[rows, at] = dot(normed[rows, :], s["wv"][:, at]).astype(BF16)

    own, ctx_rows = slice(0, ROWS), slice(ROWS, ALL)
    low = dot_dims(normed[own, :], s["wd"][...], 1, 1).astype(BF16)
    kk[own, :] = dot(normed[own, :], s["wk"][...]).astype(BF16)
    ld[own, :] = log_decays(dot(low, s["up_w"][...]) + s["bias"][...])
    vv[own, 0:512] = dot(normed[own, :], s["wv"][:, 0:512]).astype(BF16)
    lcum[own, :] = sum_rows(tri[...], ld[own, :])
    vv[own, 512:1024] = dot(normed[own, :], s["wv"][:, 512:1024]).astype(BF16)

    ent, tots, kd = s["ent"], s["tots"], s["kd"]
    ctx_msg, seg_msg = s["ctx_msg"], s["seg_msg"]
    ctx_all, recv_a, grp_all, back, recv_c = (
        s["ctx_all"],
        s["recv_a"],
        s["grp_all"],
        s["back"],
        s["recv_c"],
    )
    lane_head = lax.rem(iota((64, 256), 1), 128) // 32
    closings = [lcum[n * T + T - 8 : n * T + T, :][7:8] for n in range(NB)]
    whole = closings[0] + closings[1] + closings[2] + closings[3]

    def own_lanes(full):
        state = jnp.zeros((64, 256), F32)
        for h in range(4):
            state = jnp.where(lane_head == h, full[h * 64 : (h + 1) * 64], state)
        return state

    for n in range(NB):
        tots[n : n + 1, :] = closings[n]
        rows = slice(n * T, (n + 1) * T)
        ahead = behind = jnp.zeros((1, 512), F32)
        for m in range(n):
            ahead = ahead + closings[m]
        for m in range(n + 1, NB):
            behind = behind + closings[m]
        cum = lcum[rows, :]
        keys = kk[rows, :].astype(F32)
        key_f = (keys * jnp.exp(closings[n] - cum + behind)).astype(BF16)
        key_b = (keys * jnp.exp(cum - ld[rows, :] + ahead)).astype(BF16)
        for g in range(NG):
            k_at = slice(g * 128, (g + 1) * 128)
            kd[rows, g * 256 : (g + 1) * 256] = jnp.concatenate(
                [key_f[:, k_at], key_b[:, k_at]], axis=1
            )
    for g in range(NG):
        v_at = slice(g * 256, (g + 1) * 256)
        state = own_lanes(dot_dims(vv[own, v_at], kd[:, v_at], 0, 0))
        for d in range(2):
            put_message(
                seg_msg,
                d * NG + g,
                state[:, d * 128 : (d + 1) * 128],
                whole[:, g * 128 : (g + 1) * 128],
            )
    recv_a[tp] = seg_msg[tp]
    exchange("tp", lambda to: seg_msg.at[to], lambda i: recv_a.at[i], s["as"], s["ar"])

    project(ctx_rows)
    lcum[ctx_rows, :] = sum_rows(tri[0:CROWS, 0:CROWS], ld[ctx_rows, :])
    summ = s["summ"]

    def summaries(rows, count, put):
        cum = lcum[rows, :]
        before = cum - ld[rows, :]
        closing = cum[count - 1 : count, :]
        keys = kk[rows, :].astype(F32)
        key_f = (keys * jnp.exp(closing - cum)).astype(BF16)
        key_b = (keys * jnp.exp(before)).astype(BF16)
        for g in range(NG):
            k_at = slice(g * 128, (g + 1) * 128)
            both = jnp.concatenate([key_f[:, k_at], key_b[:, k_at]], axis=1)
            put(g, own_lanes(dot_dims(vv[rows, g * 256 : (g + 1) * 256], both, 0, 0)))

    ctx_total = lcum[ALL - 8 : ALL, :][7:8]

    def put_context(g, state):
        for d in range(2):
            put_message(
                ctx_msg,
                d * NG + g,
                state[:, d * 128 : (d + 1) * 128],
                ctx_total[:, g * 128 : (g + 1) * 128],
            )

    summaries(ctx_rows, CROWS, put_context)
    ctx_all[sp] = ctx_msg[tp]
    exchange("sp", lambda to: ctx_all.at[sp], lambda i: ctx_all.at[i], s["cs"], s["cr"])

    qq, gg = s["qq"], s["gg"]
    qq[...] = dot(normed[0:ROWS, :], s["wq"][...]).astype(BF16)

    @pl.loop(0, NB)
    def _(n):
        def put(g, state):
            summ[n, :, g * 256 : (g + 1) * 256] = state

        summaries(pl.ds(pl.multiple_of(n * T, T), T), T, put)

    for g in range(NG):
        close = [jnp.exp(tots[n : n + 1, g * 128 : (g + 1) * 128]) for n in range(NB)]
        for d in range(2):
            at = slice(g * 256 + d * 128, g * 256 + (d + 1) * 128)
            run = jnp.zeros((64, 128), F32)
            for n in range(NB) if d == 0 else reversed(range(NB)):
                ent[n, :, at] = run.astype(BF16)
                run = close[n] * run + summ[n, :, at]

    arrive("tp", lambda i: recv_a.at[i], s["as"], s["ar"])
    pre_s, pre_c = s["pre_s"], s["pre_c"]
    run = jnp.zeros((64, 128), F32)
    run_log = jnp.zeros((1, 128), F32)
    for i in range(NTP):
        at = i + flip * (NTP - 1 - 2 * i)
        pre_s[at] = run
        pre_c[at] = jnp.broadcast_to(run_log, (8, 128))
        state, total = get_message(recv_a, at)
        run = jnp.exp(total) * run + state
        run_log = run_log + total
    put_message(grp_all, sp, run, run_log)
    exchange("sp", lambda to: grp_all.at[sp], lambda i: grp_all.at[i], s["gs"], s["gr"], True)


    @pl.loop(0, 2)
    def _(c):
        at = pl.ds(pl.multiple_of(c * 512, 512), 512)
        gg[:, at] = dot(normed[0:ROWS, :], s["wg"][:, at]).astype(BF16)

    mixed, qd = s["mixed"], s["qd"]
    t_row = iota((64, 256), 0)
    s_col = lax.rem(iota((64, 256), 1), 64)
    up_to, from_on = s_col <= t_row, s_col >= t_row

    def four(x, mask):
        return jnp.concatenate([x, x, x, x], axis=0) * mask

    @pl.loop(0, NB)
    def _(n):
        rows = pl.ds(pl.multiple_of(n * T, T), T)
        cum = lcum[rows, :]
        before = cum - ld[rows, :]
        middle, closing = cum[T // 2 - 1 : T // 2, :], cum[T - 1 : T, :]
        ahead = jnp.zeros((1, 512), F32)
        behind = jnp.zeros((1, 512), F32)
        for m in range(NB):
            ahead = ahead + jnp.where(m < n, tots[m : m + 1, :], 0.0)
            behind = behind + jnp.where(m > n, tots[m : m + 1, :], 0.0)
        q = qq[rows, :].astype(F32) * DK**-0.5
        k = kk[rows, :].astype(F32)
        qm_f = (q * jnp.exp(cum - middle)).astype(BF16)
        qm_b = (q * jnp.exp(middle - before)).astype(BF16)
        km_f = (k * jnp.exp(middle - cum)).astype(BF16)
        km_b = (k * jnp.exp(before - middle)).astype(BF16)
        qs_f = (q * jnp.exp(cum)).astype(BF16)
        qs_b = (q * jnp.exp(closing - before)).astype(BF16)
        qd_f = (q * jnp.exp(cum + ahead)).astype(BF16)
        qd_b = (q * jnp.exp(closing - before + behind)).astype(BF16)
        for g in range(NG):
            k_at = slice(g * 128, (g + 1) * 128)
            v_at = slice(g * 256, (g + 1) * 256)
            qd[rows, v_at] = jnp.concatenate([qd_f[:, k_at], qd_b[:, k_at]], axis=1)
            score_f = dot_dims(qm_f[:, k_at], four(km_f[:, k_at], head128[...]), 1, 1)
            score_b = dot_dims(qm_b[:, k_at], four(km_b[:, k_at], head128[...]), 1, 1)
            score = jnp.where(up_to, score_f, 0.0) + jnp.where(from_on, score_b, 0.0)
            within = dot(score.astype(BF16), four(vv[rows, v_at], head256[...]))
            entering = ent[n, :, v_at]
            states = jnp.concatenate(
                [
                    four(entering[:, 0:128], head128[...]),
                    four(entering[:, 128:256], head128[...]),
                ],
                axis=1,
            )
            across = dot_dims(
                jnp.concatenate([qs_f[:, k_at], qs_b[:, k_at]], axis=1), states, 1, 1
            )
            mixed[rows, v_at] = within + across

    arrive("sp", lambda i: ctx_all.at[i], s["cs"], s["cr"])
    reach = jnp.zeros((64, 128), F32)
    for i in range(NSP):
        state, total = get_message(ctx_all, i + flip * (NSP - 1 - 2 * i))
        reach = jnp.exp(total) * reach + state
    arrive("sp", lambda i: grp_all.at[i], s["gs"], s["gr"], True)
    rank = sp + flip * (NSP - 1 - 2 * sp)
    for i in range(NSP):
        state, total = get_message(grp_all, i + flip * (NSP - 1 - 2 * i))
        reach = jnp.where(i < rank, jnp.exp(total) * reach + state, reach)
    for j in range(NTP):
        back[j] = (pre_s[j] + jnp.exp(pre_c[j][0:1]) * reach).astype(BF16)
    recv_c[tp] = back[tp]
    exchange("tp", lambda to: back.at[to], lambda i: recv_c.at[i], s["bs"], s["br"])
    ones[...] = head256[...]
    silu = s["silu"]

    @pl.loop(0, ROWS // 32)
    def _(i):
        at = pl.ds(pl.multiple_of(i * 32, 32), 32)
        gate = gg[at, :].astype(F32)
        silu[at, :] = gate * lax.logistic(gate)

    weight = s["weight"]
    weight[...] = jnp.broadcast_to(modv[4:5, :] * s["post_gain"][...], (8, D))
    arrive("tp", lambda i: recv_c.at[i], s["bs"], s["br"])

    gated = s["gated"]
    for g in range(NG):
        v_at = slice(g * 256, (g + 1) * 256)
        states = jnp.concatenate(
            [four(recv_c[g], head128[...]), four(recv_c[NG + g], head128[...])], axis=1
        )
        values = mixed[:, v_at] + dot_dims(qd[:, v_at], states, 1, 1)
        square = values * values
        hi = square.astype(BF16)
        low = (square - hi.astype(F32)).astype(BF16)
        power = dot(hi, ones[...]) + dot(low, ones[...])
        normal = values * lax.rsqrt(power * (1.0 / DV) + EPS)
        gated[:, v_at] = (normal * silu[:, v_at]).astype(BF16)

    branch = s["branch"]
    for half in range(1):
        rows = slice(half * 256, (half + 1) * 256)
        squares = jnp.zeros((256, 128), F32)
        for i in range(8):
            at = slice(i * 256, (i + 1) * 256)
            part = dot(gated[rows, :], s["wo"][:, at]).astype(BF16)
            branch[rows, at] = part
            part = part.astype(F32)
            part = part * part
            for j in range(2):
                squares = squares + part[:, j * 128 : (j + 1) * 128]
        mean = jnp.sum(squares, axis=-1, keepdims=True) * (1.0 / D)
        factors = lax.rsqrt(mean + EPS)
        for k in range(16):
            at = slice(half * 256 + k * 16, half * 256 + (k + 1) * 16)
            added = branch[at, :].astype(F32) * factors[k * 16 : (k + 1) * 16] * weight[0:1, :]
            out[at, :] = (lat[at, :].astype(F32) + added).astype(BF16)

    for copy, later in sends:
        if later is None:
            copy.wait_send()
        else:
            pl.when(later)(copy.wait_send)


def scratch():
    vmem, sems = pltpu.VMEM, pltpu.SemaphoreType.DMA
    return dict(
        lat=vmem((ROWS, D), BF16),
        ctx=vmem((CROWS, D), BF16),
        wd=vmem((32, D), BF16),
        wk=vmem((D, 512), BF16),
        wv=vmem((D, 1024), BF16),
        wq=vmem((D, 512), BF16),
        wg=vmem((D, 1024), BF16),
        wo=vmem((1024, D), BF16),
        mod1=vmem((NSP, 8, 256), F32),
        mod2=vmem((NTP, 8, 256), F32),
        modv=vmem((8, D), F32),
        normed=vmem((ALL, D), BF16),
        head128=vmem((256, 128), BF16),
        head256=vmem((256, 256), BF16),
        ones=vmem((256, 256), BF16),
        tri=vmem((256, 256), BF16),
        ld=vmem((ALL, 512), F32),
        lcum=vmem((ALL, 512), F32),
        kk=vmem((ALL, 512), BF16),
        vv=vmem((ALL, 1024), BF16),
        qq=vmem((ROWS, 512), BF16),
        gg=vmem((ROWS, 1024), BF16),
        summ=vmem((NB, 64, 1024), F32),
        kd=vmem((ROWS, 1024), BF16),
        silu=vmem((ROWS, 1024), F32),
        ent=vmem((NB, 64, 1024), BF16),
        tots=vmem((8, 512), F32),
        ctx_msg=vmem((NTP, MSG, 128), BF16),
        seg_msg=vmem((NTP, MSG, 128), BF16),
        ctx_all=vmem((NSP, MSG, 128), BF16),
        grp_all=vmem((NSP, MSG, 128), BF16),
        recv_a=vmem((NTP, MSG, 128), BF16),
        pre_s=vmem((NTP, 64, 128), F32),
        pre_c=vmem((NTP, 8, 128), F32),
        back=vmem((NTP, 64, 128), BF16),
        recv_c=vmem((NTP, 64, 128), BF16),
        mixed=vmem((ROWS, 1024), F32),
        qd=vmem((ROWS, 1024), BF16),
        gated=vmem((ROWS, 1024), BF16),
        branch=vmem((ROWS, D), BF16),
        lat_cond=vmem((16, 128), BF16),
        ctx_cond=vmem((16, 128), BF16),
        shift_w=vmem((128, 256), BF16),
        scale_w=vmem((128, 256), BF16),
        gate_w=vmem((128, 256), BF16),
        gain=vmem((1, D), F32),
        bias=vmem((1, 512), F32),
        up_w=vmem((32, 512), BF16),
        post_gain=vmem((1, D), F32),
        ready=vmem((ALL, D), F32),
        factor=vmem((ROWS, 128), F32),
        weight=vmem((8, D), F32),
        load_sem=sems((17,)),
        m1s=sems((NSP - 1,)),
        m1r=sems((NSP - 1,)),
        m2s=sems((NTP - 1,)),
        m2r=sems((NTP - 1,)),
        cs=sems((NSP - 1,)),
        cr=sems((NSP - 1,)),
        gs=sems((NSP - 1,)),
        gr=sems((NSP - 1,)),
        bs=sems((NTP - 1,)),
        br=sems((NTP - 1,)),
        **{"as": sems((NTP - 1,)), "ar": sems((NTP - 1,))},
    )


def shards(
    latent,
    context,
    latent_condition,
    context_condition,
    shift_weight,
    scale_weight,
    gate_weight,
    norm_gain,
    query_weight,
    key_weight,
    value_weight,
    outgate_weight,
    down_weight,
    up_weight,
    decay_bias,
    out_weight,
    post_gain,
):
    hbm = pl.BlockSpec(memory_space=pl.ANY)
    return pl.pallas_call(
        kernel,
        out_shape=pltpu.VMEM((ROWS, D), BF16),
        in_specs=[hbm] * 17,
        out_specs=pl.BlockSpec(memory_space=pltpu.VMEM),
        scratch_shapes=[scratch()],
        compiler_params=pltpu.CompilerParams(
            collective_id=0, has_side_effects=True, vmem_limit_bytes=60 * 1024 * 1024
        ),
    )(
        latent,
        context,
        latent_condition.reshape(16, 128),
        context_condition.reshape(16, 128),
        shift_weight,
        scale_weight,
        gate_weight,
        norm_gain[None],
        query_weight,
        key_weight,
        value_weight,
        outgate_weight,
        down_weight.T,
        up_weight,
        decay_bias[None],
        out_weight,
        post_gain[None],
    )


def solution(mesh):
    tokens = P(("sp", "tp"), None)
    maps = P("sp", "tp")
    placed = (tokens, P("sp", None), P(), P(), maps, maps, maps) + (P(),) * 10
    return jax.shard_map(
        shards, mesh=mesh, in_specs=placed, out_specs=tokens, check_vma=False
    )
```

```python
import jax
import jax.numpy as jnp
from jax import lax
from jax.experimental import pallas as pl
from jax.experimental.pallas import tpu as pltpu
from jax.sharding import PartitionSpec as P

F32 = jnp.float32
BF16 = jnp.bfloat16
MESH = pl.DeviceIdType.MESH
EPS = 1e-06

NSP = 16
NTP = 8
D = 2048
HEADS = 16
DK = 32
DV = 64
ROWS = 256
CROWS = 32
ALL = ROWS + CROWS
T = 64
NB = ROWS // T
NG = 4
MSG = 80


def far_first(lengths):
    steps = [(a, b) for a in range(lengths[0]) for b in range(lengths[1]) if (a, b) != (0, 0)]
    hops = [0, 1, 2, 1]
    weight = 2 if lengths[1] == 2 else 1
    return sorted(steps, key=lambda t: -(weight * hops[t[0]] + hops[t[1]]))


SP_STEPS = far_first((4, 4))
TP_STEPS = far_first((4, 2))


def dot(a, b):
    return jnp.dot(a, b, preferred_element_type=F32)


def dot_dims(a, b, ca, cb):
    return lax.dot_general(a, b, (((ca,), (cb,)), ((), ())), preferred_element_type=F32)


def iota(shape, dim):
    return lax.broadcasted_iota(jnp.int32, shape, dim)


def split3(x):
    hi = x.astype(BF16)
    rest = x - hi.astype(F32)
    mid = rest.astype(BF16)
    return hi, mid, (rest - mid.astype(F32)).astype(BF16)


def sum_rows(tri, x):
    hi, mid, lo = split3(x)
    return dot(tri, hi) + dot(tri, mid) + dot(tri, lo)


def log_decays(pre):
    return (jnp.minimum(pre, 0.0) - jnp.log1p(jnp.exp(-jnp.abs(pre)))) * (1.0 / 16.0)


def put_message(ref, at, state, total):
    hi, mid, lo = split3(total)
    row = iota((16, 128), 0)
    tail = jnp.where(
        row == 0,
        hi.astype(F32),
        jnp.where(row == 1, mid.astype(F32), jnp.where(row == 2, lo.astype(F32), 0.0)),
    )
    ref[at, 0:64, :] = state.astype(BF16)
    ref[at, 64:MSG, :] = tail.astype(BF16)


def get_message(ref, at):
    state = ref[at, 0:64, :].astype(F32)
    tail = ref[at, 64:MSG, :].astype(F32)
    return state, tail[0:1] + tail[1:2] + tail[2:3]


def kernel(
    latent,
    context,
    lat_cond,
    ctx_cond,
    shift_w,
    scale_w,
    gate_w,
    gain,
    query_w,
    key_w,
    value_w,
    outgate_w,
    down_w,
    up_w,
    bias,
    out_w,
    post_gain,
    out,
    s,
):
    sp = lax.axis_index("sp")
    tp = lax.axis_index("tp")

    z, x = lax.div(sp, 4), lax.rem(sp, 4)
    y, c = lax.div(tp, 2), lax.rem(tp, 2)

    def sp_peer(step):
        return lax.rem(z + step[0], 4) * 4 + lax.rem(x + step[1], 4)

    def tp_peer(step):
        return lax.rem(y + step[0], 4) * 2 + lax.rem(c + step[1], 2)

    barrier = pltpu.get_barrier_semaphore()
    for step in SP_STEPS:
        pl.semaphore_signal(barrier, inc=1, device_id=(sp_peer(step), tp), device_id_type=MESH)
    for step in TP_STEPS:
        pl.semaphore_signal(barrier, inc=1, device_id=(sp, tp_peer(step)), device_id_type=MESH)

    pairs = dict(
        lat_cond=(lat_cond, s["lat_cond"]),
        ctx_cond=(ctx_cond, s["ctx_cond"]),
        shift=(shift_w, s["shift_w"]),
        scale=(scale_w, s["scale_w"]),
        gate=(gate_w, s["gate_w"]),
        latent=(latent, s["lat"]),
        context=(context, s["ctx"]),
        gain=(gain, s["gain"]),
        bias=(bias, s["bias"]),
        up=(up_w, s["up_w"]),
        post=(post_gain, s["post_gain"]),
        down=(down_w, s["wd"]),
        key=(key_w, s["wk"]),
        value=(value_w, s["wv"]),
        query=(query_w, s["wq"]),
        outgate=(outgate_w, s["wg"]),
        out=(out_w, s["wo"]),
    )
    loads = {
        name: pltpu.make_async_copy(src, dst, s["load_sem"].at[i])
        for i, (name, (src, dst)) in enumerate(pairs.items())
    }
    for name in loads:
        loads[name].start()

    def loaded(*names):
        for name in names:
            loads[name].wait()

    sends = []

    flip = lax.div(tp, NTP // 2)

    def exchange(axis, src, dst, send_sem, recv_sem, ordered=False):
        steps, peer = (SP_STEPS, sp_peer) if axis == "sp" else (TP_STEPS, tp_peer)
        for d, step in enumerate(steps):
            to = peer(step)
            copy = pltpu.make_async_remote_copy(
                src_ref=src(to),
                dst_ref=dst(sp if axis == "sp" else tp),
                send_sem=send_sem.at[d],
                recv_sem=recv_sem.at[d],
                device_id=(to, tp) if axis == "sp" else (sp, to),
                device_id_type=MESH,
            )
            later = (to - sp) * (1 - 2 * flip) > 0 if ordered else None
            if ordered:
                pl.when(later)(copy.start)
            else:
                copy.start()
            sends.append((copy, later))

    def arrive(axis, dst, send_sem, recv_sem, ordered=False, only=None):
        steps, wrap, peer = (
            (SP_STEPS, (4, 4), sp_peer) if axis == "sp" else (TP_STEPS, (4, 2), tp_peer)
        )
        for d, step in reversed(list(enumerate(steps))):
            if only is not None and step != only:
                continue
            origin = peer((wrap[0] - step[0], wrap[1] - step[1]))
            copy = pltpu.make_async_remote_copy(
                src_ref=dst(origin),
                dst_ref=dst(origin),
                send_sem=send_sem.at[d],
                recv_sem=recv_sem.at[d],
                device_id=(origin, tp) if axis == "sp" else (sp, origin),
                device_id_type=MESH,
            )
            if ordered:
                pl.when((sp - origin) * (1 - 2 * flip) > 0)(copy.wait_recv)
            else:
                copy.wait_recv()

    loaded("lat_cond", "ctx_cond", "shift", "scale", "gate")
    row16 = iota((16, 128), 0)

    def cond_row(name):
        mine = jnp.where(row16 == sp, s[name][...].astype(F32), 0.0)
        return jnp.broadcast_to(jnp.sum(mine, axis=0, keepdims=True), (16, 128))

    cond = jnp.where(lax.rem(row16, 2) == 0, cond_row("lat_cond"), cond_row("ctx_cond"))
    act = (cond * lax.logistic(cond)).astype(BF16)
    row8 = iota((8, 256), 0)
    part = jnp.where(
        row8 < 2,
        dot(act, s["shift_w"][...])[0:8],
        jnp.where(row8 < 4, dot(act, s["scale_w"][...])[0:8], dot(act, s["gate_w"][...])[0:8]),
    )
    mod1, mod2 = s["mod1"], s["mod2"]
    mod1[sp, 0:5, :] = part[0:5, 0:128]
    mod1[sp, 5:10, :] = part[0:5, 128:256]
    pl.semaphore_wait(barrier, NSP + NTP - 2)
    exchange("sp", lambda to: mod1.at[sp], lambda i: mod1.at[i], s["m1s"], s["m1r"])

    head128, head256, tri, ones = s["head128"], s["head256"], s["tri"], s["ones"]

    def as_bf16(cond):
        return jnp.where(cond, 1.0, 0.0).astype(BF16)

    head128[...] = as_bf16(iota((256, 128), 0) // 64 == iota((256, 128), 1) // 32)
    head256[...] = as_bf16(iota((256, 256), 0) // 64 == iota((256, 256), 1) // 64)
    r256, c256 = iota((256, 256), 0), iota((256, 256), 1)
    tri[...] = as_bf16((r256 // T == c256 // T) & (c256 <= r256))

    lat, ctx, normed, ready = s["lat"], s["ctx"], s["normed"], s["ready"]
    gain_row = s["gain"]

    def norm_rows(x):
        x = x.astype(F32)
        factor = lax.rsqrt(jnp.mean(x * x, axis=-1, keepdims=True) + EPS)
        return x * factor * gain_row[...]

    loaded("latent", "context", "gain")

    @pl.loop(0, CROWS // 16)
    def _(i):
        at = pl.multiple_of(i * 16, 16)
        ready[pl.ds(ROWS + at, 16), :] = norm_rows(ctx[pl.ds(at, 16), :])

    @pl.loop(0, ROWS // 16)
    def _(i):
        at = pl.ds(pl.multiple_of(i * 16, 16), 16)
        ready[at, :] = norm_rows(lat[at, :])

    arrive("sp", lambda i: mod1.at[i], s["m1s"], s["m1r"])
    total = mod1[0]
    for i in range(1, NSP):
        total = total + mod1[i]
    mod2[tp] = total
    exchange("tp", lambda to: mod2.at[tp], lambda i: mod2.at[i], s["m2s"], s["m2r"])
    ld, lcum, kk, vv = s["ld"], s["lcum"], s["kk"], s["vv"]
    acc, acc_low = s["acc"], s["acc_low"]
    own, ctx_rows = slice(0, ROWS), slice(ROWS, ALL)
    loaded("bias", "up", "post", "down", "key", "value", "query", "outgate", "out")

    def columns(origin):
        return pl.ds(pl.multiple_of(origin * 256, 256), 256)

    def modulate(origin):
        slot = mod2[origin]

        def row(i):
            return jnp.concatenate([slot[i : i + 1], slot[5 + i : 6 + i]], axis=1)

        cols = columns(origin)
        for rows, i in ((own, 0), (ctx_rows, 1)):
            values = ready[rows, cols] * (1.0 + row(2 + i)) + row(i)
            normed[rows, cols] = values.astype(BF16)

    def low_part(origin):
        cols = columns(origin)
        return dot_dims(normed[own, cols], s["wd"][:, cols], 1, 1)

    def key_part(origin):
        cols = columns(origin)
        return dot(normed[own, cols], s["wk"][cols, :])

    def value_part(origin, at):
        cols = columns(origin)
        return dot(normed[own, cols], s["wv"][cols, at])

    v_half = (slice(0, 512), slice(512, 1024))
    a_half = (slice(512, 1024), slice(1024, 1536))

    def take(origin, first=False):
        modulate(origin)
        low, key = low_part(origin), key_part(origin)
        acc_low[...] = low if first else acc_low[...] + low
        acc[:, 0:512] = key if first else acc[:, 0:512] + key
        for v_at, a_at in zip(v_half, a_half):
            value = value_part(origin, v_at)
            acc[:, a_at] = value if first else acc[:, a_at] + value

    def tp_origin(step):
        return tp_peer((4 - step[0], 2 - step[1]))

    def arrive_mod(step):
        arrive("tp", lambda i: mod2.at[i], s["m2s"], s["m2r"], only=step)

    take(tp, True)
    for step in ((0, 1), (1, 0), (3, 0), (1, 1), (3, 1)):
        arrive_mod(step)
        take(tp_origin(step))
    last = ((2, 0), (2, 1))
    for step in last:
        arrive_mod(step)
    one, two = (tp_origin(step) for step in last)
    modulate(one)
    modulate(two)
    low = (acc_low[...] + low_part(one) + low_part(two)).astype(BF16)
    kk[own, :] = (acc[:, 0:512] + key_part(one) + key_part(two)).astype(BF16)
    ld[own, :] = log_decays(dot(low, s["up_w"][...]) + s["bias"][...])

    def put_values(i):
        at = v_half[i]
        total = acc[:, a_half[i]] + value_part(one, at) + value_part(two, at)
        vv[own, at] = total.astype(BF16)

    put_values(0)
    lcum[own, :] = sum_rows(tri[...], ld[own, :])
    put_values(1)

    def project(rows):
        low = dot_dims(normed[rows, :], s["wd"][...], 1, 1).astype(BF16)
        ld[rows, :] = log_decays(dot(low, s["up_w"][...]) + s["bias"][...])
        kk[rows, :] = dot(normed[rows, :], s["wk"][...]).astype(BF16)
        for at in v_half:
            vv[rows, at] = dot(normed[rows, :], s["wv"][:, at]).astype(BF16)

    ent, tots, kd = s["ent"], s["tots"], s["kd"]
    ctx_msg, seg_msg = s["ctx_msg"], s["seg_msg"]
    ctx_all, recv_a, grp_all, back, recv_c = (
        s["ctx_all"],
        s["recv_a"],
        s["grp_all"],
        s["back"],
        s["recv_c"],
    )
    lane_head = lax.rem(iota((64, 256), 1), 128) // 32
    closings = [lcum[n * T + T - 8 : n * T + T, :][7:8] for n in range(NB)]
    whole = closings[0] + closings[1] + closings[2] + closings[3]

    def own_lanes(full):
        state = jnp.zeros((64, 256), F32)
        for h in range(4):
            state = jnp.where(lane_head == h, full[h * 64 : (h + 1) * 64], state)
        return state

    for n in range(NB):
        tots[n : n + 1, :] = closings[n]
        rows = slice(n * T, (n + 1) * T)
        ahead = behind = jnp.zeros((1, 512), F32)
        for m in range(n):
            ahead = ahead + closings[m]
        for m in range(n + 1, NB):
            behind = behind + closings[m]
        cum = lcum[rows, :]
        keys = kk[rows, :].astype(F32)
        key_f = (keys * jnp.exp(closings[n] - cum + behind)).astype(BF16)
        key_b = (keys * jnp.exp(cum - ld[rows, :] + ahead)).astype(BF16)
        for g in range(NG):
            k_at = slice(g * 128, (g + 1) * 128)
            kd[rows, g * 256 : (g + 1) * 256] = jnp.concatenate(
                [key_f[:, k_at], key_b[:, k_at]], axis=1
            )
    for g in range(NG):
        v_at = slice(g * 256, (g + 1) * 256)
        state = own_lanes(dot_dims(vv[own, v_at], kd[:, v_at], 0, 0))
        for d in range(2):
            put_message(
                seg_msg,
                d * NG + g,
                state[:, d * 128 : (d + 1) * 128],
                whole[:, g * 128 : (g + 1) * 128],
            )
    recv_a[tp] = seg_msg[tp]
    exchange("tp", lambda to: seg_msg.at[to], lambda i: recv_a.at[i], s["as"], s["ar"])

    project(ctx_rows)
    lcum[ctx_rows, :] = sum_rows(tri[0:CROWS, 0:CROWS], ld[ctx_rows, :])
    summ = s["summ"]

    def summaries(rows, count, put):
        cum = lcum[rows, :]
        before = cum - ld[rows, :]
        closing = cum[count - 1 : count, :]
        keys = kk[rows, :].astype(F32)
        key_f = (keys * jnp.exp(closing - cum)).astype(BF16)
        key_b = (keys * jnp.exp(before)).astype(BF16)
        for g in range(NG):
            k_at = slice(g * 128, (g + 1) * 128)
            both = jnp.concatenate([key_f[:, k_at], key_b[:, k_at]], axis=1)
            put(g, own_lanes(dot_dims(vv[rows, g * 256 : (g + 1) * 256], both, 0, 0)))

    ctx_total = lcum[ALL - 8 : ALL, :][7:8]

    def put_context(g, state):
        for d in range(2):
            put_message(
                ctx_msg,
                d * NG + g,
                state[:, d * 128 : (d + 1) * 128],
                ctx_total[:, g * 128 : (g + 1) * 128],
            )

    summaries(ctx_rows, CROWS, put_context)
    ctx_all[sp] = ctx_msg[tp]
    exchange("sp", lambda to: ctx_all.at[sp], lambda i: ctx_all.at[i], s["cs"], s["cr"])

    qq, gg = s["qq"], s["gg"]
    qq[...] = dot(normed[0:ROWS, :], s["wq"][...]).astype(BF16)

    @pl.loop(0, NB)
    def _(n):
        def put(g, state):
            summ[n, :, g * 256 : (g + 1) * 256] = state

        summaries(pl.ds(pl.multiple_of(n * T, T), T), T, put)

    for g in range(NG):
        close = [jnp.exp(tots[n : n + 1, g * 128 : (g + 1) * 128]) for n in range(NB)]
        for d in range(2):
            at = slice(g * 256 + d * 128, g * 256 + (d + 1) * 128)
            run = jnp.zeros((64, 128), F32)
            for n in range(NB) if d == 0 else reversed(range(NB)):
                ent[n, :, at] = run.astype(BF16)
                run = close[n] * run + summ[n, :, at]

    arrive("tp", lambda i: recv_a.at[i], s["as"], s["ar"])
    pre_s, pre_c = s["pre_s"], s["pre_c"]
    run = jnp.zeros((64, 128), F32)
    run_log = jnp.zeros((1, 128), F32)
    for i in range(NTP):
        at = i + flip * (NTP - 1 - 2 * i)
        pre_s[at] = run
        pre_c[at] = jnp.broadcast_to(run_log, (8, 128))
        state, total = get_message(recv_a, at)
        run = jnp.exp(total) * run + state
        run_log = run_log + total
    put_message(grp_all, sp, run, run_log)
    exchange("sp", lambda to: grp_all.at[sp], lambda i: grp_all.at[i], s["gs"], s["gr"], True)


    @pl.loop(0, 2)
    def _(c):
        at = pl.ds(pl.multiple_of(c * 512, 512), 512)
        gg[:, at] = dot(normed[0:ROWS, :], s["wg"][:, at]).astype(BF16)

    mixed, qd = s["mixed"], s["qd"]
    t_row = iota((64, 256), 0)
    s_col = lax.rem(iota((64, 256), 1), 64)
    up_to, from_on = s_col <= t_row, s_col >= t_row

    def four(x, mask):
        return jnp.concatenate([x, x, x, x], axis=0) * mask

    @pl.loop(0, NB)
    def _(n):
        rows = pl.ds(pl.multiple_of(n * T, T), T)
        cum = lcum[rows, :]
        before = cum - ld[rows, :]
        middle, closing = cum[T // 2 - 1 : T // 2, :], cum[T - 1 : T, :]
        ahead = jnp.zeros((1, 512), F32)
        behind = jnp.zeros((1, 512), F32)
        for m in range(NB):
            ahead = ahead + jnp.where(m < n, tots[m : m + 1, :], 0.0)
            behind = behind + jnp.where(m > n, tots[m : m + 1, :], 0.0)
        q = qq[rows, :].astype(F32) * DK**-0.5
        k = kk[rows, :].astype(F32)
        qm_f = (q * jnp.exp(cum - middle)).astype(BF16)
        qm_b = (q * jnp.exp(middle - before)).astype(BF16)
        km_f = (k * jnp.exp(middle - cum)).astype(BF16)
        km_b = (k * jnp.exp(before - middle)).astype(BF16)
        qs_f = (q * jnp.exp(cum)).astype(BF16)
        qs_b = (q * jnp.exp(closing - before)).astype(BF16)
        qd_f = (q * jnp.exp(cum + ahead)).astype(BF16)
        qd_b = (q * jnp.exp(closing - before + behind)).astype(BF16)
        for g in range(NG):
            k_at = slice(g * 128, (g + 1) * 128)
            v_at = slice(g * 256, (g + 1) * 256)
            qd[rows, v_at] = jnp.concatenate([qd_f[:, k_at], qd_b[:, k_at]], axis=1)
            score_f = dot_dims(qm_f[:, k_at], four(km_f[:, k_at], head128[...]), 1, 1)
            score_b = dot_dims(qm_b[:, k_at], four(km_b[:, k_at], head128[...]), 1, 1)
            score = jnp.where(up_to, score_f, 0.0) + jnp.where(from_on, score_b, 0.0)
            within = dot(score.astype(BF16), four(vv[rows, v_at], head256[...]))
            entering = ent[n, :, v_at]
            states = jnp.concatenate(
                [
                    four(entering[:, 0:128], head128[...]),
                    four(entering[:, 128:256], head128[...]),
                ],
                axis=1,
            )
            across = dot_dims(
                jnp.concatenate([qs_f[:, k_at], qs_b[:, k_at]], axis=1), states, 1, 1
            )
            mixed[rows, v_at] = within + across

    arrive("sp", lambda i: ctx_all.at[i], s["cs"], s["cr"])
    reach = jnp.zeros((64, 128), F32)
    for i in range(NSP):
        state, total = get_message(ctx_all, i + flip * (NSP - 1 - 2 * i))
        reach = jnp.exp(total) * reach + state
    arrive("sp", lambda i: grp_all.at[i], s["gs"], s["gr"], True)
    rank = sp + flip * (NSP - 1 - 2 * sp)
    for i in range(NSP):
        state, total = get_message(grp_all, i + flip * (NSP - 1 - 2 * i))
        reach = jnp.where(i < rank, jnp.exp(total) * reach + state, reach)
    for j in range(NTP):
        back[j] = (pre_s[j] + jnp.exp(pre_c[j][0:1]) * reach).astype(BF16)
    recv_c[tp] = back[tp]
    exchange("tp", lambda to: back.at[to], lambda i: recv_c.at[i], s["bs"], s["br"])
    ones[...] = head256[...]
    silu = s["silu"]

    @pl.loop(0, ROWS // 32)
    def _(i):
        at = pl.ds(pl.multiple_of(i * 32, 32), 32)
        gate = gg[at, :].astype(F32)
        silu[at, :] = gate * lax.logistic(gate)

    weight = s["weight"]
    for j in range(2 * NTP):
        at = slice(j * 128, (j + 1) * 128)
        gate_row = mod2[j // 2][4 + 5 * (j % 2) : 5 + 5 * (j % 2)]
        weight[:, at] = jnp.broadcast_to(gate_row * s["post_gain"][:, at], (8, 128))
    arrive("tp", lambda i: recv_c.at[i], s["bs"], s["br"])

    gated = s["gated"]
    for g in range(NG):
        v_at = slice(g * 256, (g + 1) * 256)
        states = jnp.concatenate(
            [four(recv_c[g], head128[...]), four(recv_c[NG + g], head128[...])], axis=1
        )
        values = mixed[:, v_at] + dot_dims(qd[:, v_at], states, 1, 1)
        square = values * values
        hi = square.astype(BF16)
        low = (square - hi.astype(F32)).astype(BF16)
        power = dot(hi, ones[...]) + dot(low, ones[...])
        normal = values * lax.rsqrt(power * (1.0 / DV) + EPS)
        gated[:, v_at] = (normal * silu[:, v_at]).astype(BF16)

    branch = s["branch"]
    for half in range(1):
        rows = slice(half * 256, (half + 1) * 256)
        squares = jnp.zeros((256, 128), F32)
        for i in range(8):
            at = slice(i * 256, (i + 1) * 256)
            part = dot(gated[rows, :], s["wo"][:, at]).astype(BF16)
            branch[rows, at] = part
            part = part.astype(F32)
            part = part * part
            for j in range(2):
                squares = squares + part[:, j * 128 : (j + 1) * 128]
        mean = jnp.sum(squares, axis=-1, keepdims=True) * (1.0 / D)
        factors = lax.rsqrt(mean + EPS)
        for k in range(16):
            at = slice(half * 256 + k * 16, half * 256 + (k + 1) * 16)
            added = branch[at, :].astype(F32) * factors[k * 16 : (k + 1) * 16] * weight[0:1, :]
            out[at, :] = (lat[at, :].astype(F32) + added).astype(BF16)

    for copy, later in sends:
        if later is None:
            copy.wait_send()
        else:
            pl.when(later)(copy.wait_send)


def scratch():
    vmem, sems = pltpu.VMEM, pltpu.SemaphoreType.DMA
    return dict(
        lat=vmem((ROWS, D), BF16),
        ctx=vmem((CROWS, D), BF16),
        wd=vmem((32, D), BF16),
        wk=vmem((D, 512), BF16),
        wv=vmem((D, 1024), BF16),
        wq=vmem((D, 512), BF16),
        wg=vmem((D, 1024), BF16),
        wo=vmem((1024, D), BF16),
        mod1=vmem((NSP, 10, 128), F32),
        mod2=vmem((NTP, 10, 128), F32),
        acc=vmem((ROWS, 1536), F32),
        acc_low=vmem((ROWS, 32), F32),
        normed=vmem((ALL, D), BF16),
        head128=vmem((256, 128), BF16),
        head256=vmem((256, 256), BF16),
        ones=vmem((256, 256), BF16),
        tri=vmem((256, 256), BF16),
        ld=vmem((ALL, 512), F32),
        lcum=vmem((ALL, 512), F32),
        kk=vmem((ALL, 512), BF16),
        vv=vmem((ALL, 1024), BF16),
        qq=vmem((ROWS, 512), BF16),
        gg=vmem((ROWS, 1024), BF16),
        summ=vmem((NB, 64, 1024), F32),
        kd=vmem((ROWS, 1024), BF16),
        silu=vmem((ROWS, 1024), F32),
        ent=vmem((NB, 64, 1024), BF16),
        tots=vmem((8, 512), F32),
        ctx_msg=vmem((NTP, MSG, 128), BF16),
        seg_msg=vmem((NTP, MSG, 128), BF16),
        ctx_all=vmem((NSP, MSG, 128), BF16),
        grp_all=vmem((NSP, MSG, 128), BF16),
        recv_a=vmem((NTP, MSG, 128), BF16),
        pre_s=vmem((NTP, 64, 128), F32),
        pre_c=vmem((NTP, 8, 128), F32),
        back=vmem((NTP, 64, 128), BF16),
        recv_c=vmem((NTP, 64, 128), BF16),
        mixed=vmem((ROWS, 1024), F32),
        qd=vmem((ROWS, 1024), BF16),
        gated=vmem((ROWS, 1024), BF16),
        branch=vmem((ROWS, D), BF16),
        lat_cond=vmem((16, 128), BF16),
        ctx_cond=vmem((16, 128), BF16),
        shift_w=vmem((128, 256), BF16),
        scale_w=vmem((128, 256), BF16),
        gate_w=vmem((128, 256), BF16),
        gain=vmem((1, D), F32),
        bias=vmem((1, 512), F32),
        up_w=vmem((32, 512), BF16),
        post_gain=vmem((1, D), F32),
        ready=vmem((ALL, D), F32),
        factor=vmem((ROWS, 128), F32),
        weight=vmem((8, D), F32),
        load_sem=sems((17,)),
        m1s=sems((NSP - 1,)),
        m1r=sems((NSP - 1,)),
        m2s=sems((NTP - 1,)),
        m2r=sems((NTP - 1,)),
        cs=sems((NSP - 1,)),
        cr=sems((NSP - 1,)),
        gs=sems((NSP - 1,)),
        gr=sems((NSP - 1,)),
        bs=sems((NTP - 1,)),
        br=sems((NTP - 1,)),
        **{"as": sems((NTP - 1,)), "ar": sems((NTP - 1,))},
    )


def shards(
    latent,
    context,
    latent_condition,
    context_condition,
    shift_weight,
    scale_weight,
    gate_weight,
    norm_gain,
    query_weight,
    key_weight,
    value_weight,
    outgate_weight,
    down_weight,
    up_weight,
    decay_bias,
    out_weight,
    post_gain,
):
    hbm = pl.BlockSpec(memory_space=pl.ANY)
    return pl.pallas_call(
        kernel,
        out_shape=pltpu.VMEM((ROWS, D), BF16),
        in_specs=[hbm] * 17,
        out_specs=pl.BlockSpec(memory_space=pltpu.VMEM),
        scratch_shapes=[scratch()],
        compiler_params=pltpu.CompilerParams(
            collective_id=0, has_side_effects=True, vmem_limit_bytes=60 * 1024 * 1024
        ),
    )(
        latent,
        context,
        latent_condition.reshape(16, 128),
        context_condition.reshape(16, 128),
        shift_weight,
        scale_weight,
        gate_weight,
        norm_gain[None],
        query_weight,
        key_weight,
        value_weight,
        outgate_weight,
        down_weight.T,
        up_weight,
        decay_bias[None],
        out_weight,
        post_gain[None],
    )


def solution(mesh):
    tokens = P(("sp", "tp"), None)
    maps = P("sp", "tp")
    placed = (tokens, P("sp", None), P(), P(), maps, maps, maps) + (P(),) * 10
    return jax.shard_map(
        shards, mesh=mesh, in_specs=placed, out_specs=tokens, check_vma=False
    )
```

```python
import jax
import jax.numpy as jnp
from jax import lax
from jax.experimental import pallas as pl
from jax.experimental.pallas import tpu as pltpu
from jax.sharding import PartitionSpec as P

F32 = jnp.float32
BF16 = jnp.bfloat16
MESH = pl.DeviceIdType.MESH
EPS = 1e-06

NSP = 16
NTP = 8
D = 2048
HEADS = 16
DK = 32
DV = 64
ROWS = 256
CROWS = 32
ALL = ROWS + CROWS
T = 64
NB = ROWS // T
NG = 4
MSG = 80


def far_first(lengths):
    steps = [(a, b) for a in range(lengths[0]) for b in range(lengths[1]) if (a, b) != (0, 0)]
    hops = [0, 1, 2, 1]
    weight = 2 if lengths[1] == 2 else 1
    return sorted(steps, key=lambda t: -(weight * hops[t[0]] + hops[t[1]]))


SP_STEPS = far_first((4, 4))
TP_STEPS = far_first((4, 2))


def dot(a, b):
    return jnp.dot(a, b, preferred_element_type=F32)


def dot_dims(a, b, ca, cb):
    return lax.dot_general(a, b, (((ca,), (cb,)), ((), ())), preferred_element_type=F32)


def iota(shape, dim):
    return lax.broadcasted_iota(jnp.int32, shape, dim)


def split3(x):
    hi = x.astype(BF16)
    rest = x - hi.astype(F32)
    mid = rest.astype(BF16)
    return hi, mid, (rest - mid.astype(F32)).astype(BF16)


def sum_rows(tri, x):
    hi, mid, lo = split3(x)
    return dot(tri, hi) + dot(tri, mid) + dot(tri, lo)


def log_decays(pre):
    return (jnp.minimum(pre, 0.0) - jnp.log1p(jnp.exp(-jnp.abs(pre)))) * (1.0 / 16.0)


def put_message(ref, at, state, total):
    hi, mid, lo = split3(total)
    row = iota((16, 128), 0)
    tail = jnp.where(
        row == 0,
        hi.astype(F32),
        jnp.where(row == 1, mid.astype(F32), jnp.where(row == 2, lo.astype(F32), 0.0)),
    )
    ref[at, 0:64, :] = state.astype(BF16)
    ref[at, 64:MSG, :] = tail.astype(BF16)


def get_message(ref, at):
    state = ref[at, 0:64, :].astype(F32)
    tail = ref[at, 64:MSG, :].astype(F32)
    return state, tail[0:1] + tail[1:2] + tail[2:3]


def kernel(
    latent,
    context,
    lat_cond,
    ctx_cond,
    shift_w,
    scale_w,
    gate_w,
    gain,
    query_w,
    key_w,
    value_w,
    outgate_w,
    down_w,
    up_w,
    bias,
    out_w,
    post_gain,
    out,
    s,
):
    sp = lax.axis_index("sp")
    tp = lax.axis_index("tp")

    z, x = lax.div(sp, 4), lax.rem(sp, 4)
    y, c = lax.div(tp, 2), lax.rem(tp, 2)

    def sp_peer(step):
        return lax.rem(z + step[0], 4) * 4 + lax.rem(x + step[1], 4)

    def tp_peer(step):
        return lax.rem(y + step[0], 4) * 2 + lax.rem(c + step[1], 2)

    barrier = pltpu.get_barrier_semaphore()
    for step in SP_STEPS:
        pl.semaphore_signal(barrier, inc=1, device_id=(sp_peer(step), tp), device_id_type=MESH)
    for step in TP_STEPS:
        pl.semaphore_signal(barrier, inc=1, device_id=(sp, tp_peer(step)), device_id_type=MESH)

    pairs = dict(
        lat_cond=(lat_cond, s["lat_cond"]),
        ctx_cond=(ctx_cond, s["ctx_cond"]),
        shift=(shift_w, s["shift_w"]),
        scale=(scale_w, s["scale_w"]),
        gate=(gate_w, s["gate_w"]),
        latent=(latent, s["lat"]),
        context=(context, s["ctx"]),
        gain=(gain, s["gain"]),
        bias=(bias, s["bias"]),
        up=(up_w, s["up_w"]),
        post=(post_gain, s["post_gain"]),
        down=(down_w, s["wd"]),
        key=(key_w, s["wk"]),
        value=(value_w, s["wv"]),
        query=(query_w, s["wq"]),
        outgate=(outgate_w, s["wg"]),
        out=(out_w, s["wo"]),
    )
    loads = {
        name: pltpu.make_async_copy(src, dst, s["load_sem"].at[i])
        for i, (name, (src, dst)) in enumerate(pairs.items())
    }
    for name in loads:
        loads[name].start()

    def loaded(*names):
        for name in names:
            loads[name].wait()

    sends = []

    flip = c

    def exchange(axis, src, dst, send_sem, recv_sem, ordered=False):
        steps, peer = (SP_STEPS, sp_peer) if axis == "sp" else (TP_STEPS, tp_peer)
        for d, step in enumerate(steps):
            to = peer(step)
            copy = pltpu.make_async_remote_copy(
                src_ref=src(to),
                dst_ref=dst(sp if axis == "sp" else tp),
                send_sem=send_sem.at[d],
                recv_sem=recv_sem.at[d],
                device_id=(to, tp) if axis == "sp" else (sp, to),
                device_id_type=MESH,
            )
            later = (to - sp) * (1 - 2 * flip) > 0 if ordered else None
            if ordered:
                pl.when(later)(copy.start)
            else:
                copy.start()
            sends.append((copy, later))

    def arrive(axis, dst, send_sem, recv_sem, ordered=False, only=None):
        steps, wrap, peer = (
            (SP_STEPS, (4, 4), sp_peer) if axis == "sp" else (TP_STEPS, (4, 2), tp_peer)
        )
        for d, step in reversed(list(enumerate(steps))):
            if only is not None and step != only:
                continue
            origin = peer((wrap[0] - step[0], wrap[1] - step[1]))
            copy = pltpu.make_async_remote_copy(
                src_ref=dst(origin),
                dst_ref=dst(origin),
                send_sem=send_sem.at[d],
                recv_sem=recv_sem.at[d],
                device_id=(origin, tp) if axis == "sp" else (sp, origin),
                device_id_type=MESH,
            )
            if ordered:
                pl.when((sp - origin) * (1 - 2 * flip) > 0)(copy.wait_recv)
            else:
                copy.wait_recv()

    loaded("lat_cond", "ctx_cond", "shift", "scale", "gate")
    row16 = iota((16, 128), 0)

    def cond_row(name):
        mine = jnp.where(row16 == sp, s[name][...].astype(F32), 0.0)
        return jnp.broadcast_to(jnp.sum(mine, axis=0, keepdims=True), (16, 128))

    cond = jnp.where(lax.rem(row16, 2) == 0, cond_row("lat_cond"), cond_row("ctx_cond"))
    act = (cond * lax.logistic(cond)).astype(BF16)
    row8 = iota((8, 256), 0)
    part = jnp.where(
        row8 < 2,
        dot(act, s["shift_w"][...])[0:8],
        jnp.where(row8 < 4, dot(act, s["scale_w"][...])[0:8], dot(act, s["gate_w"][...])[0:8]),
    )
    mod1, mod2 = s["mod1"], s["mod2"]
    mod1[sp, 0:5, :] = part[0:5, 0:128]
    mod1[sp, 5:10, :] = part[0:5, 128:256]
    pl.semaphore_wait(barrier, NSP + NTP - 2)
    exchange("sp", lambda to: mod1.at[sp], lambda i: mod1.at[i], s["m1s"], s["m1r"])

    head128, head256, tri, ones = s["head128"], s["head256"], s["tri"], s["ones"]

    def as_bf16(cond):
        return jnp.where(cond, 1.0, 0.0).astype(BF16)

    head128[...] = as_bf16(iota((256, 128), 0) // 64 == iota((256, 128), 1) // 32)
    head256[...] = as_bf16(iota((256, 256), 0) // 64 == iota((256, 256), 1) // 64)
    r256, c256 = iota((256, 256), 0), iota((256, 256), 1)
    tri[...] = as_bf16((r256 // T == c256 // T) & (c256 <= r256))

    lat, ctx, normed, ready = s["lat"], s["ctx"], s["normed"], s["ready"]
    gain_row = s["gain"]

    def norm_rows(x):
        x = x.astype(F32)
        factor = lax.rsqrt(jnp.mean(x * x, axis=-1, keepdims=True) + EPS)
        return x * factor * gain_row[...]

    loaded("latent", "context", "gain")

    @pl.loop(0, CROWS // 16)
    def _(i):
        at = pl.multiple_of(i * 16, 16)
        ready[pl.ds(ROWS + at, 16), :] = norm_rows(ctx[pl.ds(at, 16), :])

    @pl.loop(0, ROWS // 16)
    def _(i):
        at = pl.ds(pl.multiple_of(i * 16, 16), 16)
        ready[at, :] = norm_rows(lat[at, :])

    arrive("sp", lambda i: mod1.at[i], s["m1s"], s["m1r"])
    total = mod1[0]
    for i in range(1, NSP):
        total = total + mod1[i]
    mod2[tp] = total
    exchange("tp", lambda to: mod2.at[tp], lambda i: mod2.at[i], s["m2s"], s["m2r"])
    ld, lcum, kk, vv = s["ld"], s["lcum"], s["kk"], s["vv"]
    acc, acc_low = s["acc"], s["acc_low"]
    own, ctx_rows = slice(0, ROWS), slice(ROWS, ALL)
    loaded("bias", "up", "post", "down", "key", "value", "query", "outgate", "out")

    def columns(origin):
        return pl.ds(pl.multiple_of(origin * 256, 256), 256)

    def modulate(origin):
        slot = mod2[origin]

        def row(i):
            return jnp.concatenate([slot[i : i + 1], slot[5 + i : 6 + i]], axis=1)

        cols = columns(origin)
        for rows, i in ((own, 0), (ctx_rows, 1)):
            values = ready[rows, cols] * (1.0 + row(2 + i)) + row(i)
            normed[rows, cols] = values.astype(BF16)

    def low_part(origin):
        cols = columns(origin)
        return dot_dims(normed[own, cols], s["wd"][:, cols], 1, 1)

    def key_part(origin):
        cols = columns(origin)
        return dot(normed[own, cols], s["wk"][cols, :])

    def value_part(origin, at):
        cols = columns(origin)
        return dot(normed[own, cols], s["wv"][cols, at])

    v_half = (slice(0, 512), slice(512, 1024))
    a_half = (slice(512, 1024), slice(1024, 1536))

    def take(origin, first=False):
        modulate(origin)
        low, key = low_part(origin), key_part(origin)
        acc_low[...] = low if first else acc_low[...] + low
        acc[:, 0:512] = key if first else acc[:, 0:512] + key
        for v_at, a_at in zip(v_half, a_half):
            value = value_part(origin, v_at)
            acc[:, a_at] = value if first else acc[:, a_at] + value

    def tp_origin(step):
        return tp_peer((4 - step[0], 2 - step[1]))

    def arrive_mod(step):
        arrive("tp", lambda i: mod2.at[i], s["m2s"], s["m2r"], only=step)

    take(tp, True)
    for step in ((0, 1), (1, 0), (3, 0), (1, 1), (3, 1)):
        arrive_mod(step)
        take(tp_origin(step))
    last = ((2, 0), (2, 1))
    for step in last:
        arrive_mod(step)
    one, two = (tp_origin(step) for step in last)
    modulate(one)
    modulate(two)
    low = (acc_low[...] + low_part(one) + low_part(two)).astype(BF16)
    kk[own, :] = (acc[:, 0:512] + key_part(one) + key_part(two)).astype(BF16)
    ld[own, :] = log_decays(dot(low, s["up_w"][...]) + s["bias"][...])

    def put_values(i):
        at = v_half[i]
        total = acc[:, a_half[i]] + value_part(one, at) + value_part(two, at)
        vv[own, at] = total.astype(BF16)

    put_values(0)
    lcum[own, :] = sum_rows(tri[...], ld[own, :])
    put_values(1)

    def project(rows):
        low = dot_dims(normed[rows, :], s["wd"][...], 1, 1).astype(BF16)
        ld[rows, :] = log_decays(dot(low, s["up_w"][...]) + s["bias"][...])
        kk[rows, :] = dot(normed[rows, :], s["wk"][...]).astype(BF16)
        for at in v_half:
            vv[rows, at] = dot(normed[rows, :], s["wv"][:, at]).astype(BF16)

    ent, tots, kd = s["ent"], s["tots"], s["kd"]
    ctx_msg, seg_msg = s["ctx_msg"], s["seg_msg"]
    ctx_all, recv_a, grp_all, back, recv_c = (
        s["ctx_all"],
        s["recv_a"],
        s["grp_all"],
        s["back"],
        s["recv_c"],
    )
    lane_head = lax.rem(iota((64, 256), 1), 128) // 32
    closings = [lcum[n * T + T - 8 : n * T + T, :][7:8] for n in range(NB)]
    whole = closings[0] + closings[1] + closings[2] + closings[3]

    def own_lanes(full):
        state = jnp.zeros((64, 256), F32)
        for h in range(4):
            state = jnp.where(lane_head == h, full[h * 64 : (h + 1) * 64], state)
        return state

    for n in range(NB):
        tots[n : n + 1, :] = closings[n]
        rows = slice(n * T, (n + 1) * T)
        ahead = behind = jnp.zeros((1, 512), F32)
        for m in range(n):
            ahead = ahead + closings[m]
        for m in range(n + 1, NB):
            behind = behind + closings[m]
        cum = lcum[rows, :]
        keys = kk[rows, :].astype(F32)
        key_f = (keys * jnp.exp(closings[n] - cum + behind)).astype(BF16)
        key_b = (keys * jnp.exp(cum - ld[rows, :] + ahead)).astype(BF16)
        for g in range(NG):
            k_at = slice(g * 128, (g + 1) * 128)
            kd[rows, g * 256 : (g + 1) * 256] = jnp.concatenate(
                [key_f[:, k_at], key_b[:, k_at]], axis=1
            )
    for g in range(NG):
        v_at = slice(g * 256, (g + 1) * 256)
        state = own_lanes(dot_dims(vv[own, v_at], kd[:, v_at], 0, 0))
        for d in range(2):
            put_message(
                seg_msg,
                2 * g + d,
                state[:, d * 128 : (d + 1) * 128],
                whole[:, g * 128 : (g + 1) * 128],
            )
    recv_a[tp] = seg_msg[tp]
    exchange("tp", lambda to: seg_msg.at[to], lambda i: recv_a.at[i], s["as"], s["ar"])

    project(ctx_rows)
    lcum[ctx_rows, :] = sum_rows(tri[0:CROWS, 0:CROWS], ld[ctx_rows, :])
    summ = s["summ"]

    def summaries(rows, count, put):
        cum = lcum[rows, :]
        before = cum - ld[rows, :]
        closing = cum[count - 1 : count, :]
        keys = kk[rows, :].astype(F32)
        key_f = (keys * jnp.exp(closing - cum)).astype(BF16)
        key_b = (keys * jnp.exp(before)).astype(BF16)
        for g in range(NG):
            k_at = slice(g * 128, (g + 1) * 128)
            both = jnp.concatenate([key_f[:, k_at], key_b[:, k_at]], axis=1)
            put(g, own_lanes(dot_dims(vv[rows, g * 256 : (g + 1) * 256], both, 0, 0)))

    ctx_total = lcum[ALL - 8 : ALL, :][7:8]

    def put_context(g, state):
        for d in range(2):
            put_message(
                ctx_msg,
                2 * g + d,
                state[:, d * 128 : (d + 1) * 128],
                ctx_total[:, g * 128 : (g + 1) * 128],
            )

    summaries(ctx_rows, CROWS, put_context)
    ctx_all[sp] = ctx_msg[tp]
    exchange("sp", lambda to: ctx_all.at[sp], lambda i: ctx_all.at[i], s["cs"], s["cr"])

    qq, gg = s["qq"], s["gg"]
    qq[...] = dot(normed[0:ROWS, :], s["wq"][...]).astype(BF16)

    @pl.loop(0, NB)
    def _(n):
        def put(g, state):
            summ[n, :, g * 256 : (g + 1) * 256] = state

        summaries(pl.ds(pl.multiple_of(n * T, T), T), T, put)

    for g in range(NG):
        close = [jnp.exp(tots[n : n + 1, g * 128 : (g + 1) * 128]) for n in range(NB)]
        for d in range(2):
            at = slice(g * 256 + d * 128, g * 256 + (d + 1) * 128)
            run = jnp.zeros((64, 128), F32)
            for n in range(NB) if d == 0 else reversed(range(NB)):
                ent[n, :, at] = run.astype(BF16)
                run = close[n] * run + summ[n, :, at]

    arrive("tp", lambda i: recv_a.at[i], s["as"], s["ar"])
    pre_s, pre_c = s["pre_s"], s["pre_c"]
    run = jnp.zeros((64, 128), F32)
    run_log = jnp.zeros((1, 128), F32)
    for i in range(NTP):
        at = i + flip * (NTP - 1 - 2 * i)
        pre_s[at] = run
        pre_c[at] = jnp.broadcast_to(run_log, (8, 128))
        state, total = get_message(recv_a, at)
        run = jnp.exp(total) * run + state
        run_log = run_log + total
    put_message(grp_all, sp, run, run_log)
    exchange("sp", lambda to: grp_all.at[sp], lambda i: grp_all.at[i], s["gs"], s["gr"], True)


    @pl.loop(0, 2)
    def _(c):
        at = pl.ds(pl.multiple_of(c * 512, 512), 512)
        gg[:, at] = dot(normed[0:ROWS, :], s["wg"][:, at]).astype(BF16)

    mixed, qd = s["mixed"], s["qd"]
    t_row = iota((64, 256), 0)
    s_col = lax.rem(iota((64, 256), 1), 64)
    up_to, from_on = s_col <= t_row, s_col >= t_row

    def four(x, mask):
        return jnp.concatenate([x, x, x, x], axis=0) * mask

    @pl.loop(0, NB)
    def _(n):
        rows = pl.ds(pl.multiple_of(n * T, T), T)
        cum = lcum[rows, :]
        before = cum - ld[rows, :]
        middle, closing = cum[T // 2 - 1 : T // 2, :], cum[T - 1 : T, :]
        ahead = jnp.zeros((1, 512), F32)
        behind = jnp.zeros((1, 512), F32)
        for m in range(NB):
            ahead = ahead + jnp.where(m < n, tots[m : m + 1, :], 0.0)
            behind = behind + jnp.where(m > n, tots[m : m + 1, :], 0.0)
        q = qq[rows, :].astype(F32) * DK**-0.5
        k = kk[rows, :].astype(F32)
        qm_f = (q * jnp.exp(cum - middle)).astype(BF16)
        qm_b = (q * jnp.exp(middle - before)).astype(BF16)
        km_f = (k * jnp.exp(middle - cum)).astype(BF16)
        km_b = (k * jnp.exp(before - middle)).astype(BF16)
        qs_f = (q * jnp.exp(cum)).astype(BF16)
        qs_b = (q * jnp.exp(closing - before)).astype(BF16)
        qd_f = (q * jnp.exp(cum + ahead)).astype(BF16)
        qd_b = (q * jnp.exp(closing - before + behind)).astype(BF16)
        for g in range(NG):
            k_at = slice(g * 128, (g + 1) * 128)
            v_at = slice(g * 256, (g + 1) * 256)
            qd[rows, v_at] = jnp.concatenate([qd_f[:, k_at], qd_b[:, k_at]], axis=1)
            score_f = dot_dims(qm_f[:, k_at], four(km_f[:, k_at], head128[...]), 1, 1)
            score_b = dot_dims(qm_b[:, k_at], four(km_b[:, k_at], head128[...]), 1, 1)
            score = jnp.where(up_to, score_f, 0.0) + jnp.where(from_on, score_b, 0.0)
            within = dot(score.astype(BF16), four(vv[rows, v_at], head256[...]))
            entering = ent[n, :, v_at]
            states = jnp.concatenate(
                [
                    four(entering[:, 0:128], head128[...]),
                    four(entering[:, 128:256], head128[...]),
                ],
                axis=1,
            )
            across = dot_dims(
                jnp.concatenate([qs_f[:, k_at], qs_b[:, k_at]], axis=1), states, 1, 1
            )
            mixed[rows, v_at] = within + across

    arrive("sp", lambda i: ctx_all.at[i], s["cs"], s["cr"])
    reach = jnp.zeros((64, 128), F32)
    for i in range(NSP):
        state, total = get_message(ctx_all, i + flip * (NSP - 1 - 2 * i))
        reach = jnp.exp(total) * reach + state
    arrive("sp", lambda i: grp_all.at[i], s["gs"], s["gr"], True)
    rank = sp + flip * (NSP - 1 - 2 * sp)
    for i in range(NSP):
        state, total = get_message(grp_all, i + flip * (NSP - 1 - 2 * i))
        reach = jnp.where(i < rank, jnp.exp(total) * reach + state, reach)
    for j in range(NTP):
        back[j] = (pre_s[j] + jnp.exp(pre_c[j][0:1]) * reach).astype(BF16)
    recv_c[tp] = back[tp]
    exchange("tp", lambda to: back.at[to], lambda i: recv_c.at[i], s["bs"], s["br"])
    ones[...] = head256[...]
    silu = s["silu"]

    @pl.loop(0, ROWS // 32)
    def _(i):
        at = pl.ds(pl.multiple_of(i * 32, 32), 32)
        gate = gg[at, :].astype(F32)
        silu[at, :] = gate * lax.logistic(gate)

    weight = s["weight"]
    for j in range(2 * NTP):
        at = slice(j * 128, (j + 1) * 128)
        gate_row = mod2[j // 2][4 + 5 * (j % 2) : 5 + 5 * (j % 2)]
        weight[:, at] = jnp.broadcast_to(gate_row * s["post_gain"][:, at], (8, 128))

    acc_out = s["acc_out"]

    def gated_group(dy):
        for dc in (0, 1):
            if (dy, dc) != (0, 0):
                arrive("tp", lambda i: recv_c.at[i], s["bs"], s["br"], only=(dy, dc))
        g = lax.rem(y + 4 - dy, 4)
        v_at = pl.ds(pl.multiple_of(g * 256, 256), 256)
        states = jnp.concatenate(
            [four(recv_c[2 * g], head128[...]), four(recv_c[2 * g + 1], head128[...])], axis=1
        )
        values = mixed[:, v_at] + dot_dims(qd[:, v_at], states, 1, 1)
        square = values * values
        hi = square.astype(BF16)
        low = (square - hi.astype(F32)).astype(BF16)
        power = dot(hi, ones[...]) + dot(low, ones[...])
        normal = values * lax.rsqrt(power * (1.0 / DV) + EPS)
        return (normal * silu[:, v_at]).astype(BF16), v_at

    for i, dy in enumerate((0, 1, 3)):
        gated, k_rows = gated_group(dy)
        for j in range(4):
            at = slice(j * 512, (j + 1) * 512)
            part = dot(gated, s["wo"][k_rows, at])
            acc_out[:, at] = part if i == 0 else acc_out[:, at] + part
    gated, k_rows = gated_group(2)

    branch = s["branch"]
    squares = jnp.zeros((ROWS, 128), F32)
    for i in range(8):
        at = slice(i * 256, (i + 1) * 256)
        part = (acc_out[:, at] + dot(gated, s["wo"][k_rows, at])).astype(BF16)
        branch[:, at] = part
        part = part.astype(F32)
        part = part * part
        for j in range(2):
            squares = squares + part[:, j * 128 : (j + 1) * 128]
    mean = jnp.sum(squares, axis=-1, keepdims=True) * (1.0 / D)
    factors = lax.rsqrt(mean + EPS)
    for k in range(ROWS // 16):
        at = slice(k * 16, (k + 1) * 16)
        added = branch[at, :].astype(F32) * factors[at] * weight[0:1, :]
        out[at, :] = (lat[at, :].astype(F32) + added).astype(BF16)

    for copy, later in sends:
        if later is None:
            copy.wait_send()
        else:
            pl.when(later)(copy.wait_send)


def scratch():
    vmem, sems = pltpu.VMEM, pltpu.SemaphoreType.DMA
    return dict(
        lat=vmem((ROWS, D), BF16),
        ctx=vmem((CROWS, D), BF16),
        wd=vmem((32, D), BF16),
        wk=vmem((D, 512), BF16),
        wv=vmem((D, 1024), BF16),
        wq=vmem((D, 512), BF16),
        wg=vmem((D, 1024), BF16),
        wo=vmem((1024, D), BF16),
        mod1=vmem((NSP, 10, 128), F32),
        mod2=vmem((NTP, 10, 128), F32),
        acc=vmem((ROWS, 1536), F32),
        acc_low=vmem((ROWS, 32), F32),
        normed=vmem((ALL, D), BF16),
        head128=vmem((256, 128), BF16),
        head256=vmem((256, 256), BF16),
        ones=vmem((256, 256), BF16),
        tri=vmem((256, 256), BF16),
        ld=vmem((ALL, 512), F32),
        lcum=vmem((ALL, 512), F32),
        kk=vmem((ALL, 512), BF16),
        vv=vmem((ALL, 1024), BF16),
        qq=vmem((ROWS, 512), BF16),
        gg=vmem((ROWS, 1024), BF16),
        summ=vmem((NB, 64, 1024), F32),
        kd=vmem((ROWS, 1024), BF16),
        silu=vmem((ROWS, 1024), F32),
        ent=vmem((NB, 64, 1024), BF16),
        tots=vmem((8, 512), F32),
        ctx_msg=vmem((NTP, MSG, 128), BF16),
        seg_msg=vmem((NTP, MSG, 128), BF16),
        ctx_all=vmem((NSP, MSG, 128), BF16),
        grp_all=vmem((NSP, MSG, 128), BF16),
        recv_a=vmem((NTP, MSG, 128), BF16),
        pre_s=vmem((NTP, 64, 128), F32),
        pre_c=vmem((NTP, 8, 128), F32),
        back=vmem((NTP, 64, 128), BF16),
        recv_c=vmem((NTP, 64, 128), BF16),
        mixed=vmem((ROWS, 1024), F32),
        qd=vmem((ROWS, 1024), BF16),
        acc_out=vmem((ROWS, D), F32),
        branch=vmem((ROWS, D), BF16),
        lat_cond=vmem((16, 128), BF16),
        ctx_cond=vmem((16, 128), BF16),
        shift_w=vmem((128, 256), BF16),
        scale_w=vmem((128, 256), BF16),
        gate_w=vmem((128, 256), BF16),
        gain=vmem((1, D), F32),
        bias=vmem((1, 512), F32),
        up_w=vmem((32, 512), BF16),
        post_gain=vmem((1, D), F32),
        ready=vmem((ALL, D), F32),
        weight=vmem((8, D), F32),
        load_sem=sems((17,)),
        m1s=sems((NSP - 1,)),
        m1r=sems((NSP - 1,)),
        m2s=sems((NTP - 1,)),
        m2r=sems((NTP - 1,)),
        cs=sems((NSP - 1,)),
        cr=sems((NSP - 1,)),
        gs=sems((NSP - 1,)),
        gr=sems((NSP - 1,)),
        bs=sems((NTP - 1,)),
        br=sems((NTP - 1,)),
        **{"as": sems((NTP - 1,)), "ar": sems((NTP - 1,))},
    )


def shards(
    latent,
    context,
    latent_condition,
    context_condition,
    shift_weight,
    scale_weight,
    gate_weight,
    norm_gain,
    query_weight,
    key_weight,
    value_weight,
    outgate_weight,
    down_weight,
    up_weight,
    decay_bias,
    out_weight,
    post_gain,
):
    hbm = pl.BlockSpec(memory_space=pl.ANY)
    return pl.pallas_call(
        kernel,
        out_shape=pltpu.VMEM((ROWS, D), BF16),
        in_specs=[hbm] * 17,
        out_specs=pl.BlockSpec(memory_space=pltpu.VMEM),
        scratch_shapes=[scratch()],
        compiler_params=pltpu.CompilerParams(
            collective_id=0, has_side_effects=True, vmem_limit_bytes=60 * 1024 * 1024
        ),
    )(
        latent,
        context,
        latent_condition.reshape(16, 128),
        context_condition.reshape(16, 128),
        shift_weight,
        scale_weight,
        gate_weight,
        norm_gain[None],
        query_weight,
        key_weight,
        value_weight,
        outgate_weight,
        down_weight.T,
        up_weight,
        decay_bias[None],
        out_weight,
        post_gain[None],
    )


def solution(mesh):
    tokens = P(("sp", "tp"), None)
    maps = P("sp", "tp")
    placed = (tokens, P("sp", None), P(), P(), maps, maps, maps) + (P(),) * 10
    return jax.shard_map(
        shards, mesh=mesh, in_specs=placed, out_specs=tokens, check_vma=False
    )
```

```python
import jax
import jax.numpy as jnp
from jax import lax
from jax.experimental import pallas as pl
from jax.experimental.pallas import tpu as pltpu
from jax.sharding import PartitionSpec as P

F32 = jnp.float32
BF16 = jnp.bfloat16
MESH = pl.DeviceIdType.MESH
EPS = 1e-06

NSP = 16
NTP = 8
D = 2048
HEADS = 16
DK = 32
DV = 64
ROWS = 256
CROWS = 32
ALL = ROWS + CROWS
T = 64
NB = ROWS // T
NG = 4
MSG = 80


def far_first(lengths):
    steps = [(a, b) for a in range(lengths[0]) for b in range(lengths[1]) if (a, b) != (0, 0)]
    hops = [0, 1, 2, 1]
    weight = 2 if lengths[1] == 2 else 1
    return sorted(steps, key=lambda t: -(weight * hops[t[0]] + hops[t[1]]))


SP_STEPS = far_first((4, 4))
TP_STEPS = far_first((4, 2))


def dot(a, b):
    return jnp.dot(a, b, preferred_element_type=F32)


def dot_dims(a, b, ca, cb):
    return lax.dot_general(a, b, (((ca,), (cb,)), ((), ())), preferred_element_type=F32)


def iota(shape, dim):
    return lax.broadcasted_iota(jnp.int32, shape, dim)


def split3(x):
    hi = x.astype(BF16)
    rest = x - hi.astype(F32)
    mid = rest.astype(BF16)
    return hi, mid, (rest - mid.astype(F32)).astype(BF16)


def sum_rows(tri, x):
    hi, mid, lo = split3(x)
    return dot(tri, hi) + dot(tri, mid) + dot(tri, lo)


def log_decays(pre):
    return (jnp.minimum(pre, 0.0) - jnp.log1p(jnp.exp(-jnp.abs(pre)))) * (1.0 / 16.0)


def put_message(ref, at, state, total):
    hi, mid, lo = split3(total)
    row = iota((16, 128), 0)
    tail = jnp.where(
        row == 0,
        hi.astype(F32),
        jnp.where(row == 1, mid.astype(F32), jnp.where(row == 2, lo.astype(F32), 0.0)),
    )
    ref[at, 0:64, :] = state.astype(BF16)
    ref[at, 64:MSG, :] = tail.astype(BF16)


def get_message(ref, at):
    state = ref[at, 0:64, :].astype(F32)
    tail = ref[at, 64:MSG, :].astype(F32)
    return state, tail[0:1] + tail[1:2] + tail[2:3]


def kernel(
    latent,
    context,
    lat_cond,
    ctx_cond,
    shift_w,
    scale_w,
    gate_w,
    gain,
    query_w,
    key_w,
    value_w,
    outgate_w,
    down_w,
    up_w,
    bias,
    out_w,
    post_gain,
    out,
    s,
):
    sp = lax.axis_index("sp")
    tp = lax.axis_index("tp")

    z, x = lax.div(sp, 4), lax.rem(sp, 4)
    y, c = lax.div(tp, 2), lax.rem(tp, 2)

    def sp_peer(step):
        return lax.rem(z + step[0], 4) * 4 + lax.rem(x + step[1], 4)

    def tp_peer(step):
        return lax.rem(y + step[0], 4) * 2 + lax.rem(c + step[1], 2)

    barrier = pltpu.get_barrier_semaphore()
    for step in SP_STEPS:
        pl.semaphore_signal(barrier, inc=1, device_id=(sp_peer(step), tp), device_id_type=MESH)
    for step in TP_STEPS:
        pl.semaphore_signal(barrier, inc=1, device_id=(sp, tp_peer(step)), device_id_type=MESH)

    pairs = dict(
        lat_cond=(lat_cond, s["lat_cond"]),
        ctx_cond=(ctx_cond, s["ctx_cond"]),
        shift=(shift_w, s["shift_w"]),
        scale=(scale_w, s["scale_w"]),
        gate=(gate_w, s["gate_w"]),
        latent=(latent, s["lat"]),
        context=(context, s["ctx"]),
        gain=(gain, s["gain"]),
        bias=(bias, s["bias"]),
        up=(up_w, s["up_w"]),
        post=(post_gain, s["post_gain"]),
        down=(down_w, s["wd"]),
        key=(key_w, s["wk"]),
        value=(value_w, s["wv"]),
        query=(query_w, s["wq"]),
        outgate=(outgate_w, s["wg"]),
        out=(out_w, s["wo"]),
    )
    loads = {
        name: pltpu.make_async_copy(src, dst, s["load_sem"].at[i])
        for i, (name, (src, dst)) in enumerate(pairs.items())
    }
    for name in loads:
        loads[name].start()

    def loaded(*names):
        for name in names:
            loads[name].wait()

    sends = []

    flip = c

    def exchange(axis, src, dst, send_sem, recv_sem, ordered=False, only=None):
        steps, peer = (SP_STEPS, sp_peer) if axis == "sp" else (TP_STEPS, tp_peer)
        for d, step in enumerate(steps):
            if only is not None and step[0] != only:
                continue
            to = peer(step)
            copy = pltpu.make_async_remote_copy(
                src_ref=src(to),
                dst_ref=dst(sp if axis == "sp" else tp),
                send_sem=send_sem.at[d],
                recv_sem=recv_sem.at[d],
                device_id=(to, tp) if axis == "sp" else (sp, to),
                device_id_type=MESH,
            )
            later = (to - sp) * (1 - 2 * flip) > 0 if ordered else None
            if ordered:
                pl.when(later)(copy.start)
            else:
                copy.start()
            sends.append((copy, later))

    def arrive(axis, dst, send_sem, recv_sem, ordered=False, only=None):
        steps, wrap, peer = (
            (SP_STEPS, (4, 4), sp_peer) if axis == "sp" else (TP_STEPS, (4, 2), tp_peer)
        )
        for d, step in reversed(list(enumerate(steps))):
            if only is not None and step != only:
                continue
            origin = peer((wrap[0] - step[0], wrap[1] - step[1]))
            copy = pltpu.make_async_remote_copy(
                src_ref=dst(origin),
                dst_ref=dst(origin),
                send_sem=send_sem.at[d],
                recv_sem=recv_sem.at[d],
                device_id=(origin, tp) if axis == "sp" else (sp, origin),
                device_id_type=MESH,
            )
            if ordered:
                pl.when((sp - origin) * (1 - 2 * flip) > 0)(copy.wait_recv)
            else:
                copy.wait_recv()

    loaded("lat_cond", "ctx_cond", "shift", "scale", "gate")
    row16 = iota((16, 128), 0)

    def cond_row(name):
        mine = jnp.where(row16 == sp, s[name][...].astype(F32), 0.0)
        return jnp.broadcast_to(jnp.sum(mine, axis=0, keepdims=True), (16, 128))

    cond = jnp.where(lax.rem(row16, 2) == 0, cond_row("lat_cond"), cond_row("ctx_cond"))
    act = (cond * lax.logistic(cond)).astype(BF16)
    row8 = iota((8, 256), 0)
    part = jnp.where(
        row8 < 2,
        dot(act, s["shift_w"][...])[0:8],
        jnp.where(row8 < 4, dot(act, s["scale_w"][...])[0:8], dot(act, s["gate_w"][...])[0:8]),
    )
    mod1, mod2 = s["mod1"], s["mod2"]
    mod1[sp, 0:5, :] = part[0:5, 0:128]
    mod1[sp, 5:10, :] = part[0:5, 128:256]
    pl.semaphore_wait(barrier, NSP + NTP - 2)
    exchange("sp", lambda to: mod1.at[sp], lambda i: mod1.at[i], s["m1s"], s["m1r"])

    head128, head256, tri, ones = s["head128"], s["head256"], s["tri"], s["ones"]

    def as_bf16(cond):
        return jnp.where(cond, 1.0, 0.0).astype(BF16)

    head128[...] = as_bf16(iota((256, 128), 0) // 64 == iota((256, 128), 1) // 32)
    head256[...] = as_bf16(iota((256, 256), 0) // 64 == iota((256, 256), 1) // 64)
    r256, c256 = iota((256, 256), 0), iota((256, 256), 1)
    tri[...] = as_bf16((r256 // T == c256 // T) & (c256 <= r256))

    lat, ctx, normed, ready = s["lat"], s["ctx"], s["normed"], s["ready"]
    gain_row = s["gain"]

    def norm_rows(x):
        x = x.astype(F32)
        factor = lax.rsqrt(jnp.mean(x * x, axis=-1, keepdims=True) + EPS)
        return x * factor * gain_row[...]

    loaded("latent", "context", "gain")

    @pl.loop(0, CROWS // 16)
    def _(i):
        at = pl.multiple_of(i * 16, 16)
        ready[pl.ds(ROWS + at, 16), :] = norm_rows(ctx[pl.ds(at, 16), :])

    @pl.loop(0, ROWS // 16)
    def _(i):
        at = pl.ds(pl.multiple_of(i * 16, 16), 16)
        ready[at, :] = norm_rows(lat[at, :])

    arrive("sp", lambda i: mod1.at[i], s["m1s"], s["m1r"])
    total = mod1[0]
    for i in range(1, NSP):
        total = total + mod1[i]
    mod2[tp] = total
    exchange("tp", lambda to: mod2.at[tp], lambda i: mod2.at[i], s["m2s"], s["m2r"])
    ld, lcum, kk, vv = s["ld"], s["lcum"], s["kk"], s["vv"]
    acc, acc_low = s["acc"], s["acc_low"]
    own, ctx_rows = slice(0, ROWS), slice(ROWS, ALL)
    loaded("bias", "up", "post", "down", "key", "value", "query", "outgate", "out")

    def columns(origin):
        return pl.ds(pl.multiple_of(origin * 256, 256), 256)

    def modulate(origin):
        slot = mod2[origin]

        def row(i):
            return jnp.concatenate([slot[i : i + 1], slot[5 + i : 6 + i]], axis=1)

        cols = columns(origin)
        for rows, i in ((own, 0), (ctx_rows, 1)):
            values = ready[rows, cols] * (1.0 + row(2 + i)) + row(i)
            normed[rows, cols] = values.astype(BF16)

    def low_part(origin):
        cols = columns(origin)
        return dot_dims(normed[own, cols], s["wd"][:, cols], 1, 1)

    def key_part(origin):
        cols = columns(origin)
        return dot(normed[own, cols], s["wk"][cols, :])

    def value_part(origin, at):
        cols = columns(origin)
        return dot(normed[own, cols], s["wv"][cols, at])

    v_half = (slice(0, 512), slice(512, 1024))
    a_half = (slice(512, 1024), slice(1024, 1536))

    def take(origin, first=False):
        modulate(origin)
        low, key = low_part(origin), key_part(origin)
        acc_low[...] = low if first else acc_low[...] + low
        acc[:, 0:512] = key if first else acc[:, 0:512] + key
        for v_at, a_at in zip(v_half, a_half):
            value = value_part(origin, v_at)
            acc[:, a_at] = value if first else acc[:, a_at] + value

    def tp_origin(step):
        return tp_peer((4 - step[0], 2 - step[1]))

    def arrive_mod(step):
        arrive("tp", lambda i: mod2.at[i], s["m2s"], s["m2r"], only=step)

    take(tp, True)
    for step in ((0, 1), (1, 0), (3, 0), (1, 1), (3, 1)):
        arrive_mod(step)
        take(tp_origin(step))
    last = ((2, 0), (2, 1))
    for step in last:
        arrive_mod(step)
    one, two = (tp_origin(step) for step in last)
    modulate(one)
    modulate(two)
    low = (acc_low[...] + low_part(one) + low_part(two)).astype(BF16)
    kk[own, :] = (acc[:, 0:512] + key_part(one) + key_part(two)).astype(BF16)
    ld[own, :] = log_decays(dot(low, s["up_w"][...]) + s["bias"][...])

    def put_values(i):
        at = v_half[i]
        total = acc[:, a_half[i]] + value_part(one, at) + value_part(two, at)
        vv[own, at] = total.astype(BF16)

    put_values(0)
    lcum[own, :] = sum_rows(tri[...], ld[own, :])
    put_values(1)

    def project(rows):
        low = dot_dims(normed[rows, :], s["wd"][...], 1, 1).astype(BF16)
        ld[rows, :] = log_decays(dot(low, s["up_w"][...]) + s["bias"][...])
        kk[rows, :] = dot(normed[rows, :], s["wk"][...]).astype(BF16)
        for at in v_half:
            vv[rows, at] = dot(normed[rows, :], s["wv"][:, at]).astype(BF16)

    ent, tots, kd = s["ent"], s["tots"], s["kd"]
    ctx_msg, seg_msg = s["ctx_msg"], s["seg_msg"]
    ctx_all, recv_a, grp_all, back, recv_c = (
        s["ctx_all"],
        s["recv_a"],
        s["grp_all"],
        s["back"],
        s["recv_c"],
    )
    lane_head = lax.rem(iota((64, 256), 1), 128) // 32
    closings = [lcum[n * T + T - 8 : n * T + T, :][7:8] for n in range(NB)]
    whole = closings[0] + closings[1] + closings[2] + closings[3]

    def own_lanes(full):
        state = jnp.zeros((64, 256), F32)
        for h in range(4):
            state = jnp.where(lane_head == h, full[h * 64 : (h + 1) * 64], state)
        return state

    for n in range(NB):
        tots[n : n + 1, :] = closings[n]
        rows = slice(n * T, (n + 1) * T)
        ahead = behind = jnp.zeros((1, 512), F32)
        for m in range(n):
            ahead = ahead + closings[m]
        for m in range(n + 1, NB):
            behind = behind + closings[m]
        cum = lcum[rows, :]
        keys = kk[rows, :].astype(F32)
        key_f = (keys * jnp.exp(closings[n] - cum + behind)).astype(BF16)
        key_b = (keys * jnp.exp(cum - ld[rows, :] + ahead)).astype(BF16)
        for g in range(NG):
            k_at = slice(g * 128, (g + 1) * 128)
            kd[rows, g * 256 : (g + 1) * 256] = jnp.concatenate(
                [key_f[:, k_at], key_b[:, k_at]], axis=1
            )
    tots[NB : NB + 1, :] = whole
    for dy in (2, 1, 3, 0):
        g = lax.rem(y + dy, 4)
        v_at = pl.ds(pl.multiple_of(g * 256, 256), 256)
        state = own_lanes(dot_dims(vv[own, v_at], kd[:, v_at], 0, 0))
        whole_g = tots[NB : NB + 1, pl.ds(pl.multiple_of(g * 128, 128), 128)]
        for d in range(2):
            put_message(seg_msg, 2 * g + d, state[:, d * 128 : (d + 1) * 128], whole_g)
        exchange(
            "tp", lambda to: seg_msg.at[to], lambda i: recv_a.at[i], s["as"], s["ar"], only=dy
        )
    recv_a[tp] = seg_msg[tp]

    project(ctx_rows)
    lcum[ctx_rows, :] = sum_rows(tri[0:CROWS, 0:CROWS], ld[ctx_rows, :])
    summ = s["summ"]

    def summaries(rows, count, put):
        cum = lcum[rows, :]
        before = cum - ld[rows, :]
        closing = cum[count - 1 : count, :]
        keys = kk[rows, :].astype(F32)
        key_f = (keys * jnp.exp(closing - cum)).astype(BF16)
        key_b = (keys * jnp.exp(before)).astype(BF16)
        for g in range(NG):
            k_at = slice(g * 128, (g + 1) * 128)
            both = jnp.concatenate([key_f[:, k_at], key_b[:, k_at]], axis=1)
            put(g, own_lanes(dot_dims(vv[rows, g * 256 : (g + 1) * 256], both, 0, 0)))

    ctx_total = lcum[ALL - 8 : ALL, :][7:8]

    def put_context(g, state):
        for d in range(2):
            put_message(
                ctx_msg,
                2 * g + d,
                state[:, d * 128 : (d + 1) * 128],
                ctx_total[:, g * 128 : (g + 1) * 128],
            )

    summaries(ctx_rows, CROWS, put_context)
    ctx_all[sp] = ctx_msg[tp]
    exchange("sp", lambda to: ctx_all.at[sp], lambda i: ctx_all.at[i], s["cs"], s["cr"])

    qq, gg = s["qq"], s["gg"]
    qq[...] = dot(normed[0:ROWS, :], s["wq"][...]).astype(BF16)

    @pl.loop(0, NB)
    def _(n):
        def put(g, state):
            summ[n, :, g * 256 : (g + 1) * 256] = state

        summaries(pl.ds(pl.multiple_of(n * T, T), T), T, put)

    for g in range(NG):
        close = [jnp.exp(tots[n : n + 1, g * 128 : (g + 1) * 128]) for n in range(NB)]
        for d in range(2):
            at = slice(g * 256 + d * 128, g * 256 + (d + 1) * 128)
            run = jnp.zeros((64, 128), F32)
            for n in range(NB) if d == 0 else reversed(range(NB)):
                ent[n, :, at] = run.astype(BF16)
                run = close[n] * run + summ[n, :, at]

    arrive("tp", lambda i: recv_a.at[i], s["as"], s["ar"])
    pre_s, pre_c = s["pre_s"], s["pre_c"]
    run = jnp.zeros((64, 128), F32)
    run_log = jnp.zeros((1, 128), F32)
    for i in range(NTP):
        at = i + flip * (NTP - 1 - 2 * i)
        pre_s[at] = run
        pre_c[at] = jnp.broadcast_to(run_log, (8, 128))
        state, total = get_message(recv_a, at)
        run = jnp.exp(total) * run + state
        run_log = run_log + total
    put_message(grp_all, sp, run, run_log)
    exchange("sp", lambda to: grp_all.at[sp], lambda i: grp_all.at[i], s["gs"], s["gr"], True)


    @pl.loop(0, 2)
    def _(c):
        at = pl.ds(pl.multiple_of(c * 512, 512), 512)
        gg[:, at] = dot(normed[0:ROWS, :], s["wg"][:, at]).astype(BF16)

    mixed, qd = s["mixed"], s["qd"]
    t_row = iota((64, 256), 0)
    s_col = lax.rem(iota((64, 256), 1), 64)
    up_to, from_on = s_col <= t_row, s_col >= t_row

    def four(x, mask):
        return jnp.concatenate([x, x, x, x], axis=0) * mask

    @pl.loop(0, NB)
    def _(n):
        rows = pl.ds(pl.multiple_of(n * T, T), T)
        cum = lcum[rows, :]
        before = cum - ld[rows, :]
        middle, closing = cum[T // 2 - 1 : T // 2, :], cum[T - 1 : T, :]
        ahead = jnp.zeros((1, 512), F32)
        behind = jnp.zeros((1, 512), F32)
        for m in range(NB):
            ahead = ahead + jnp.where(m < n, tots[m : m + 1, :], 0.0)
            behind = behind + jnp.where(m > n, tots[m : m + 1, :], 0.0)
        q = qq[rows, :].astype(F32) * DK**-0.5
        k = kk[rows, :].astype(F32)
        qm_f = (q * jnp.exp(cum - middle)).astype(BF16)
        qm_b = (q * jnp.exp(middle - before)).astype(BF16)
        km_f = (k * jnp.exp(middle - cum)).astype(BF16)
        km_b = (k * jnp.exp(before - middle)).astype(BF16)
        qs_f = (q * jnp.exp(cum)).astype(BF16)
        qs_b = (q * jnp.exp(closing - before)).astype(BF16)
        qd_f = (q * jnp.exp(cum + ahead)).astype(BF16)
        qd_b = (q * jnp.exp(closing - before + behind)).astype(BF16)
        for g in range(NG):
            k_at = slice(g * 128, (g + 1) * 128)
            v_at = slice(g * 256, (g + 1) * 256)
            qd[rows, v_at] = jnp.concatenate([qd_f[:, k_at], qd_b[:, k_at]], axis=1)
            score_f = dot_dims(qm_f[:, k_at], four(km_f[:, k_at], head128[...]), 1, 1)
            score_b = dot_dims(qm_b[:, k_at], four(km_b[:, k_at], head128[...]), 1, 1)
            score = jnp.where(up_to, score_f, 0.0) + jnp.where(from_on, score_b, 0.0)
            within = dot(score.astype(BF16), four(vv[rows, v_at], head256[...]))
            entering = ent[n, :, v_at]
            states = jnp.concatenate(
                [
                    four(entering[:, 0:128], head128[...]),
                    four(entering[:, 128:256], head128[...]),
                ],
                axis=1,
            )
            across = dot_dims(
                jnp.concatenate([qs_f[:, k_at], qs_b[:, k_at]], axis=1), states, 1, 1
            )
            mixed[rows, v_at] = within + across

    arrive("sp", lambda i: ctx_all.at[i], s["cs"], s["cr"])
    reach = jnp.zeros((64, 128), F32)
    for i in range(NSP):
        state, total = get_message(ctx_all, i + flip * (NSP - 1 - 2 * i))
        reach = jnp.exp(total) * reach + state
    arrive("sp", lambda i: grp_all.at[i], s["gs"], s["gr"], True)
    rank = sp + flip * (NSP - 1 - 2 * sp)
    for i in range(NSP):
        state, total = get_message(grp_all, i + flip * (NSP - 1 - 2 * i))
        reach = jnp.where(i < rank, jnp.exp(total) * reach + state, reach)
    for dy in (2, 1, 3, 0):
        for dc in range(2):
            j = tp_peer((dy, dc))
            back[j] = (pre_s[j] + jnp.exp(pre_c[j][0:1]) * reach).astype(BF16)
        exchange(
            "tp", lambda to: back.at[to], lambda i: recv_c.at[i], s["bs"], s["br"], only=dy
        )
    recv_c[tp] = back[tp]
    ones[...] = head256[...]
    silu = s["silu"]

    @pl.loop(0, ROWS // 32)
    def _(i):
        at = pl.ds(pl.multiple_of(i * 32, 32), 32)
        gate = gg[at, :].astype(F32)
        silu[at, :] = gate * lax.logistic(gate)

    weight = s["weight"]
    for j in range(2 * NTP):
        at = slice(j * 128, (j + 1) * 128)
        gate_row = mod2[j // 2][4 + 5 * (j % 2) : 5 + 5 * (j % 2)]
        weight[:, at] = jnp.broadcast_to(gate_row * s["post_gain"][:, at], (8, 128))

    acc_out = s["acc_out"]

    def gated_group(dy):
        for dc in (0, 1):
            if (dy, dc) != (0, 0):
                arrive("tp", lambda i: recv_c.at[i], s["bs"], s["br"], only=(dy, dc))
        g = lax.rem(y + 4 - dy, 4)
        v_at = pl.ds(pl.multiple_of(g * 256, 256), 256)
        states = jnp.concatenate(
            [four(recv_c[2 * g], head128[...]), four(recv_c[2 * g + 1], head128[...])], axis=1
        )
        values = mixed[:, v_at] + dot_dims(qd[:, v_at], states, 1, 1)
        square = values * values
        hi = square.astype(BF16)
        low = (square - hi.astype(F32)).astype(BF16)
        power = dot(hi, ones[...]) + dot(low, ones[...])
        normal = values * lax.rsqrt(power * (1.0 / DV) + EPS)
        return (normal * silu[:, v_at]).astype(BF16), v_at

    for i, dy in enumerate((0, 1, 3)):
        gated, k_rows = gated_group(dy)
        for j in range(4):
            at = slice(j * 512, (j + 1) * 512)
            part = dot(gated, s["wo"][k_rows, at])
            acc_out[:, at] = part if i == 0 else acc_out[:, at] + part
    gated, k_rows = gated_group(2)

    branch = s["branch"]
    squares = jnp.zeros((ROWS, 128), F32)
    for i in range(8):
        at = slice(i * 256, (i + 1) * 256)
        part = (acc_out[:, at] + dot(gated, s["wo"][k_rows, at])).astype(BF16)
        branch[:, at] = part
        part = part.astype(F32)
        part = part * part
        for j in range(2):
            squares = squares + part[:, j * 128 : (j + 1) * 128]
    mean = jnp.sum(squares, axis=-1, keepdims=True) * (1.0 / D)
    factors = lax.rsqrt(mean + EPS)
    for k in range(ROWS // 16):
        at = slice(k * 16, (k + 1) * 16)
        added = branch[at, :].astype(F32) * factors[at] * weight[0:1, :]
        out[at, :] = (lat[at, :].astype(F32) + added).astype(BF16)

    for copy, later in sends:
        if later is None:
            copy.wait_send()
        else:
            pl.when(later)(copy.wait_send)


def scratch():
    vmem, sems = pltpu.VMEM, pltpu.SemaphoreType.DMA
    return dict(
        lat=vmem((ROWS, D), BF16),
        ctx=vmem((CROWS, D), BF16),
        wd=vmem((32, D), BF16),
        wk=vmem((D, 512), BF16),
        wv=vmem((D, 1024), BF16),
        wq=vmem((D, 512), BF16),
        wg=vmem((D, 1024), BF16),
        wo=vmem((1024, D), BF16),
        mod1=vmem((NSP, 10, 128), F32),
        mod2=vmem((NTP, 10, 128), F32),
        acc=vmem((ROWS, 1536), F32),
        acc_low=vmem((ROWS, 32), F32),
        normed=vmem((ALL, D), BF16),
        head128=vmem((256, 128), BF16),
        head256=vmem((256, 256), BF16),
        ones=vmem((256, 256), BF16),
        tri=vmem((256, 256), BF16),
        ld=vmem((ALL, 512), F32),
        lcum=vmem((ALL, 512), F32),
        kk=vmem((ALL, 512), BF16),
        vv=vmem((ALL, 1024), BF16),
        qq=vmem((ROWS, 512), BF16),
        gg=vmem((ROWS, 1024), BF16),
        summ=vmem((NB, 64, 1024), F32),
        kd=vmem((ROWS, 1024), BF16),
        silu=vmem((ROWS, 1024), F32),
        ent=vmem((NB, 64, 1024), BF16),
        tots=vmem((8, 512), F32),
        ctx_msg=vmem((NTP, MSG, 128), BF16),
        seg_msg=vmem((NTP, MSG, 128), BF16),
        ctx_all=vmem((NSP, MSG, 128), BF16),
        grp_all=vmem((NSP, MSG, 128), BF16),
        recv_a=vmem((NTP, MSG, 128), BF16),
        pre_s=vmem((NTP, 64, 128), F32),
        pre_c=vmem((NTP, 8, 128), F32),
        back=vmem((NTP, 64, 128), BF16),
        recv_c=vmem((NTP, 64, 128), BF16),
        mixed=vmem((ROWS, 1024), F32),
        qd=vmem((ROWS, 1024), BF16),
        acc_out=vmem((ROWS, D), F32),
        branch=vmem((ROWS, D), BF16),
        lat_cond=vmem((16, 128), BF16),
        ctx_cond=vmem((16, 128), BF16),
        shift_w=vmem((128, 256), BF16),
        scale_w=vmem((128, 256), BF16),
        gate_w=vmem((128, 256), BF16),
        gain=vmem((1, D), F32),
        bias=vmem((1, 512), F32),
        up_w=vmem((32, 512), BF16),
        post_gain=vmem((1, D), F32),
        ready=vmem((ALL, D), F32),
        weight=vmem((8, D), F32),
        load_sem=sems((17,)),
        m1s=sems((NSP - 1,)),
        m1r=sems((NSP - 1,)),
        m2s=sems((NTP - 1,)),
        m2r=sems((NTP - 1,)),
        cs=sems((NSP - 1,)),
        cr=sems((NSP - 1,)),
        gs=sems((NSP - 1,)),
        gr=sems((NSP - 1,)),
        bs=sems((NTP - 1,)),
        br=sems((NTP - 1,)),
        **{"as": sems((NTP - 1,)), "ar": sems((NTP - 1,))},
    )


def shards(
    latent,
    context,
    latent_condition,
    context_condition,
    shift_weight,
    scale_weight,
    gate_weight,
    norm_gain,
    query_weight,
    key_weight,
    value_weight,
    outgate_weight,
    down_weight,
    up_weight,
    decay_bias,
    out_weight,
    post_gain,
):
    hbm = pl.BlockSpec(memory_space=pl.ANY)
    return pl.pallas_call(
        kernel,
        out_shape=pltpu.VMEM((ROWS, D), BF16),
        in_specs=[hbm] * 17,
        out_specs=pl.BlockSpec(memory_space=pltpu.VMEM),
        scratch_shapes=[scratch()],
        compiler_params=pltpu.CompilerParams(
            collective_id=0, has_side_effects=True, vmem_limit_bytes=60 * 1024 * 1024
        ),
    )(
        latent,
        context,
        latent_condition.reshape(16, 128),
        context_condition.reshape(16, 128),
        shift_weight,
        scale_weight,
        gate_weight,
        norm_gain[None],
        query_weight,
        key_weight,
        value_weight,
        outgate_weight,
        down_weight.T,
        up_weight,
        decay_bias[None],
        out_weight,
        post_gain[None],
    )


def solution(mesh):
    tokens = P(("sp", "tp"), None)
    maps = P("sp", "tp")
    placed = (tokens, P("sp", None), P(), P(), maps, maps, maps) + (P(),) * 10
    return jax.shard_map(
        shards, mesh=mesh, in_specs=placed, out_specs=tokens, check_vma=False
    )
```

```python
import jax
import jax.numpy as jnp
from jax import lax
from jax.experimental import pallas as pl
from jax.experimental.pallas import tpu as pltpu
from jax.sharding import PartitionSpec as P

F32 = jnp.float32
BF16 = jnp.bfloat16
MESH = pl.DeviceIdType.MESH
EPS = 1e-06

NSP = 16
NTP = 8
D = 2048
HEADS = 16
DK = 32
DV = 64
ROWS = 256
CROWS = 32
ALL = ROWS + CROWS
T = 64
NB = ROWS // T
NG = 4
MSG = 80


def far_first(lengths):
    steps = [(a, b) for a in range(lengths[0]) for b in range(lengths[1]) if (a, b) != (0, 0)]
    hops = [0, 1, 2, 1]
    weight = 2 if lengths[1] == 2 else 1
    return sorted(steps, key=lambda t: -(weight * hops[t[0]] + hops[t[1]]))


SP_STEPS = far_first((4, 4))
TP_STEPS = far_first((4, 2))


def dot(a, b):
    return jnp.dot(a, b, preferred_element_type=F32)


def dot_dims(a, b, ca, cb):
    return lax.dot_general(a, b, (((ca,), (cb,)), ((), ())), preferred_element_type=F32)


def iota(shape, dim):
    return lax.broadcasted_iota(jnp.int32, shape, dim)


def split3(x):
    hi = x.astype(BF16)
    rest = x - hi.astype(F32)
    mid = rest.astype(BF16)
    return hi, mid, (rest - mid.astype(F32)).astype(BF16)


def sum_rows(tri, x):
    hi, mid, lo = split3(x)
    return dot(tri, hi) + dot(tri, mid) + dot(tri, lo)


def log_decays(pre):
    return (jnp.minimum(pre, 0.0) - jnp.log1p(jnp.exp(-jnp.abs(pre)))) * (1.0 / 16.0)


def put_message(ref, at, state, total):
    hi, mid, lo = split3(total)
    row = iota((16, 128), 0)
    tail = jnp.where(
        row == 0,
        hi.astype(F32),
        jnp.where(row == 1, mid.astype(F32), jnp.where(row == 2, lo.astype(F32), 0.0)),
    )
    ref[at, 0:64, :] = state.astype(BF16)
    ref[at, 64:MSG, :] = tail.astype(BF16)


def get_message(ref, at):
    state = ref[at, 0:64, :].astype(F32)
    tail = ref[at, 64:MSG, :].astype(F32)
    return state, tail[0:1] + tail[1:2] + tail[2:3]


def kernel(
    latent,
    context,
    lat_cond,
    ctx_cond,
    shift_w,
    scale_w,
    gate_w,
    gain,
    query_w,
    key_w,
    value_w,
    outgate_w,
    down_w,
    up_w,
    bias,
    out_w,
    post_gain,
    out,
    s,
):
    sp = lax.axis_index("sp")
    tp = lax.axis_index("tp")

    z, x = lax.div(sp, 4), lax.rem(sp, 4)
    y, c = lax.div(tp, 2), lax.rem(tp, 2)

    def sp_peer(step):
        return lax.rem(z + step[0], 4) * 4 + lax.rem(x + step[1], 4)

    def tp_peer(step):
        return lax.rem(y + step[0], 4) * 2 + lax.rem(c + step[1], 2)

    barrier = pltpu.get_barrier_semaphore()
    for step in SP_STEPS:
        pl.semaphore_signal(barrier, inc=1, device_id=(sp_peer(step), tp), device_id_type=MESH)
    for step in TP_STEPS:
        pl.semaphore_signal(barrier, inc=1, device_id=(sp, tp_peer(step)), device_id_type=MESH)

    pairs = dict(
        lat_cond=(lat_cond, s["lat_cond"]),
        ctx_cond=(ctx_cond, s["ctx_cond"]),
        shift=(shift_w, s["shift_w"]),
        scale=(scale_w, s["scale_w"]),
        gate=(gate_w, s["gate_w"]),
        latent=(latent, s["lat"]),
        context=(context, s["ctx"]),
        gain=(gain, s["gain"]),
        bias=(bias, s["bias"]),
        up=(up_w, s["up_w"]),
        post=(post_gain, s["post_gain"]),
        down=(down_w, s["wd"]),
        key=(key_w, s["wk"]),
        value=(value_w, s["wv"]),
        query=(query_w, s["wq"]),
        outgate=(outgate_w, s["wg"]),
        out=(out_w, s["wo"]),
    )
    loads = {
        name: pltpu.make_async_copy(src, dst, s["load_sem"].at[i])
        for i, (name, (src, dst)) in enumerate(pairs.items())
    }
    for name in loads:
        loads[name].start()

    def loaded(*names):
        for name in names:
            loads[name].wait()

    sends = []

    flip = c

    def exchange(axis, src, dst, send_sem, recv_sem, ordered=False):
        steps, peer = (SP_STEPS, sp_peer) if axis == "sp" else (TP_STEPS, tp_peer)
        for d, step in enumerate(steps):
            to = peer(step)
            copy = pltpu.make_async_remote_copy(
                src_ref=src(to),
                dst_ref=dst(sp if axis == "sp" else tp),
                send_sem=send_sem.at[d],
                recv_sem=recv_sem.at[d],
                device_id=(to, tp) if axis == "sp" else (sp, to),
                device_id_type=MESH,
            )
            later = (to - sp) * (1 - 2 * flip) > 0 if ordered else None
            if ordered:
                pl.when(later)(copy.start)
            else:
                copy.start()
            sends.append((copy, later))

    def arrive(axis, dst, send_sem, recv_sem, ordered=False, only=None):
        steps, wrap, peer = (
            (SP_STEPS, (4, 4), sp_peer) if axis == "sp" else (TP_STEPS, (4, 2), tp_peer)
        )
        for d, step in reversed(list(enumerate(steps))):
            if only is not None and step != only:
                continue
            origin = peer((wrap[0] - step[0], wrap[1] - step[1]))
            copy = pltpu.make_async_remote_copy(
                src_ref=dst(origin),
                dst_ref=dst(origin),
                send_sem=send_sem.at[d],
                recv_sem=recv_sem.at[d],
                device_id=(origin, tp) if axis == "sp" else (sp, origin),
                device_id_type=MESH,
            )
            if ordered:
                pl.when((sp - origin) * (1 - 2 * flip) > 0)(copy.wait_recv)
            else:
                copy.wait_recv()

    loaded("lat_cond", "ctx_cond", "shift", "scale", "gate")
    row16 = iota((16, 128), 0)

    def cond_row(name):
        mine = jnp.where(row16 == sp, s[name][...].astype(F32), 0.0)
        return jnp.broadcast_to(jnp.sum(mine, axis=0, keepdims=True), (16, 128))

    cond = jnp.where(lax.rem(row16, 2) == 0, cond_row("lat_cond"), cond_row("ctx_cond"))
    act = (cond * lax.logistic(cond)).astype(BF16)
    shift_part, scale_part, gate_part = (
        dot(act, s[name][...])[0:8] for name in ("shift_w", "scale_w", "gate_w")
    )
    gate1, gate2 = s["gate1"], s["gate2"]
    for i in range(2):
        half = slice(i * 128, (i + 1) * 128)
        s["mod1"][sp, 4 * i : 4 * i + 2, :] = shift_part[0:2, half]
        s["mod1"][sp, 4 * i + 2 : 4 * i + 4, :] = scale_part[0:2, half]
        gate1[sp, i : i + 1, :] = gate_part[0:1, half]
    mod1, mod2 = s["mod1"], s["mod2"]
    pl.semaphore_wait(barrier, NSP + NTP - 2)
    exchange("sp", lambda to: mod1.at[sp], lambda i: mod1.at[i], s["m1s"], s["m1r"])

    head128, head256, tri, ones = s["head128"], s["head256"], s["tri"], s["ones"]

    def as_bf16(cond):
        return jnp.where(cond, 1.0, 0.0).astype(BF16)

    head128[...] = as_bf16(iota((256, 128), 0) // 64 == iota((256, 128), 1) // 32)
    head256[...] = as_bf16(iota((256, 256), 0) // 64 == iota((256, 256), 1) // 64)
    r256, c256 = iota((256, 256), 0), iota((256, 256), 1)
    tri[...] = as_bf16((r256 // T == c256 // T) & (c256 <= r256))

    lat, ctx, normed, ready = s["lat"], s["ctx"], s["normed"], s["ready"]
    gain_row = s["gain"]

    def norm_rows(x):
        x = x.astype(F32)
        factor = lax.rsqrt(jnp.mean(x * x, axis=-1, keepdims=True) + EPS)
        return x * factor * gain_row[...]

    loaded("latent", "context", "gain")

    @pl.loop(0, CROWS // 16)
    def _(i):
        at = pl.multiple_of(i * 16, 16)
        ready[pl.ds(ROWS + at, 16), :] = norm_rows(ctx[pl.ds(at, 16), :])

    @pl.loop(0, ROWS // 16)
    def _(i):
        at = pl.ds(pl.multiple_of(i * 16, 16), 16)
        ready[at, :] = norm_rows(lat[at, :])

    arrive("sp", lambda i: mod1.at[i], s["m1s"], s["m1r"])
    total = mod1[0]
    for i in range(1, NSP):
        total = total + mod1[i]
    mod2[tp] = total
    exchange("tp", lambda to: mod2.at[tp], lambda i: mod2.at[i], s["m2s"], s["m2r"])
    exchange("sp", lambda to: gate1.at[sp], lambda i: gate1.at[i], s["g1s"], s["g1r"])
    ld, lcum, kk, vv = s["ld"], s["lcum"], s["kk"], s["vv"]
    acc, acc_low = s["acc"], s["acc_low"]
    own, ctx_rows = slice(0, ROWS), slice(ROWS, ALL)
    loaded("bias", "up", "post", "down", "key", "value", "query", "outgate", "out")

    def columns(origin):
        return pl.ds(pl.multiple_of(origin * 256, 256), 256)

    def modulate(origin):
        slot = mod2[origin]

        def row(i):
            return jnp.concatenate([slot[i : i + 1], slot[4 + i : 5 + i]], axis=1)

        cols = columns(origin)
        for rows, i in ((own, 0), (ctx_rows, 1)):
            values = ready[rows, cols] * (1.0 + row(2 + i)) + row(i)
            normed[rows, cols] = values.astype(BF16)

    def low_part(origin):
        cols = columns(origin)
        return dot_dims(normed[own, cols], s["wd"][:, cols], 1, 1)

    def key_part(origin):
        cols = columns(origin)
        return dot(normed[own, cols], s["wk"][cols, :])

    def value_part(origin, at):
        cols = columns(origin)
        return dot(normed[own, cols], s["wv"][cols, at])

    v_half = (slice(0, 512), slice(512, 1024))
    a_half = (slice(512, 1024), slice(1024, 1536))

    def take(origin, first=False):
        modulate(origin)
        low, key = low_part(origin), key_part(origin)
        acc_low[...] = low if first else acc_low[...] + low
        acc[:, 0:512] = key if first else acc[:, 0:512] + key
        for v_at, a_at in zip(v_half, a_half):
            value = value_part(origin, v_at)
            acc[:, a_at] = value if first else acc[:, a_at] + value

    def tp_origin(step):
        return tp_peer((4 - step[0], 2 - step[1]))

    def arrive_mod(step):
        arrive("tp", lambda i: mod2.at[i], s["m2s"], s["m2r"], only=step)

    take(tp, True)
    for step in ((0, 1), (1, 0), (3, 0), (1, 1), (3, 1)):
        arrive_mod(step)
        take(tp_origin(step))
    last = ((2, 0), (2, 1))
    for step in last:
        arrive_mod(step)
    one, two = (tp_origin(step) for step in last)
    modulate(one)
    modulate(two)
    low = (acc_low[...] + low_part(one) + low_part(two)).astype(BF16)
    kk[own, :] = (acc[:, 0:512] + key_part(one) + key_part(two)).astype(BF16)
    ld[own, :] = log_decays(dot(low, s["up_w"][...]) + s["bias"][...])

    def put_values(i):
        at = v_half[i]
        total = acc[:, a_half[i]] + value_part(one, at) + value_part(two, at)
        vv[own, at] = total.astype(BF16)

    put_values(0)
    lcum[own, :] = sum_rows(tri[...], ld[own, :])
    put_values(1)

    def project(rows):
        low = dot_dims(normed[rows, :], s["wd"][...], 1, 1).astype(BF16)
        ld[rows, :] = log_decays(dot(low, s["up_w"][...]) + s["bias"][...])
        kk[rows, :] = dot(normed[rows, :], s["wk"][...]).astype(BF16)
        for at in v_half:
            vv[rows, at] = dot(normed[rows, :], s["wv"][:, at]).astype(BF16)

    ent, tots, kd = s["ent"], s["tots"], s["kd"]
    ctx_msg, seg_msg = s["ctx_msg"], s["seg_msg"]
    ctx_all, recv_a, grp_all, back, recv_c = (
        s["ctx_all"],
        s["recv_a"],
        s["grp_all"],
        s["back"],
        s["recv_c"],
    )
    lane_head = lax.rem(iota((64, 256), 1), 128) // 32
    closings = [lcum[n * T + T - 8 : n * T + T, :][7:8] for n in range(NB)]
    whole = closings[0] + closings[1] + closings[2] + closings[3]

    def own_lanes(full):
        state = jnp.zeros((64, 256), F32)
        for h in range(4):
            state = jnp.where(lane_head == h, full[h * 64 : (h + 1) * 64], state)
        return state

    for n in range(NB):
        tots[n : n + 1, :] = closings[n]
        rows = slice(n * T, (n + 1) * T)
        ahead = behind = jnp.zeros((1, 512), F32)
        for m in range(n):
            ahead = ahead + closings[m]
        for m in range(n + 1, NB):
            behind = behind + closings[m]
        cum = lcum[rows, :]
        keys = kk[rows, :].astype(F32)
        key_f = (keys * jnp.exp(closings[n] - cum + behind)).astype(BF16)
        key_b = (keys * jnp.exp(cum - ld[rows, :] + ahead)).astype(BF16)
        for g in range(NG):
            k_at = slice(g * 128, (g + 1) * 128)
            kd[rows, g * 256 : (g + 1) * 256] = jnp.concatenate(
                [key_f[:, k_at], key_b[:, k_at]], axis=1
            )
    for g in range(NG):
        v_at = slice(g * 256, (g + 1) * 256)
        state = own_lanes(dot_dims(vv[own, v_at], kd[:, v_at], 0, 0))
        for d in range(2):
            put_message(
                seg_msg,
                2 * g + d,
                state[:, d * 128 : (d + 1) * 128],
                whole[:, g * 128 : (g + 1) * 128],
            )
    recv_a[tp] = seg_msg[tp]
    exchange("tp", lambda to: seg_msg.at[to], lambda i: recv_a.at[i], s["as"], s["ar"])

    project(ctx_rows)
    lcum[ctx_rows, :] = sum_rows(tri[0:CROWS, 0:CROWS], ld[ctx_rows, :])
    summ = s["summ"]

    def summaries(rows, count, put):
        cum = lcum[rows, :]
        before = cum - ld[rows, :]
        closing = cum[count - 1 : count, :]
        keys = kk[rows, :].astype(F32)
        key_f = (keys * jnp.exp(closing - cum)).astype(BF16)
        key_b = (keys * jnp.exp(before)).astype(BF16)
        for g in range(NG):
            k_at = slice(g * 128, (g + 1) * 128)
            both = jnp.concatenate([key_f[:, k_at], key_b[:, k_at]], axis=1)
            put(g, own_lanes(dot_dims(vv[rows, g * 256 : (g + 1) * 256], both, 0, 0)))

    ctx_total = lcum[ALL - 8 : ALL, :][7:8]

    def put_context(g, state):
        for d in range(2):
            put_message(
                ctx_msg,
                2 * g + d,
                state[:, d * 128 : (d + 1) * 128],
                ctx_total[:, g * 128 : (g + 1) * 128],
            )

    summaries(ctx_rows, CROWS, put_context)
    ctx_all[sp] = ctx_msg[tp]
    exchange("sp", lambda to: ctx_all.at[sp], lambda i: ctx_all.at[i], s["cs"], s["cr"])

    qq, gg = s["qq"], s["gg"]
    qq[...] = dot(normed[0:ROWS, :], s["wq"][...]).astype(BF16)

    @pl.loop(0, NB)
    def _(n):
        def put(g, state):
            summ[n, :, g * 256 : (g + 1) * 256] = state

        summaries(pl.ds(pl.multiple_of(n * T, T), T), T, put)

    for g in range(NG):
        close = [jnp.exp(tots[n : n + 1, g * 128 : (g + 1) * 128]) for n in range(NB)]
        for d in range(2):
            at = slice(g * 256 + d * 128, g * 256 + (d + 1) * 128)
            run = jnp.zeros((64, 128), F32)
            for n in range(NB) if d == 0 else reversed(range(NB)):
                ent[n, :, at] = run.astype(BF16)
                run = close[n] * run + summ[n, :, at]

    arrive("sp", lambda i: gate1.at[i], s["g1s"], s["g1r"])
    total = gate1[0]
    for i in range(1, NSP):
        total = total + gate1[i]
    gate2[tp] = total
    exchange("tp", lambda to: gate2.at[tp], lambda i: gate2.at[i], s["g2s"], s["g2r"])

    arrive("tp", lambda i: recv_a.at[i], s["as"], s["ar"])
    pre_s, pre_c = s["pre_s"], s["pre_c"]
    run = jnp.zeros((64, 128), F32)
    run_log = jnp.zeros((1, 128), F32)
    for i in range(NTP):
        at = i + flip * (NTP - 1 - 2 * i)
        pre_s[at] = run
        pre_c[at] = jnp.broadcast_to(run_log, (8, 128))
        state, total = get_message(recv_a, at)
        run = jnp.exp(total) * run + state
        run_log = run_log + total
    put_message(grp_all, sp, run, run_log)
    exchange("sp", lambda to: grp_all.at[sp], lambda i: grp_all.at[i], s["gs"], s["gr"], True)


    @pl.loop(0, 2)
    def _(c):
        at = pl.ds(pl.multiple_of(c * 512, 512), 512)
        gg[:, at] = dot(normed[0:ROWS, :], s["wg"][:, at]).astype(BF16)

    mixed, qd = s["mixed"], s["qd"]
    t_row = iota((64, 256), 0)
    s_col = lax.rem(iota((64, 256), 1), 64)
    up_to, from_on = s_col <= t_row, s_col >= t_row

    def four(x, mask):
        return jnp.concatenate([x, x, x, x], axis=0) * mask

    @pl.loop(0, NB)
    def _(n):
        rows = pl.ds(pl.multiple_of(n * T, T), T)
        cum = lcum[rows, :]
        before = cum - ld[rows, :]
        middle, closing = cum[T // 2 - 1 : T // 2, :], cum[T - 1 : T, :]
        ahead = jnp.zeros((1, 512), F32)
        behind = jnp.zeros((1, 512), F32)
        for m in range(NB):
            ahead = ahead + jnp.where(m < n, tots[m : m + 1, :], 0.0)
            behind = behind + jnp.where(m > n, tots[m : m + 1, :], 0.0)
        q = qq[rows, :].astype(F32) * DK**-0.5
        k = kk[rows, :].astype(F32)
        qm_f = (q * jnp.exp(cum - middle)).astype(BF16)
        qm_b = (q * jnp.exp(middle - before)).astype(BF16)
        km_f = (k * jnp.exp(middle - cum)).astype(BF16)
        km_b = (k * jnp.exp(before - middle)).astype(BF16)
        qs_f = (q * jnp.exp(cum)).astype(BF16)
        qs_b = (q * jnp.exp(closing - before)).astype(BF16)
        qd_f = (q * jnp.exp(cum + ahead)).astype(BF16)
        qd_b = (q * jnp.exp(closing - before + behind)).astype(BF16)
        for g in range(NG):
            k_at = slice(g * 128, (g + 1) * 128)
            v_at = slice(g * 256, (g + 1) * 256)
            qd[rows, v_at] = jnp.concatenate([qd_f[:, k_at], qd_b[:, k_at]], axis=1)
            score_f = dot_dims(qm_f[:, k_at], four(km_f[:, k_at], head128[...]), 1, 1)
            score_b = dot_dims(qm_b[:, k_at], four(km_b[:, k_at], head128[...]), 1, 1)
            score = jnp.where(up_to, score_f, 0.0) + jnp.where(from_on, score_b, 0.0)
            within = dot(score.astype(BF16), four(vv[rows, v_at], head256[...]))
            entering = ent[n, :, v_at]
            states = jnp.concatenate(
                [
                    four(entering[:, 0:128], head128[...]),
                    four(entering[:, 128:256], head128[...]),
                ],
                axis=1,
            )
            across = dot_dims(
                jnp.concatenate([qs_f[:, k_at], qs_b[:, k_at]], axis=1), states, 1, 1
            )
            mixed[rows, v_at] = within + across

    arrive("sp", lambda i: ctx_all.at[i], s["cs"], s["cr"])
    reach = jnp.zeros((64, 128), F32)
    for i in range(NSP):
        state, total = get_message(ctx_all, i + flip * (NSP - 1 - 2 * i))
        reach = jnp.exp(total) * reach + state
    arrive("sp", lambda i: grp_all.at[i], s["gs"], s["gr"], True)
    rank = sp + flip * (NSP - 1 - 2 * sp)
    for i in range(NSP):
        state, total = get_message(grp_all, i + flip * (NSP - 1 - 2 * i))
        reach = jnp.where(i < rank, jnp.exp(total) * reach + state, reach)
    for j in range(NTP):
        back[j] = (pre_s[j] + jnp.exp(pre_c[j][0:1]) * reach).astype(BF16)
    recv_c[tp] = back[tp]
    exchange("tp", lambda to: back.at[to], lambda i: recv_c.at[i], s["bs"], s["br"])
    ones[...] = head256[...]
    silu = s["silu"]

    @pl.loop(0, ROWS // 32)
    def _(i):
        at = pl.ds(pl.multiple_of(i * 32, 32), 32)
        gate = gg[at, :].astype(F32)
        silu[at, :] = gate * lax.logistic(gate)

    weight = s["weight"]
    arrive("tp", lambda i: gate2.at[i], s["g2s"], s["g2r"])
    for j in range(2 * NTP):
        at = slice(j * 128, (j + 1) * 128)
        gate_row = gate2[j // 2][j % 2 : j % 2 + 1]
        weight[:, at] = jnp.broadcast_to(gate_row * s["post_gain"][:, at], (8, 128))

    acc_out = s["acc_out"]

    def gated_group(dy):
        for dc in (0, 1):
            if (dy, dc) != (0, 0):
                arrive("tp", lambda i: recv_c.at[i], s["bs"], s["br"], only=(dy, dc))
        g = lax.rem(y + 4 - dy, 4)
        v_at = pl.ds(pl.multiple_of(g * 256, 256), 256)
        states = jnp.concatenate(
            [four(recv_c[2 * g], head128[...]), four(recv_c[2 * g + 1], head128[...])], axis=1
        )
        values = mixed[:, v_at] + dot_dims(qd[:, v_at], states, 1, 1)
        square = values * values
        hi = square.astype(BF16)
        low = (square - hi.astype(F32)).astype(BF16)
        power = dot(hi, ones[...]) + dot(low, ones[...])
        normal = values * lax.rsqrt(power * (1.0 / DV) + EPS)
        return (normal * silu[:, v_at]).astype(BF16), v_at

    for i, dy in enumerate((0, 1, 3)):
        gated, k_rows = gated_group(dy)
        for j in range(4):
            at = slice(j * 512, (j + 1) * 512)
            part = dot(gated, s["wo"][k_rows, at])
            acc_out[:, at] = part if i == 0 else acc_out[:, at] + part
    gated, k_rows = gated_group(2)

    branch = s["branch"]
    squares = jnp.zeros((ROWS, 128), F32)
    for i in range(8):
        at = slice(i * 256, (i + 1) * 256)
        part = (acc_out[:, at] + dot(gated, s["wo"][k_rows, at])).astype(BF16)
        branch[:, at] = part
        part = part.astype(F32)
        part = part * part
        for j in range(2):
            squares = squares + part[:, j * 128 : (j + 1) * 128]
    mean = jnp.sum(squares, axis=-1, keepdims=True) * (1.0 / D)
    factors = lax.rsqrt(mean + EPS)
    for k in range(ROWS // 16):
        at = slice(k * 16, (k + 1) * 16)
        added = branch[at, :].astype(F32) * factors[at] * weight[0:1, :]
        out[at, :] = (lat[at, :].astype(F32) + added).astype(BF16)

    for copy, later in sends:
        if later is None:
            copy.wait_send()
        else:
            pl.when(later)(copy.wait_send)


def scratch():
    vmem, sems = pltpu.VMEM, pltpu.SemaphoreType.DMA
    return dict(
        lat=vmem((ROWS, D), BF16),
        ctx=vmem((CROWS, D), BF16),
        wd=vmem((32, D), BF16),
        wk=vmem((D, 512), BF16),
        wv=vmem((D, 1024), BF16),
        wq=vmem((D, 512), BF16),
        wg=vmem((D, 1024), BF16),
        wo=vmem((1024, D), BF16),
        mod1=vmem((NSP, 8, 128), F32),
        gate1=vmem((NSP, 2, 128), F32),
        mod2=vmem((NTP, 8, 128), F32),
        gate2=vmem((NTP, 2, 128), F32),
        acc=vmem((ROWS, 1536), F32),
        acc_low=vmem((ROWS, 32), F32),
        normed=vmem((ALL, D), BF16),
        head128=vmem((256, 128), BF16),
        head256=vmem((256, 256), BF16),
        ones=vmem((256, 256), BF16),
        tri=vmem((256, 256), BF16),
        ld=vmem((ALL, 512), F32),
        lcum=vmem((ALL, 512), F32),
        kk=vmem((ALL, 512), BF16),
        vv=vmem((ALL, 1024), BF16),
        qq=vmem((ROWS, 512), BF16),
        gg=vmem((ROWS, 1024), BF16),
        summ=vmem((NB, 64, 1024), F32),
        kd=vmem((ROWS, 1024), BF16),
        silu=vmem((ROWS, 1024), F32),
        ent=vmem((NB, 64, 1024), BF16),
        tots=vmem((8, 512), F32),
        ctx_msg=vmem((NTP, MSG, 128), BF16),
        seg_msg=vmem((NTP, MSG, 128), BF16),
        ctx_all=vmem((NSP, MSG, 128), BF16),
        grp_all=vmem((NSP, MSG, 128), BF16),
        recv_a=vmem((NTP, MSG, 128), BF16),
        pre_s=vmem((NTP, 64, 128), F32),
        pre_c=vmem((NTP, 8, 128), F32),
        back=vmem((NTP, 64, 128), BF16),
        recv_c=vmem((NTP, 64, 128), BF16),
        mixed=vmem((ROWS, 1024), F32),
        qd=vmem((ROWS, 1024), BF16),
        acc_out=vmem((ROWS, D), F32),
        branch=vmem((ROWS, D), BF16),
        lat_cond=vmem((16, 128), BF16),
        ctx_cond=vmem((16, 128), BF16),
        shift_w=vmem((128, 256), BF16),
        scale_w=vmem((128, 256), BF16),
        gate_w=vmem((128, 256), BF16),
        gain=vmem((1, D), F32),
        bias=vmem((1, 512), F32),
        up_w=vmem((32, 512), BF16),
        post_gain=vmem((1, D), F32),
        ready=vmem((ALL, D), F32),
        weight=vmem((8, D), F32),
        load_sem=sems((17,)),
        g1s=sems((NSP - 1,)),
        g1r=sems((NSP - 1,)),
        g2s=sems((NTP - 1,)),
        g2r=sems((NTP - 1,)),
        m1s=sems((NSP - 1,)),
        m1r=sems((NSP - 1,)),
        m2s=sems((NTP - 1,)),
        m2r=sems((NTP - 1,)),
        cs=sems((NSP - 1,)),
        cr=sems((NSP - 1,)),
        gs=sems((NSP - 1,)),
        gr=sems((NSP - 1,)),
        bs=sems((NTP - 1,)),
        br=sems((NTP - 1,)),
        **{"as": sems((NTP - 1,)), "ar": sems((NTP - 1,))},
    )


def shards(
    latent,
    context,
    latent_condition,
    context_condition,
    shift_weight,
    scale_weight,
    gate_weight,
    norm_gain,
    query_weight,
    key_weight,
    value_weight,
    outgate_weight,
    down_weight,
    up_weight,
    decay_bias,
    out_weight,
    post_gain,
):
    hbm = pl.BlockSpec(memory_space=pl.ANY)
    return pl.pallas_call(
        kernel,
        out_shape=pltpu.VMEM((ROWS, D), BF16),
        in_specs=[hbm] * 17,
        out_specs=pl.BlockSpec(memory_space=pltpu.VMEM),
        scratch_shapes=[scratch()],
        compiler_params=pltpu.CompilerParams(
            collective_id=0, has_side_effects=True, vmem_limit_bytes=60 * 1024 * 1024
        ),
    )(
        latent,
        context,
        latent_condition.reshape(16, 128),
        context_condition.reshape(16, 128),
        shift_weight,
        scale_weight,
        gate_weight,
        norm_gain[None],
        query_weight,
        key_weight,
        value_weight,
        outgate_weight,
        down_weight.T,
        up_weight,
        decay_bias[None],
        out_weight,
        post_gain[None],
    )


def solution(mesh):
    tokens = P(("sp", "tp"), None)
    maps = P("sp", "tp")
    placed = (tokens, P("sp", None), P(), P(), maps, maps, maps) + (P(),) * 10
    return jax.shard_map(
        shards, mesh=mesh, in_specs=placed, out_specs=tokens, check_vma=False
    )
```

```python
import jax
import jax.numpy as jnp
from jax import lax
from jax.experimental import pallas as pl
from jax.experimental.pallas import tpu as pltpu
from jax.sharding import PartitionSpec as P

F32 = jnp.float32
BF16 = jnp.bfloat16
MESH = pl.DeviceIdType.MESH
EPS = 1e-06

NSP = 16
NTP = 8
D = 2048
HEADS = 16
DK = 32
DV = 64
ROWS = 256
CROWS = 32
ALL = ROWS + CROWS
T = 64
NB = ROWS // T
NG = 4
MSG = 80


def far_first(lengths):
    steps = [(a, b) for a in range(lengths[0]) for b in range(lengths[1]) if (a, b) != (0, 0)]
    hops = [0, 1, 2, 1]
    weight = 2 if lengths[1] == 2 else 1
    return sorted(steps, key=lambda t: -(weight * hops[t[0]] + hops[t[1]]))


SP_STEPS = far_first((4, 4))
TP_STEPS = far_first((4, 2))


def dot(a, b):
    return jnp.dot(a, b, preferred_element_type=F32)


def dot_dims(a, b, ca, cb):
    return lax.dot_general(a, b, (((ca,), (cb,)), ((), ())), preferred_element_type=F32)


def iota(shape, dim):
    return lax.broadcasted_iota(jnp.int32, shape, dim)


def split3(x):
    hi = x.astype(BF16)
    rest = x - hi.astype(F32)
    mid = rest.astype(BF16)
    return hi, mid, (rest - mid.astype(F32)).astype(BF16)


def sum_rows(tri, x):
    hi, mid, lo = split3(x)
    return dot(tri, hi) + dot(tri, mid) + dot(tri, lo)


def log_decays(pre):
    return (jnp.minimum(pre, 0.0) - jnp.log1p(jnp.exp(-jnp.abs(pre)))) * (1.0 / 16.0)


def put_message(ref, at, state, total):
    hi, mid, lo = split3(total)
    row = iota((16, 128), 0)
    tail = jnp.where(
        row == 0,
        hi.astype(F32),
        jnp.where(row == 1, mid.astype(F32), jnp.where(row == 2, lo.astype(F32), 0.0)),
    )
    ref[at, 0:64, :] = state.astype(BF16)
    ref[at, 64:MSG, :] = tail.astype(BF16)


def get_message(ref, at):
    state = ref[at, 0:64, :].astype(F32)
    tail = ref[at, 64:MSG, :].astype(F32)
    return state, tail[0:1] + tail[1:2] + tail[2:3]


def kernel(
    latent,
    context,
    lat_cond,
    ctx_cond,
    shift_w,
    scale_w,
    gate_w,
    gain,
    query_w,
    key_w,
    value_w,
    outgate_w,
    down_w,
    up_w,
    bias,
    out_w,
    post_gain,
    out,
    s,
):
    sp = lax.axis_index("sp")
    tp = lax.axis_index("tp")

    z, x = lax.div(sp, 4), lax.rem(sp, 4)
    y, c = lax.div(tp, 2), lax.rem(tp, 2)

    def sp_peer(step):
        return lax.rem(z + step[0], 4) * 4 + lax.rem(x + step[1], 4)

    def tp_peer(step):
        return lax.rem(y + step[0], 4) * 2 + lax.rem(c + step[1], 2)

    barrier = pltpu.get_barrier_semaphore()
    for step in SP_STEPS:
        pl.semaphore_signal(barrier, inc=1, device_id=(sp_peer(step), tp), device_id_type=MESH)
    for step in TP_STEPS:
        pl.semaphore_signal(barrier, inc=1, device_id=(sp, tp_peer(step)), device_id_type=MESH)

    pairs = dict(
        lat_cond=(lat_cond, s["lat_cond"]),
        ctx_cond=(ctx_cond, s["ctx_cond"]),
        shift=(shift_w, s["shift_w"]),
        scale=(scale_w, s["scale_w"]),
        gate=(gate_w, s["gate_w"]),
        latent=(latent, s["lat"]),
        context=(context, s["ctx"]),
        gain=(gain, s["gain"]),
        bias=(bias, s["bias"]),
        up=(up_w, s["up_w"]),
        post=(post_gain, s["post_gain"]),
        down=(down_w, s["wd"]),
        key=(key_w, s["wk"]),
        value=(value_w, s["wv"]),
        query=(query_w, s["wq"]),
        outgate=(outgate_w, s["wg"]),
        out=(out_w, s["wo"]),
    )
    loads = {
        name: pltpu.make_async_copy(src, dst, s["load_sem"].at[i])
        for i, (name, (src, dst)) in enumerate(pairs.items())
    }
    for name in loads:
        loads[name].start()

    def loaded(*names):
        for name in names:
            loads[name].wait()

    sends, bulk = [], []

    flip = c

    def exchange(axis, src, dst, send_sem, recv_sem, slots=None, once=False):
        steps, peer = (SP_STEPS, sp_peer) if axis == "sp" else (TP_STEPS, tp_peer)
        for d, step in enumerate(steps):
            to = peer(step)
            copy = pltpu.make_async_remote_copy(
                src_ref=src(to),
                dst_ref=dst(sp if axis == "sp" else tp),
                send_sem=send_sem.at[0 if slots is not None else d],
                recv_sem=recv_sem.at[0 if once else d],
                device_id=(to, tp) if axis == "sp" else (sp, to),
                device_id_type=MESH,
            )
            if slots is None:
                later = (to - sp) * (1 - 2 * flip) > 0
                pl.when(later)(copy.start)
                sends.append((copy, later))
            else:
                copy.start()
        if slots is not None:
            bulk.append((slots.at[pl.ds(0, len(steps))], send_sem.at[0]))

    def wait_bulk(slots, sem):
        pltpu.make_async_copy(slots, slots, sem).wait()

    def arrive(axis, dst, send_sem, recv_sem, ordered=False, only=None):
        steps, wrap, peer = (
            (SP_STEPS, (4, 4), sp_peer) if axis == "sp" else (TP_STEPS, (4, 2), tp_peer)
        )
        for d, step in reversed(list(enumerate(steps))):
            if only is not None and step != only:
                continue
            origin = peer((wrap[0] - step[0], wrap[1] - step[1]))
            copy = pltpu.make_async_remote_copy(
                src_ref=dst(origin),
                dst_ref=dst(origin),
                send_sem=send_sem.at[d if ordered else 0],
                recv_sem=recv_sem.at[d],
                device_id=(origin, tp) if axis == "sp" else (sp, origin),
                device_id_type=MESH,
            )
            if ordered:
                pl.when((sp - origin) * (1 - 2 * flip) > 0)(copy.wait_recv)
            else:
                copy.wait_recv()

    loaded("lat_cond", "ctx_cond", "shift", "scale", "gate")
    row16 = iota((16, 128), 0)

    def cond_row(name):
        mine = jnp.where(row16 == sp, s[name][...].astype(F32), 0.0)
        return jnp.broadcast_to(jnp.sum(mine, axis=0, keepdims=True), (16, 128))

    cond = jnp.where(lax.rem(row16, 2) == 0, cond_row("lat_cond"), cond_row("ctx_cond"))
    act = (cond * lax.logistic(cond)).astype(BF16)
    row8 = iota((8, 256), 0)
    part = jnp.where(
        row8 < 2,
        dot(act, s["shift_w"][...])[0:8],
        jnp.where(row8 < 4, dot(act, s["scale_w"][...])[0:8], dot(act, s["gate_w"][...])[0:8]),
    )
    mod1, mod2 = s["mod1"], s["mod2"]
    mod1[sp, 0:5, :] = part[0:5, 0:128]
    mod1[sp, 5:10, :] = part[0:5, 128:256]
    pl.semaphore_wait(barrier, NSP + NTP - 2)
    exchange("sp", lambda to: mod1.at[sp], lambda i: mod1.at[i], s["m1s"], s["m1r"], mod1, True)

    head128, head256, tri, ones = s["head128"], s["head256"], s["tri"], s["ones"]

    def as_bf16(cond):
        return jnp.where(cond, 1.0, 0.0).astype(BF16)

    head128[...] = as_bf16(iota((256, 128), 0) // 64 == iota((256, 128), 1) // 32)
    head256[...] = as_bf16(iota((256, 256), 0) // 64 == iota((256, 256), 1) // 64)
    r256, c256 = iota((256, 256), 0), iota((256, 256), 1)
    tri[...] = as_bf16((r256 // T == c256 // T) & (c256 <= r256))

    lat, ctx, normed, ready = s["lat"], s["ctx"], s["normed"], s["ready"]
    gain_row = s["gain"]

    def norm_rows(x):
        x = x.astype(F32)
        factor = lax.rsqrt(jnp.mean(x * x, axis=-1, keepdims=True) + EPS)
        return x * factor * gain_row[...]

    loaded("latent", "context", "gain")

    @pl.loop(0, CROWS // 16)
    def _(i):
        at = pl.multiple_of(i * 16, 16)
        ready[pl.ds(ROWS + at, 16), :] = norm_rows(ctx[pl.ds(at, 16), :])

    @pl.loop(0, ROWS // 16)
    def _(i):
        at = pl.ds(pl.multiple_of(i * 16, 16), 16)
        ready[at, :] = norm_rows(lat[at, :])

    wait_bulk(mod1.at[pl.ds(0, NSP - 1)], s["m1r"].at[0])
    total = mod1[0]
    for i in range(1, NSP):
        total = total + mod1[i]
    mod2[tp] = total
    exchange("tp", lambda to: mod2.at[tp], lambda i: mod2.at[i], s["m2s"], s["m2r"], mod2)
    ld, lcum, kk, vv = s["ld"], s["lcum"], s["kk"], s["vv"]
    acc, acc_low = s["acc"], s["acc_low"]
    own, ctx_rows = slice(0, ROWS), slice(ROWS, ALL)
    loaded("bias", "up", "post", "down", "key", "value", "query", "outgate", "out")

    def columns(origin):
        return pl.ds(pl.multiple_of(origin * 256, 256), 256)

    def modulate(origin):
        slot = mod2[origin]

        def row(i):
            return jnp.concatenate([slot[i : i + 1], slot[5 + i : 6 + i]], axis=1)

        cols = columns(origin)
        for rows, i in ((own, 0), (ctx_rows, 1)):
            values = ready[rows, cols] * (1.0 + row(2 + i)) + row(i)
            normed[rows, cols] = values.astype(BF16)

    def low_part(origin):
        cols = columns(origin)
        return dot_dims(normed[own, cols], s["wd"][:, cols], 1, 1)

    def key_part(origin):
        cols = columns(origin)
        return dot(normed[own, cols], s["wk"][cols, :])

    def value_part(origin, at):
        cols = columns(origin)
        return dot(normed[own, cols], s["wv"][cols, at])

    v_half = (slice(0, 512), slice(512, 1024))
    a_half = (slice(512, 1024), slice(1024, 1536))

    def take(origin, first=False):
        modulate(origin)
        low, key = low_part(origin), key_part(origin)
        acc_low[...] = low if first else acc_low[...] + low
        acc[:, 0:512] = key if first else acc[:, 0:512] + key
        for v_at, a_at in zip(v_half, a_half):
            value = value_part(origin, v_at)
            acc[:, a_at] = value if first else acc[:, a_at] + value

    def tp_origin(step):
        return tp_peer((4 - step[0], 2 - step[1]))

    def arrive_mod(step):
        arrive("tp", lambda i: mod2.at[i], s["m2s"], s["m2r"], only=step)

    take(tp, True)
    for step in ((0, 1), (1, 0), (3, 0), (1, 1), (3, 1)):
        arrive_mod(step)
        take(tp_origin(step))
    last = ((2, 0), (2, 1))
    for step in last:
        arrive_mod(step)
    one, two = (tp_origin(step) for step in last)
    modulate(one)
    modulate(two)
    low = (acc_low[...] + low_part(one) + low_part(two)).astype(BF16)
    kk[own, :] = (acc[:, 0:512] + key_part(one) + key_part(two)).astype(BF16)
    ld[own, :] = log_decays(dot(low, s["up_w"][...]) + s["bias"][...])

    def put_values(i):
        at = v_half[i]
        total = acc[:, a_half[i]] + value_part(one, at) + value_part(two, at)
        vv[own, at] = total.astype(BF16)

    put_values(0)
    lcum[own, :] = sum_rows(tri[...], ld[own, :])
    put_values(1)

    def project(rows):
        low = dot_dims(normed[rows, :], s["wd"][...], 1, 1).astype(BF16)
        ld[rows, :] = log_decays(dot(low, s["up_w"][...]) + s["bias"][...])
        kk[rows, :] = dot(normed[rows, :], s["wk"][...]).astype(BF16)
        for at in v_half:
            vv[rows, at] = dot(normed[rows, :], s["wv"][:, at]).astype(BF16)

    ent, tots, kd = s["ent"], s["tots"], s["kd"]
    ctx_msg, seg_msg = s["ctx_msg"], s["seg_msg"]
    ctx_all, recv_a, grp_all, back, recv_c = (
        s["ctx_all"],
        s["recv_a"],
        s["grp_all"],
        s["back"],
        s["recv_c"],
    )
    lane_head = lax.rem(iota((64, 256), 1), 128) // 32
    closings = [lcum[n * T + T - 8 : n * T + T, :][7:8] for n in range(NB)]
    whole = closings[0] + closings[1] + closings[2] + closings[3]

    def own_lanes(full):
        state = jnp.zeros((64, 256), F32)
        for h in range(4):
            state = jnp.where(lane_head == h, full[h * 64 : (h + 1) * 64], state)
        return state

    for n in range(NB):
        tots[n : n + 1, :] = closings[n]
        rows = slice(n * T, (n + 1) * T)
        ahead = behind = jnp.zeros((1, 512), F32)
        for m in range(n):
            ahead = ahead + closings[m]
        for m in range(n + 1, NB):
            behind = behind + closings[m]
        cum = lcum[rows, :]
        keys = kk[rows, :].astype(F32)
        key_f = (keys * jnp.exp(closings[n] - cum + behind)).astype(BF16)
        key_b = (keys * jnp.exp(cum - ld[rows, :] + ahead)).astype(BF16)
        for g in range(NG):
            k_at = slice(g * 128, (g + 1) * 128)
            kd[rows, g * 256 : (g + 1) * 256] = jnp.concatenate(
                [key_f[:, k_at], key_b[:, k_at]], axis=1
            )
    for g in range(NG):
        v_at = slice(g * 256, (g + 1) * 256)
        state = own_lanes(dot_dims(vv[own, v_at], kd[:, v_at], 0, 0))
        for d in range(2):
            put_message(
                seg_msg,
                2 * g + d,
                state[:, d * 128 : (d + 1) * 128],
                whole[:, g * 128 : (g + 1) * 128],
            )
    recv_a[tp] = seg_msg[tp]
    exchange("tp", lambda to: seg_msg.at[to], lambda i: recv_a.at[i], s["as"], s["ar"], recv_a, True)

    project(ctx_rows)
    lcum[ctx_rows, :] = sum_rows(tri[0:CROWS, 0:CROWS], ld[ctx_rows, :])
    summ = s["summ"]

    def summaries(rows, count, put):
        cum = lcum[rows, :]
        before = cum - ld[rows, :]
        closing = cum[count - 1 : count, :]
        keys = kk[rows, :].astype(F32)
        key_f = (keys * jnp.exp(closing - cum)).astype(BF16)
        key_b = (keys * jnp.exp(before)).astype(BF16)
        for g in range(NG):
            k_at = slice(g * 128, (g + 1) * 128)
            both = jnp.concatenate([key_f[:, k_at], key_b[:, k_at]], axis=1)
            put(g, own_lanes(dot_dims(vv[rows, g * 256 : (g + 1) * 256], both, 0, 0)))

    ctx_total = lcum[ALL - 8 : ALL, :][7:8]

    def put_context(g, state):
        for d in range(2):
            put_message(
                ctx_msg,
                2 * g + d,
                state[:, d * 128 : (d + 1) * 128],
                ctx_total[:, g * 128 : (g + 1) * 128],
            )

    summaries(ctx_rows, CROWS, put_context)
    ctx_all[sp] = ctx_msg[tp]
    exchange("sp", lambda to: ctx_all.at[sp], lambda i: ctx_all.at[i], s["cs"], s["cr"], ctx_all, True)

    qq, gg = s["qq"], s["gg"]
    qq[...] = dot(normed[0:ROWS, :], s["wq"][...]).astype(BF16)

    @pl.loop(0, NB)
    def _(n):
        def put(g, state):
            summ[n, :, g * 256 : (g + 1) * 256] = state

        summaries(pl.ds(pl.multiple_of(n * T, T), T), T, put)

    for g in range(NG):
        close = [jnp.exp(tots[n : n + 1, g * 128 : (g + 1) * 128]) for n in range(NB)]
        for d in range(2):
            at = slice(g * 256 + d * 128, g * 256 + (d + 1) * 128)
            run = jnp.zeros((64, 128), F32)
            for n in range(NB) if d == 0 else reversed(range(NB)):
                ent[n, :, at] = run.astype(BF16)
                run = close[n] * run + summ[n, :, at]

    wait_bulk(recv_a.at[pl.ds(0, NTP - 1)], s["ar"].at[0])
    pre_s, pre_c = s["pre_s"], s["pre_c"]
    run = jnp.zeros((64, 128), F32)
    run_log = jnp.zeros((1, 128), F32)
    for i in range(NTP):
        at = i + flip * (NTP - 1 - 2 * i)
        pre_s[at] = run
        pre_c[at] = jnp.broadcast_to(run_log, (8, 128))
        state, total = get_message(recv_a, at)
        run = jnp.exp(total) * run + state
        run_log = run_log + total
    put_message(grp_all, sp, run, run_log)
    exchange("sp", lambda to: grp_all.at[sp], lambda i: grp_all.at[i], s["gs"], s["gr"])


    @pl.loop(0, 2)
    def _(c):
        at = pl.ds(pl.multiple_of(c * 512, 512), 512)
        gg[:, at] = dot(normed[0:ROWS, :], s["wg"][:, at]).astype(BF16)

    mixed, qd = s["mixed"], s["qd"]
    t_row = iota((64, 256), 0)
    s_col = lax.rem(iota((64, 256), 1), 64)
    up_to, from_on = s_col <= t_row, s_col >= t_row

    def four(x, mask):
        return jnp.concatenate([x, x, x, x], axis=0) * mask

    @pl.loop(0, NB)
    def _(n):
        rows = pl.ds(pl.multiple_of(n * T, T), T)
        cum = lcum[rows, :]
        before = cum - ld[rows, :]
        middle, closing = cum[T // 2 - 1 : T // 2, :], cum[T - 1 : T, :]
        ahead = jnp.zeros((1, 512), F32)
        behind = jnp.zeros((1, 512), F32)
        for m in range(NB):
            ahead = ahead + jnp.where(m < n, tots[m : m + 1, :], 0.0)
            behind = behind + jnp.where(m > n, tots[m : m + 1, :], 0.0)
        q = qq[rows, :].astype(F32) * DK**-0.5
        k = kk[rows, :].astype(F32)
        qm_f = (q * jnp.exp(cum - middle)).astype(BF16)
        qm_b = (q * jnp.exp(middle - before)).astype(BF16)
        km_f = (k * jnp.exp(middle - cum)).astype(BF16)
        km_b = (k * jnp.exp(before - middle)).astype(BF16)
        qs_f = (q * jnp.exp(cum)).astype(BF16)
        qs_b = (q * jnp.exp(closing - before)).astype(BF16)
        qd_f = (q * jnp.exp(cum + ahead)).astype(BF16)
        qd_b = (q * jnp.exp(closing - before + behind)).astype(BF16)
        for g in range(NG):
            k_at = slice(g * 128, (g + 1) * 128)
            v_at = slice(g * 256, (g + 1) * 256)
            qd[rows, v_at] = jnp.concatenate([qd_f[:, k_at], qd_b[:, k_at]], axis=1)
            score_f = dot_dims(qm_f[:, k_at], four(km_f[:, k_at], head128[...]), 1, 1)
            score_b = dot_dims(qm_b[:, k_at], four(km_b[:, k_at], head128[...]), 1, 1)
            score = jnp.where(up_to, score_f, 0.0) + jnp.where(from_on, score_b, 0.0)
            within = dot(score.astype(BF16), four(vv[rows, v_at], head256[...]))
            entering = ent[n, :, v_at]
            states = jnp.concatenate(
                [
                    four(entering[:, 0:128], head128[...]),
                    four(entering[:, 128:256], head128[...]),
                ],
                axis=1,
            )
            across = dot_dims(
                jnp.concatenate([qs_f[:, k_at], qs_b[:, k_at]], axis=1), states, 1, 1
            )
            mixed[rows, v_at] = within + across

    wait_bulk(ctx_all.at[pl.ds(0, NSP - 1)], s["cr"].at[0])
    reach = jnp.zeros((64, 128), F32)
    for i in range(NSP):
        state, total = get_message(ctx_all, i + flip * (NSP - 1 - 2 * i))
        reach = jnp.exp(total) * reach + state
    arrive("sp", lambda i: grp_all.at[i], s["gs"], s["gr"], True)
    rank = sp + flip * (NSP - 1 - 2 * sp)
    for i in range(NSP):
        state, total = get_message(grp_all, i + flip * (NSP - 1 - 2 * i))
        reach = jnp.where(i < rank, jnp.exp(total) * reach + state, reach)
    for j in range(NTP):
        back[j] = (pre_s[j] + jnp.exp(pre_c[j][0:1]) * reach).astype(BF16)
    recv_c[tp] = back[tp]
    exchange("tp", lambda to: back.at[to], lambda i: recv_c.at[i], s["bs"], s["br"], recv_c)
    ones[...] = head256[...]
    silu = s["silu"]

    @pl.loop(0, ROWS // 32)
    def _(i):
        at = pl.ds(pl.multiple_of(i * 32, 32), 32)
        gate = gg[at, :].astype(F32)
        silu[at, :] = gate * lax.logistic(gate)

    weight = s["weight"]
    for j in range(2 * NTP):
        at = slice(j * 128, (j + 1) * 128)
        gate_row = mod2[j // 2][4 + 5 * (j % 2) : 5 + 5 * (j % 2)]
        weight[:, at] = jnp.broadcast_to(gate_row * s["post_gain"][:, at], (8, 128))

    acc_out = s["acc_out"]

    def gated_group(dy):
        for dc in (0, 1):
            if (dy, dc) != (0, 0):
                arrive("tp", lambda i: recv_c.at[i], s["bs"], s["br"], only=(dy, dc))
        g = lax.rem(y + 4 - dy, 4)
        v_at = pl.ds(pl.multiple_of(g * 256, 256), 256)
        states = jnp.concatenate(
            [four(recv_c[2 * g], head128[...]), four(recv_c[2 * g + 1], head128[...])], axis=1
        )
        values = mixed[:, v_at] + dot_dims(qd[:, v_at], states, 1, 1)
        square = values * values
        hi = square.astype(BF16)
        low = (square - hi.astype(F32)).astype(BF16)
        power = dot(hi, ones[...]) + dot(low, ones[...])
        normal = values * lax.rsqrt(power * (1.0 / DV) + EPS)
        return (normal * silu[:, v_at]).astype(BF16), v_at

    for i, dy in enumerate((0, 1, 3)):
        gated, k_rows = gated_group(dy)
        for j in range(4):
            at = slice(j * 512, (j + 1) * 512)
            part = dot(gated, s["wo"][k_rows, at])
            acc_out[:, at] = part if i == 0 else acc_out[:, at] + part
    gated, k_rows = gated_group(2)

    branch = s["branch"]
    squares = jnp.zeros((ROWS, 128), F32)
    for i in range(8):
        at = slice(i * 256, (i + 1) * 256)
        part = (acc_out[:, at] + dot(gated, s["wo"][k_rows, at])).astype(BF16)
        branch[:, at] = part
        part = part.astype(F32)
        part = part * part
        for j in range(2):
            squares = squares + part[:, j * 128 : (j + 1) * 128]
    mean = jnp.sum(squares, axis=-1, keepdims=True) * (1.0 / D)
    factors = lax.rsqrt(mean + EPS)
    for k in range(ROWS // 16):
        at = slice(k * 16, (k + 1) * 16)
        added = branch[at, :].astype(F32) * factors[at] * weight[0:1, :]
        out[at, :] = (lat[at, :].astype(F32) + added).astype(BF16)

    for copy, later in sends:
        pl.when(later)(copy.wait_send)
    for slots, sem in bulk:
        wait_bulk(slots, sem)


def scratch():
    vmem, sems = pltpu.VMEM, pltpu.SemaphoreType.DMA
    return dict(
        lat=vmem((ROWS, D), BF16),
        ctx=vmem((CROWS, D), BF16),
        wd=vmem((32, D), BF16),
        wk=vmem((D, 512), BF16),
        wv=vmem((D, 1024), BF16),
        wq=vmem((D, 512), BF16),
        wg=vmem((D, 1024), BF16),
        wo=vmem((1024, D), BF16),
        mod1=vmem((NSP, 10, 128), F32),
        mod2=vmem((NTP, 10, 128), F32),
        acc=vmem((ROWS, 1536), F32),
        acc_low=vmem((ROWS, 32), F32),
        normed=vmem((ALL, D), BF16),
        head128=vmem((256, 128), BF16),
        head256=vmem((256, 256), BF16),
        ones=vmem((256, 256), BF16),
        tri=vmem((256, 256), BF16),
        ld=vmem((ALL, 512), F32),
        lcum=vmem((ALL, 512), F32),
        kk=vmem((ALL, 512), BF16),
        vv=vmem((ALL, 1024), BF16),
        qq=vmem((ROWS, 512), BF16),
        gg=vmem((ROWS, 1024), BF16),
        summ=vmem((NB, 64, 1024), F32),
        kd=vmem((ROWS, 1024), BF16),
        silu=vmem((ROWS, 1024), F32),
        ent=vmem((NB, 64, 1024), BF16),
        tots=vmem((8, 512), F32),
        ctx_msg=vmem((NTP, MSG, 128), BF16),
        seg_msg=vmem((NTP, MSG, 128), BF16),
        ctx_all=vmem((NSP, MSG, 128), BF16),
        grp_all=vmem((NSP, MSG, 128), BF16),
        recv_a=vmem((NTP, MSG, 128), BF16),
        pre_s=vmem((NTP, 64, 128), F32),
        pre_c=vmem((NTP, 8, 128), F32),
        back=vmem((NTP, 64, 128), BF16),
        recv_c=vmem((NTP, 64, 128), BF16),
        mixed=vmem((ROWS, 1024), F32),
        qd=vmem((ROWS, 1024), BF16),
        acc_out=vmem((ROWS, D), F32),
        branch=vmem((ROWS, D), BF16),
        lat_cond=vmem((16, 128), BF16),
        ctx_cond=vmem((16, 128), BF16),
        shift_w=vmem((128, 256), BF16),
        scale_w=vmem((128, 256), BF16),
        gate_w=vmem((128, 256), BF16),
        gain=vmem((1, D), F32),
        bias=vmem((1, 512), F32),
        up_w=vmem((32, 512), BF16),
        post_gain=vmem((1, D), F32),
        ready=vmem((ALL, D), F32),
        weight=vmem((8, D), F32),
        load_sem=sems((17,)),
        m1s=sems((1,)),
        m1r=sems((1,)),
        m2s=sems((1,)),
        m2r=sems((NTP - 1,)),
        cs=sems((1,)),
        cr=sems((1,)),
        gs=sems((NSP - 1,)),
        gr=sems((NSP - 1,)),
        bs=sems((1,)),
        br=sems((NTP - 1,)),
        **{"as": sems((1,)), "ar": sems((1,))},
    )


def shards(
    latent,
    context,
    latent_condition,
    context_condition,
    shift_weight,
    scale_weight,
    gate_weight,
    norm_gain,
    query_weight,
    key_weight,
    value_weight,
    outgate_weight,
    down_weight,
    up_weight,
    decay_bias,
    out_weight,
    post_gain,
):
    hbm = pl.BlockSpec(memory_space=pl.ANY)
    return pl.pallas_call(
        kernel,
        out_shape=pltpu.VMEM((ROWS, D), BF16),
        in_specs=[hbm] * 17,
        out_specs=pl.BlockSpec(memory_space=pltpu.VMEM),
        scratch_shapes=[scratch()],
        compiler_params=pltpu.CompilerParams(
            collective_id=0, has_side_effects=True, vmem_limit_bytes=60 * 1024 * 1024
        ),
    )(
        latent,
        context,
        latent_condition.reshape(16, 128),
        context_condition.reshape(16, 128),
        shift_weight,
        scale_weight,
        gate_weight,
        norm_gain[None],
        query_weight,
        key_weight,
        value_weight,
        outgate_weight,
        down_weight.T,
        up_weight,
        decay_bias[None],
        out_weight,
        post_gain[None],
    )


def solution(mesh):
    tokens = P(("sp", "tp"), None)
    maps = P("sp", "tp")
    placed = (tokens, P("sp", None), P(), P(), maps, maps, maps) + (P(),) * 10
    return jax.shard_map(
        shards, mesh=mesh, in_specs=placed, out_specs=tokens, check_vma=False
    )
```
